32 devices in a mesh: fs: 8 (over z, y), tp: 4 (over x, core).
Axes of the slice: x: 2, y: 2, z: 4, core: 2. Of those that a mesh axis runs over, the one named last changes fastest.
Arguments:
- stream_in: bfloat16 [2048, 2112], P('fs'), may hold values from -6 to 6
- norm_gains: float32 [6, 2112], replicated, may hold values from 0.1 to 1.9
- gate_proj: bfloat16 [2112, 3072], P('fs', 'tp'), may hold values from -0.125 to 0.125
- up_proj: bfloat16 [2112, 3072], P('fs', 'tp'), may hold values from -0.125 to 0.125
- down_proj: bfloat16 [2112, 3072], P('fs', 'tp'), may hold values from -0.109375 to 0.109375
- outer_gate: bfloat16 [2112, 1056], P('fs', 'tp'), may hold values from -0.125 to 0.125
- inner_gate: bfloat16 [2112, 1056], P('fs', 'tp'), may hold values from -0.125 to 0.125
- value_proj: bfloat16 [2112, 1056], P('fs', 'tp'), may hold values from -0.125 to 0.125
- mixer_out: bfloat16 [2112, 1056], P('fs', 'tp'), may hold values from -0.1875 to 0.1875
- conv_taps: bfloat16 [3, 1056], replicated, may hold values from -3 to 3
Outputs:
- stream_out: bfloat16 [2048, 2112], P('fs')
The draws below stay inside these ranges and needn't reach their ends.
All inputs are finite; a program needn't handle non-finite values.
Results may differ from the reference program's by a relative error of at most 0.02.
Values may be sent and summed in bfloat16 or wider, within the bound.
A program may use at most 64 MiB of HBM per device.

```python
import jax
import jax.numpy as jnp
from jax import lax

D = 2112
FF = 3072
CW = 1056
CONV_K = 3
ROWS = 256
TOKENS = 2048
N_FS = 8
N_TP = 4


def shard_levels(key, dims, split, low, high):
    factor_of, own = 1.0, jax.random.fold_in(key, 6)
    for position, parts in split:
        steps = jnp.exp(jax.random.uniform(jax.random.fold_in(own, position), (parts,), jnp.float32, low / len(split), high / len(split)))
        factor_of = factor_of * jnp.repeat(steps, dims[position] // parts).reshape([-1 if axis == position else 1 for axis in range(len(dims))])
    return factor_of


def bell_draw(own_key, dims, width, most, split=(), held_as=jnp.bfloat16):
    values = jax.random.normal(own_key, dims, jnp.float32) * width
    if len(split) > 0:
        values = shard_levels(own_key, dims, split, -0.22, 0.18) * values
    return jnp.clip(values, min=-most, max=most).astype(held_as)


def setup_inputs(seed: int = 0) -> dict:
    key_of = jax.random.split(jax.random.key(seed), 11)
    stream_in = bell_draw(key_of[0], (TOKENS, D), 1.0, 6.0, ((0, 8),))
    norm_gains = jnp.clip(1.0 + 0.18 * jax.random.normal(key_of[1], (6, D), jnp.float32), 0.1, 1.9)
    gate_proj = bell_draw(key_of[2], (D, FF), D ** -0.5, 0.125, ((0, 8), (1, 4)))
    up_proj = bell_draw(key_of[3], (D, FF), D ** -0.5, 0.125, ((0, 8), (1, 4)))
    down_proj = bell_draw(key_of[4], (D, FF), FF ** -0.5, 0.109375, ((0, 8), (1, 4)))
    outer_gate = bell_draw(key_of[5], (D, CW), D ** -0.5, 0.125, ((0, 8), (1, 4)))
    inner_gate = bell_draw(key_of[6], (D, CW), D ** -0.5, 0.125, ((0, 8), (1, 4)))
    value_proj = bell_draw(key_of[7], (D, CW), D ** -0.5, 0.125, ((0, 8), (1, 4)))
    mixer_out = bell_draw(key_of[8], (D, CW), CW ** -0.5, 0.1875, ((0, 8), (1, 4)))
    conv_taps = bell_draw(key_of[9], (CONV_K, CW), 0.577, 3.0)
    return dict(stream_in=stream_in, norm_gains=norm_gains, gate_proj=gate_proj, up_proj=up_proj, down_proj=down_proj, outer_gate=outer_gate, inner_gate=inner_gate, value_proj=value_proj, mixer_out=mixer_out, conv_taps=conv_taps)


EPSILON = 1e-06

def scaled(values, gain):
    return values * lax.rsqrt(lax.optimization_barrier(jnp.mean(values * values, axis=-1, keepdims=True)) + EPSILON) * gain

def block_sum(inner, weight):
    span_width = inner.shape[1] // N_TP
    total = jnp.zeros((inner.shape[0], weight.shape[0]), jnp.float32)
    for shard_index in range(N_TP):
        left = inner[:, shard_index * span_width:(shard_index + 1) * span_width]
        right = weight[:, shard_index * span_width:(shard_index + 1) * span_width]
        part = lax.dot_general(left, right, (((1,), (1,)), ((), ())), preferred_element_type=jnp.float32)
        total = total + lax.optimization_barrier(part.astype(jnp.bfloat16)).astype(jnp.float32)
    return total

def half_step(stream, norm_gains, first, gate_proj, up_proj, down_proj):
    normed = scaled(stream.astype(jnp.float32), norm_gains[first]).astype(jnp.bfloat16)
    gate = jnp.dot(normed, gate_proj, preferred_element_type=jnp.float32)
    upward = jnp.dot(normed, up_proj, preferred_element_type=jnp.float32)
    hidden = (jax.nn.silu(gate) * upward).astype(jnp.bfloat16)
    summed = block_sum(hidden, down_proj)
    result = stream.astype(jnp.float32) + 0.5 * scaled(summed, norm_gains[first + 1])
    return result.astype(jnp.bfloat16)

def reference(stream_in, norm_gains, gate_proj, up_proj, down_proj, outer_gate, inner_gate, value_proj, mixer_out, conv_taps):
    after_ffn = half_step(stream_in, norm_gains, 0, gate_proj, up_proj, down_proj)
    normed = scaled(after_ffn.astype(jnp.float32), norm_gains[2]).astype(jnp.bfloat16)
    outer = jnp.dot(normed, outer_gate, preferred_element_type=jnp.float32).astype(jnp.bfloat16)
    inner = jnp.dot(normed, inner_gate, preferred_element_type=jnp.float32).astype(jnp.bfloat16)
    value = jnp.dot(normed, value_proj, preferred_element_type=jnp.float32).astype(jnp.bfloat16)
    gated = (inner.astype(jnp.float32) * value.astype(jnp.float32)).reshape(N_FS, ROWS, CW)
    padded = jnp.pad(gated, ((0, 0), (CONV_K - 1, 0), (0, 0)))
    taps = conv_taps.astype(jnp.float32)
    conv = jnp.zeros_like(gated)
    for offset in range(CONV_K):
        conv = conv + taps[offset] * padded[:, offset:offset + ROWS]
    mixed = (outer.astype(jnp.float32) * conv.reshape(N_FS * ROWS, CW)).astype(jnp.bfloat16)
    summed = block_sum(mixed, mixer_out)
    after_mixer = (after_ffn.astype(jnp.float32) + scaled(summed, norm_gains[3])).astype(jnp.bfloat16)
    return half_step(after_mixer, norm_gains, 4, gate_proj, up_proj, down_proj)
```

```python
import functools

import jax
import jax.numpy as jnp
from jax import lax
from jax.experimental import pallas as pl
from jax.experimental.pallas import tpu as pltpu
from jax.sharding import PartitionSpec as P

MESH = pl.DeviceIdType.MESH
EPSILON = 1e-06
CONV_K = 3
F32, BF16 = jnp.float32, jnp.bfloat16
NT = (((1,), (1,)), ((), ()))


def kernel(cfg, *refs):
    Z, Y, X, shard, sent, width, hc, nff, main, rem = cfg
    own_refs = refs[:8]
    stream_ref, gains_ref, taps_ref, out_ref = refs[8:12]
    (ff, g3, g4, normed, acc, hidden, csend, crecv, xsend, xrecv, res,
     lsem, zsend, recv, asend, arecv, csem, xssem, xrsem, rsem) = refs[12:]
    rows, Dp = stream_ref.shape
    half, quarter = rows // 2, rows // 4
    K3, K4 = nff, nff + 1
    f, t = lax.axis_index("fs"), lax.axis_index("tp")
    z, y = f // Y, f % Y
    c, x = t % 2, t // 2
    core_peer = (f, x * 2 + 1 - c)
    x_peers = [(f, ((x + j) % X) * 2 + c) for j in range(1, X)]

    def dev_z(zz):
        return (zz * Y + y, t)

    dev_y = (z * Y + (Y - 1 - y), t)

    for s in range(Z * Y):
        tail = pl.ds(s * shard + shard - 16, 16)
        for k in range(nff):
            ff[k, tail] = jnp.zeros((16, 3 * hc), BF16)
        g3[tail] = jnp.zeros((16, 2 * main), BF16)
        g4[tail] = jnp.zeros((16, 2 * main + 128), BF16)

    barrier = pltpu.get_barrier_semaphore()

    def greet(d):
        pl.semaphore_signal(barrier, inc=1, device_id=d, device_id_type=MESH)

    always = [core_peer] + x_peers + ([dev_y] if Y == 2 else [])
    for d in always:
        greet(d)
    if Z > 1:
        @pl.when(z > 0)
        def _():
            greet(dev_z(z - 1))

        @pl.when(z < Z - 1)
        def _():
            greet(dev_z(z + 1))

    def slot(k, first, count):
        at = pl.ds(pl.multiple_of(first * shard, 16), (count - 1) * shard + sent)
        if k < nff:
            return ff.at[k, at]
        return (g3 if k == K3 else g4).at[at]

    here = pl.ds(pl.multiple_of(f * shard, 16), sent)
    moves = []
    for k in range(nff):
        for j in range(3):
            moves.append((k, own_refs[j].at[:, pl.ds(k * hc, hc)],
                          ff.at[k, here, pl.ds(j * hc, hc)]))
    ow, iw, vw, mw, rw = own_refs[3:]
    lead = pl.ds(0, main)
    moves.append((K3, ow.at[:, lead], g3.at[here, lead]))
    moves.append((K3, iw.at[:, lead], g3.at[here, pl.ds(main, main)]))
    moves.append((K4, vw.at[:, lead], g4.at[here, lead]))
    moves.append((K4, rw, g4.at[here, pl.ds(main, 128)]))
    moves.append((K4, mw.at[:, lead], g4.at[here, pl.ds(main + 128, main)]))
    local = [
        (k, pltpu.make_async_copy(src, dst, lsem.at[n])) for n, (k, src, dst) in enumerate(moves)
    ]
    for _, copy in local:
        copy.start()

    peers = len(always)
    if Z > 1:
        peers = peers + (z > 0).astype(jnp.int32) + (z < Z - 1).astype(jnp.int32)
    pl.semaphore_wait(barrier, peers)

    def remote(k, s, way, d):
        ref = slot(k, s, 1)
        return pltpu.make_async_remote_copy(
            src_ref=ref, dst_ref=ref, send_sem=zsend.at[k, way, s], recv_sem=recv.at[k, s],
            device_id=d, device_id_type=MESH,
        )

    def remote_a(s, way, d):
        ref = slot(K4, s * Y, Y)
        return pltpu.make_async_remote_copy(
            src_ref=ref, dst_ref=ref, send_sem=asend.at[way, s], recv_sem=arecv.at[s],
            device_id=d, device_id_type=MESH,
        )

    def right(k, s, act):
        @pl.when(z < Z - 1)
        def _():
            act(remote(k, s * Y + y, 0, dev_z(z + 1)))

    def left(k, s, act):
        @pl.when(z > 0)
        def _():
            act(remote(k, s * Y + y, 1, dev_z(z - 1)))

    def across(k, s, act):
        if Y == 2:
            act(remote(k, s * Y + y, 2, dev_y))

    def go(copy):
        copy.start()

    def own(k):
        right(k, z, go)
        left(k, z, go)
        across(k, z, go)

    def zsteps(k):
        def step(i, carry):
            @pl.when(z - 1 - i >= 0)
            def _():
                s = z - 1 - i
                remote(k, s * Y + y, 0, dev_z(z - 1)).wait_recv()
                right(k, s, go)
                across(k, s, go)

            @pl.when(z + 1 + i < Z)
            def _():
                s = z + 1 + i
                remote(k, s * Y + y, 0, dev_z(z + 1)).wait_recv()
                left(k, s, go)
                across(k, s, go)

            return carry

        lax.fori_loop(0, Z - 1, step, 0)

    def wait_across(k):
        if Y == 2:
            def step(s, carry):
                remote(k, s * Y + 1 - y, 2, dev_y).wait_recv()
                return carry

            lax.fori_loop(0, Z, step, 0)

    def right_a(s, act):
        @pl.when(z < Z - 1)
        def _():
            act(remote_a(s, 0, dev_z(z + 1)))

    def left_a(s, act):
        @pl.when(z > 0)
        def _():
            act(remote_a(s, 1, dev_z(z - 1)))

    def start_a():
        if Y == 2:
            remote(K4, z * Y + 1 - y, 2, dev_y).wait_recv()
        right_a(z, go)
        left_a(z, go)

    def steps_a(forward):
        def step(i, carry):
            @pl.when((z - 1 - i >= 0) & ((z < Z - 1) if forward else (z == Z - 1)))
            def _():
                s = z - 1 - i
                remote_a(s, 0, dev_z(z - 1)).wait_recv()
                if forward:
                    right_a(s, go)

            @pl.when((z + 1 + i < Z) & ((z > 0) if forward else (z == 0)))
            def _():
                s = z + 1 + i
                remote_a(s, 0, dev_z(z + 1)).wait_recv()
                if forward:
                    left_a(s, go)

            return carry

        lax.fori_loop(0, Z - 1, step, 0)

    def scaled(values, row):
        mean = jnp.sum(values * values, axis=-1, keepdims=True) * (1.0 / width)
        return values * lax.rsqrt(mean + EPSILON) * gains_ref[row : row + 1, :]

    def norm_to(source, row):
        def block(i, carry):
            at = pl.ds(pl.multiple_of(i * 32, 32), 32)
            per_half, per_quarter = half // 32, quarter // 32
            h, b = i // per_half, (i % per_half) // per_quarter
            to = pl.ds(pl.multiple_of(h * quarter + (i % per_quarter) * 32, 32), 32)
            normed[b, to] = scaled(source[at].astype(F32), row).astype(BF16)
            return carry

        lax.fori_loop(0, rows // 32, block, 0)

    def ffn_block(k, b, first):
        weights = ff.at[k]
        n = normed[b]
        gate = jnp.dot(n, weights[:, 0:hc], preferred_element_type=F32)
        up = jnp.dot(n, weights[:, hc : 2 * hc], preferred_element_type=F32)
        h = (gate / (1.0 + jnp.exp(-gate)) * up).astype(BF16)
        part = lax.dot_general(h, weights[:, 2 * hc :], NT, preferred_element_type=F32)
        acc[b] = part if first else acc[b] + part

    def ffn_chunk(k, first):
        def block(b, carry):
            ffn_block(k, b, first)
            return carry

        lax.fori_loop(0, 2, block, 0)

    mine = pl.ds(pl.multiple_of(c * quarter, 16), quarter)
    other = pl.ds(pl.multiple_of((1 - c) * quarter, 16), quarter)

    def core_copy(r, b):
        return pltpu.make_async_remote_copy(
            src_ref=csend.at[r, b], dst_ref=crecv.at[r, b], send_sem=csem.at[0, r, b],
            recv_sem=csem.at[1, r, b], device_id=core_peer, device_id_type=MESH,
        )

    def x_copy(r, b, j):
        return pltpu.make_async_remote_copy(
            src_ref=xsend.at[r, b], dst_ref=xrecv.at[r, b, j], send_sem=xssem.at[r, b, j],
            recv_sem=xrsem.at[r, b, j], device_id=x_peers[j], device_id_type=MESH,
        )

    def res_copy(r, b, core):
        at = pl.ds(pl.multiple_of(core * half + b * quarter, 16), quarter)
        return pltpu.make_async_remote_copy(
            src_ref=res.at[r, at], dst_ref=res.at[r, at], send_sem=rsem.at[0, r, b],
            recv_sem=rsem.at[1, r, b], device_id=core_peer, device_id_type=MESH,
        )

    def reduce(r, compute, source, row, factor):
        def send(b, carry):
            compute(b)
            csend[r, b] = acc[b, other].astype(BF16)
            core_copy(r, b).start()
            core_copy(r, b).wait()
            xsend[r, b] = (
                acc[b, mine].astype(BF16).astype(F32) + crecv[r, b].astype(F32)
            ).astype(BF16)
            for j in range(X - 1):
                x_copy(r, b, j).start()
            return carry

        def receive(b, carry):
            for j in range(X - 1):
                x_copy(r, b, j).wait()

            def block(i, inner_carry):
                at = pl.ds(pl.multiple_of(i * 32, 16), 32)
                full = pl.ds(pl.multiple_of(c * half + b * quarter + i * 32, 16), 32)
                total = xsend[r, b, at].astype(F32)
                for j in range(X - 1):
                    total = total + xrecv[r, b, j, at].astype(F32)
                res[r, full] = (
                    source[full].astype(F32) + factor * scaled(total, row)
                ).astype(BF16)
                return inner_carry

            lax.fori_loop(0, quarter // 32, block, 0)
            res_copy(r, b, c).start()
            return carry

        def finish(b, carry):
            res_copy(r, b, c).wait_send()
            res_copy(r, b, 1 - c).wait_recv()
            return carry

        lax.fori_loop(0, 2, send, 0)
        lax.fori_loop(0, 2, receive, 0)
        lax.fori_loop(0, 2, finish, 0)

    def swapped(v):
        q = [v[j * quarter : (j + 1) * quarter] for j in range(4)]
        return jnp.concatenate([q[0], q[2], q[1], q[3]], axis=0)

    def mixer():
        edge = main + 128
        n = swapped(normed[...].reshape(rows, Dp))
        outer_inner = jnp.dot(n, g3[...], preferred_element_type=F32)
        outer_inner = outer_inner.astype(BF16).astype(F32)
        value_rest = jnp.dot(n, g4[:, 0:edge], preferred_element_type=F32)
        value_rest = value_rest.astype(BF16).astype(F32)
        rest = value_rest[:, main:]
        if rem:
            lane = lax.broadcasted_iota(jnp.int32, rest.shape, 1)
            keep = (lane >= 3 * rem) & (lane < 4 * rem)
            rests = [
                jnp.where(keep, pltpu.roll(rest, (3 - j) * rem, 1), 0.0) for j in range(3)
            ]
        else:
            rests = [jnp.zeros_like(rest)] * 3
        outer = jnp.concatenate([rests[0], outer_inner[:, 0:main]], axis=1)
        inner = jnp.concatenate([rests[1], outer_inner[:, main:]], axis=1)
        value = jnp.concatenate([rests[2], value_rest[:, 0:main]], axis=1)
        gated = inner * value
        token = lax.broadcasted_iota(jnp.int32, gated.shape, 0)
        conv = jnp.zeros_like(gated)
        for j in range(CONV_K):
            back = CONV_K - 1 - j
            moved = gated
            if back:
                moved = jnp.where(token >= back, pltpu.roll(gated, back, 0), 0.0)
            conv = conv + taps_ref[j : j + 1, :] * moved
        hidden[...] = swapped((outer * conv).astype(BF16)).reshape(hidden.shape)

    def mixer_block(b):
        acc[b] = lax.dot_general(hidden[b], g4[:, main:], NT, preferred_element_type=F32)

    def last_chunk(b):
        ffn_block(nff - 1, b, nff == 1)

    def second(b):
        acc[b] = jnp.zeros(acc.shape[1:], F32)

        def again(k, carry):
            ffn_block(k, b, False)
            return carry

        lax.fori_loop(0, nff, again, 0)

    for k in range(nff + 2):
        for owner, copy in local:
            if owner == k:
                copy.wait()
        if k < 2:
            own(k)
    norm_to(stream_ref, 0)
    for k in range(nff):
        zsteps(k)
        if k + 2 <= K3:
            own(k + 2)
        if k + 2 == K3:
            across(K4, z, go)
        if k > 0:
            wait_across(k - 1)
            ffn_chunk(k - 1, k == 1)
    zsteps(K3)
    start_a()
    steps_a(True)
    wait_across(nff - 1)
    reduce(0, last_chunk, stream_ref, 1, 0.5)
    norm_to(res.at[0], 2)
    wait_across(K3)
    steps_a(False)
    mixer()
    reduce(1, mixer_block, res.at[0], 3, 1.0)
    norm_to(res.at[1], 4)
    reduce(2, second, res.at[1], 5, 0.5)
    out_ref[...] = res[2]

    def done(copy):
        copy.wait_send()

    for k in range(nff + 1):
        def drain(s, carry):
            @pl.when(s <= z)
            def _():
                right(k, s, done)

            @pl.when(s >= z)
            def _():
                left(k, s, done)

            across(k, s, done)
            return carry

        lax.fori_loop(0, Z, drain, 0)
    across(K4, z, done)

    def drain_a(s, carry):
        @pl.when(s <= z)
        def _():
            right_a(s, done)

        @pl.when(s >= z)
        def _():
            left_a(s, done)

        return carry

    lax.fori_loop(0, Z, drain_a, 0)


def stream_kernel(cfg, *refs):
    Z, shard, part, width, hc, nff, main, rem, grp = cfg
    own_refs = refs[:7]
    stream_ref, gains_ref, taps_ref, out_ref = refs[7:11]
    (ff, g3, gv, gb, pr, edge, xt, gtmp, gcol, gains, tbuf, normed, hid, mixed,
     part_buf, crecv, xsend, xrecv, tot, res,
     lsem, zsend, recv, psend, precv, pysend, pyrecv, csem, xsem, tsem, osem) = refs[11:]
    Y = 2
    n_fs = Z * Y
    rows = normed.shape[0]
    Dp = n_fs * shard
    groups = 128 // 32
    pair = Y * shard
    last, K3, KB = nff - 1, nff, nff + 1
    f, t = lax.axis_index("fs"), lax.axis_index("tp")
    z, y = f // Y, f % Y
    c, x = t % 2, t // 2
    core_peer = (f, x * 2 + 1 - c)
    x_peer = (f, (1 - x) * 2 + c)
    dev_y = (z * Y + (1 - y), t)

    def dev_z(zz):
        return (zz * Y + y, t)

    own_row = pl.multiple_of(f * shard, 16)
    here = pl.ds(own_row, part)
    lead = pl.ds(0, main)
    gate, up, down, ow, iw, vw, mw = own_refs
    moves = []
    for k in range(nff):
        for j, w in enumerate((gate, up, down)):
            moves.append((k, w.at[:, pl.ds(k * hc, hc)], ff.at[k, here, pl.ds(j * hc, hc)]))
    moves.append((K3, ow.at[:, lead], g3.at[here, lead]))
    moves.append((K3, iw.at[:, lead], g3.at[here, pl.ds(main, main)]))
    moves.append((K3, vw.at[:, lead], gv.at[here, lead]))
    moves.append((K3, mw.at[:, lead], gb.at[here, :]))
    for j, w in enumerate((ow, iw, vw, mw)):
        moves.append((nff + 1, w, edge.at[j]))
    for s in range(n_fs):
        moves.append((nff + 2, stream_ref.at[pl.ds(s * part, part)], xt.at[pl.ds(s * shard, part)]))
    local = [
        (k, pltpu.make_async_copy(src, dst, lsem.at[n])) for n, (k, src, dst) in enumerate(moves)
    ]

    for s in range(n_fs):
        tail = pl.ds(s * shard + shard - 16, 16)
        for k in range(nff):
            ff[k, tail] = jnp.zeros((16, 3 * hc), BF16)
        g3[tail] = jnp.zeros((16, 2 * main), BF16)
        gv[tail] = jnp.zeros((16, main + 128), BF16)
        gb[tail] = jnp.zeros((16, main), BF16)
        xt[tail] = jnp.zeros((16, rows), BF16)

    barrier = pltpu.get_barrier_semaphore()

    def greet(d):
        pl.semaphore_signal(barrier, inc=1, device_id=d, device_id_type=MESH)

    for d in (core_peer, x_peer, dev_y):
        greet(d)

    @pl.when(z > 0)
    def _():
        greet(dev_z(z - 1))

    @pl.when(z < Z - 1)
    def _():
        greet(dev_z(z + 1))

    for _, copy in local:
        copy.start()
    peers = 3 + (z > 0).astype(jnp.int32) + (z < Z - 1).astype(jnp.int32)
    pl.semaphore_wait(barrier, peers)

    def local_wait(k):
        for owner, copy in local:
            if owner == k:
                copy.wait()

    def remote(k, s, way, d):
        at = pl.ds(pl.multiple_of(s * shard, 16), part)
        if k < last:
            ref = ff.at[k, at]
        elif k == last:
            ref = ff.at[k, at, 0 : 2 * hc]
        else:
            ref = (g3 if k == K3 else gb).at[at]
        return pltpu.make_async_remote_copy(
            src_ref=ref, dst_ref=ref, send_sem=zsend.at[k, way, s], recv_sem=recv.at[k, s],
            device_id=d, device_id_type=MESH,
        )

    def right(k, s, act):
        @pl.when(z < Z - 1)
        def _():
            act(remote(k, s * Y + y, 0, dev_z(z + 1)))

    def left(k, s, act):
        @pl.when(z > 0)
        def _():
            act(remote(k, s * Y + y, 1, dev_z(z - 1)))

    def across(k, s, act):
        act(remote(k, s * Y + y, 2, dev_y))

    def go(copy):
        copy.start()

    def own_z(k):
        right(k, z, go)
        left(k, z, go)

    def own_y(k):
        across(k, z, go)

    at_end = (z == 0) | (z == Z - 1)

    def zsteps(k):
        def step(i, carry):
            @pl.when(z - 1 - i >= 0)
            def _():
                s = z - 1 - i
                remote(k, s * Y + y, 0, dev_z(z - 1)).wait_recv()
                right(k, s, go)
                across(k, s, go)

            @pl.when(z + 1 + i < Z)
            def _():
                s = z + 1 + i
                remote(k, s * Y + y, 0, dev_z(z + 1)).wait_recv()
                left(k, s, go)
                across(k, s, go)

            return carry

        lax.fori_loop(0, Z - 1, step, 0)

    def wait_across(k):
        def step(s, carry):
            remote(k, s * Y + 1 - y, 2, dev_y).wait_recv()
            return carry

        lax.fori_loop(0, Z, step, 0)

    def piece(q, first, count):
        if q == 2:
            return pr.at[pl.ds(pl.multiple_of(first * grp, 16), count * grp)]
        at = pl.ds(pl.multiple_of(first * shard, 16), (count - 1) * shard + part)
        return gv.at[at, lead] if q == 1 else ff.at[last, at, 2 * hc : 3 * hc]

    def across_p(q, s):
        ref = piece(q, s, 1)
        return pltpu.make_async_remote_copy(
            src_ref=ref, dst_ref=ref, send_sem=pysend.at[q], recv_sem=pyrecv.at[q],
            device_id=dev_y, device_id_type=MESH,
        )

    def remote_p(q, s, way, d):
        ref = piece(q, s * Y, Y)
        return pltpu.make_async_remote_copy(
            src_ref=ref, dst_ref=ref, send_sem=psend.at[q, way, s], recv_sem=precv.at[q, s],
            device_id=d, device_id_type=MESH,
        )

    def right_p(q, s, act):
        @pl.when(z < Z - 1)
        def _():
            act(remote_p(q, s, 0, dev_z(z + 1)))

    def left_p(q, s, act):
        @pl.when(z > 0)
        def _():
            act(remote_p(q, s, 1, dev_z(z - 1)))

    def start_p(q):
        across_p(q, z * Y + 1 - y).wait_recv()
        right_p(q, z, go)
        left_p(q, z, go)

    def steps_p(qs, forward):
        def step(i, carry):
            @pl.when((z - 1 - i >= 0) & ((z < Z - 1) if forward else (z == Z - 1)))
            def _():
                s = z - 1 - i
                for q in qs:
                    remote_p(q, s, 0, dev_z(z - 1)).wait_recv()
                    if forward:
                        right_p(q, s, go)

            @pl.when((z + 1 + i < Z) & ((z > 0) if forward else (z == 0)))
            def _():
                s = z + 1 + i
                for q in qs:
                    remote_p(q, s, 0, dev_z(z + 1)).wait_recv()
                    if forward:
                        left_p(q, s, go)

            return carry

        lax.fori_loop(0, Z - 1, step, 0)

    def pack_edges():
        packed = jnp.zeros((grp, 128), F32)
        for j in range(groups):
            count = min(grp, part - j * grp)
            if count <= 0:
                continue
            block = jnp.zeros((count, 128), F32)
            row = lax.broadcasted_iota(jnp.int32, (rem, 128), 0)
            lane = lax.broadcasted_iota(jnp.int32, (rem, 128), 1)
            for k in range(4):
                place = jnp.where(lane == row + (32 * j + rem * k), 1.0, 0.0).astype(BF16)
                source = edge[k, j * grp : j * grp + count, main : main + rem]
                block = block + jnp.dot(source, place, preferred_element_type=F32)
            if count < grp:
                block = jnp.concatenate([block, jnp.zeros((grp - count, 128), F32)], axis=0)
            packed = packed + block
        pr[pl.ds(pl.multiple_of(f * grp, 16), grp)] = packed.astype(BF16)

    def unpack_edges():
        row = lax.broadcasted_iota(jnp.int32, (128, 128), 0)
        lane = lax.broadcasted_iota(jnp.int32, (128, 128), 1)

        def body(s, carry):
            packed = pr[pl.ds(pl.multiple_of(s * grp, 16), grp)]
            for j in range(groups):
                count = min(grp, shard - j * grp)
                if count <= 0:
                    continue
                pick = jnp.where((lane < 32) & (row == lane + 32 * j), 1.0, 0.0).astype(BF16)
                block = jnp.dot(packed, pick, preferred_element_type=F32)[:count]
                at = pl.ds(pl.multiple_of(s * shard + j * grp, 16), count)
                gv[at, main : main + 128] = block.astype(BF16)
            return carry

        lax.fori_loop(0, n_fs, body, 0)

    def prepare_gains():
        gtmp[...] = jnp.zeros(gtmp.shape, F32)
        gtmp[0:6, 0:width] = gains_ref[...]
        for i in range(gtmp.shape[1] // 128):
            gcol[i * 128 : (i + 1) * 128] = gtmp[:, i * 128 : (i + 1) * 128].T

        def body(s, carry):
            for j in range(6):
                column = gcol[pl.ds(pl.multiple_of(s * part, 8), part), j : j + 1]
                at = pl.ds(pl.multiple_of(s * shard, 16), part)
                gains[j, at] = jnp.broadcast_to(column, (part, 128))
                pad = pl.ds(pl.multiple_of(s * shard + part, 8), shard - part)
                gains[j, pad] = jnp.zeros((shard - part, 128), F32)
            return carry

        lax.fori_loop(0, n_fs, body, 0)

    def prepare_taps():
        n_tp = lax.axis_size("tp")
        channels = taps_ref.shape[1] // n_tp
        lanes = tbuf.shape[1]
        tbuf[...] = jnp.zeros(tbuf.shape, F32)
        tbuf[0:CONV_K, 0 : taps_ref.shape[1]] = taps_ref[...].astype(F32)
        full = tbuf[...]
        mine = full
        for i in range(1, n_tp):
            mine = jnp.where(t == i, pltpu.roll(full, lanes - channels * i, 1), mine)
        tbuf[:, 0:main] = mine[:, 0:main]
        rest = pltpu.roll(mine[:, main : main + 128], 3 * rem, 1)
        lane = lax.broadcasted_iota(jnp.int32, rest.shape, 1)
        tbuf[:, main : main + 128] = jnp.where((lane >= 3 * rem) & (lane < 4 * rem), rest, 0.0)

    BLK = 128
    nblk = Dp // BLK

    def squares(v):
        return jnp.sum((v * v).reshape(BLK // 8, 8, rows), axis=0)

    def block_at(i):
        return pl.ds(pl.multiple_of(i * BLK, BLK), BLK)

    def inverse(sums):
        return lax.rsqrt(jnp.sum(sums, axis=0, keepdims=True) * (1.0 / width) + EPSILON)

    def gain_block(row, at):
        g = gains[row, at]
        return jnp.concatenate([g] * (rows // 128), axis=1)

    def sum_squares(source):
        def body(i, sums):
            return sums + squares(source[block_at(i)].astype(F32))

        return lax.fori_loop(0, nblk, body, jnp.zeros((8, rows), F32))

    def norm_to(source, sums, row):
        scale = inverse(sums)

        def body(i, carry):
            at = block_at(i)
            v = source[at].astype(F32) * scale * gain_block(row, at)
            normed[:, at] = v.T.astype(BF16)
            return carry

        lax.fori_loop(0, nblk, body, 0)

    def update(r, source, row, factor):
        scale = inverse(sum_squares(tot.at[r])) * factor

        def body(i, sums):
            at = block_at(i)
            v = source[at].astype(F32) + tot[r, at].astype(F32) * scale * gain_block(row, at)
            v = v.astype(BF16)
            res[r, at] = v
            return sums + squares(v.astype(F32))

        return lax.fori_loop(0, nblk, body, jnp.zeros((8, rows), F32))

    def hidden(k):
        n = normed[...]
        gate_v = jnp.dot(n, ff[k, :, 0:hc], preferred_element_type=F32)
        up_v = jnp.dot(n, ff[k, :, hc : 2 * hc], preferred_element_type=F32)
        hid[k] = (gate_v / (1.0 + jnp.exp(-gate_v)) * up_v).astype(BF16)

    def pair_at(j):
        return pl.ds(pl.multiple_of(j * pair, 16), pair)

    def ffn_pair(r, j):
        at = pair_at(j)
        total = lax.dot_general(ff[0, at, 2 * hc :], hid[0], NT, preferred_element_type=F32)
        for k in range(1, nff):
            total = total + lax.dot_general(
                ff[k, at, 2 * hc :], hid[k], NT, preferred_element_type=F32
            )
        part_buf[r, j] = total.astype(BF16)

    def mixer_pair(r, j):
        remote(KB, j * Y + 1 - y, 2, dev_y).wait_recv()
        at = pair_at(j)
        total = lax.dot_general(gb[at], mixed[:, 0:main], NT, preferred_element_type=F32)
        total = total + lax.dot_general(
            gv[at, main : main + 128], mixed[:, main:], NT, preferred_element_type=F32
        )
        part_buf[r, j] = total.astype(BF16)

    mine = pl.ds(pl.multiple_of(c * shard, 16), shard)
    other = pl.ds(pl.multiple_of((1 - c) * shard, 16), shard)

    def core_copy(r, j):
        return pltpu.make_async_remote_copy(
            src_ref=part_buf.at[r, j, other], dst_ref=crecv.at[r, j], send_sem=csem.at[0, r, j],
            recv_sem=csem.at[1, r, j], device_id=core_peer, device_id_type=MESH,
        )

    def x_copy(r, j):
        return pltpu.make_async_remote_copy(
            src_ref=xsend.at[r, j], dst_ref=xrecv.at[r, j], send_sem=xsem.at[0, r, j],
            recv_sem=xsem.at[1, r, j], device_id=x_peer, device_id_type=MESH,
        )

    def tot_copy(r, j):
        at = pl.ds(pl.multiple_of(j * pair + c * shard, 16), shard)
        return pltpu.make_async_remote_copy(
            src_ref=tot.at[r, at], dst_ref=tot.at[r, at], send_sem=tsem.at[0, r, j],
            recv_sem=tsem.at[1, r, j], device_id=core_peer, device_id_type=MESH,
        )

    near = jnp.minimum(z, Z - 1 - z)
    low = z <= Z - 1 - z

    def order(s):
        step = (s + 1) // 2
        close = jnp.where(s % 2 == 1, z - step, z + step)
        return jnp.where(s <= 2 * near, close, jnp.where(low, s, Z - 1 - s))

    def pass_on(j):
        remote(KB, j * Y + y, 0, dev_z(jnp.where(z == 0, z + 1, z - 1))).wait_recv()
        across(KB, j, go)

    def reduce(r, compute):
        def cross(j):
            core_copy(r, j).wait_recv()
            xsend[r, j] = (
                part_buf[r, j, mine].astype(F32) + crecv[r, j].astype(F32)
            ).astype(BF16)
            x_copy(r, j).start()

        def send(s, carry):
            j = order(s)
            if r == 1:
                @pl.when(at_end & (s < Z - 1))
                def _():
                    pass_on(order(s + 1))

            compute(r, j)
            core_copy(r, j).start()

            @pl.when(s > 0)
            def _():
                cross(order(s - 1))

            return carry

        def receive(s, carry):
            j = order(s)
            x_copy(r, j).wait_recv()
            at = pl.ds(pl.multiple_of(j * pair + c * shard, 16), shard)
            tot[r, at] = (xsend[r, j].astype(F32) + xrecv[r, j].astype(F32)).astype(BF16)
            tot_copy(r, j).start()
            return carry

        def finish(s, carry):
            tot_copy(r, order(s)).wait_recv()
            return carry

        lax.fori_loop(0, Z, send, 0)
        cross(order(Z - 1))
        lax.fori_loop(0, Z, receive, 0)
        lax.fori_loop(0, Z, finish, 0)

    def mixer():
        n = normed[...]
        outer_inner = jnp.dot(n, g3[...], preferred_element_type=F32)
        outer_inner = outer_inner.astype(BF16).astype(F32)
        value_rest = jnp.dot(n, gv[...], preferred_element_type=F32)
        value_rest = value_rest.astype(BF16).astype(F32)
        rest = value_rest[:, main:]
        lane = lax.broadcasted_iota(jnp.int32, rest.shape, 1)
        keep = (lane >= 3 * rem) & (lane < 4 * rem)
        rests = [jnp.where(keep, pltpu.roll(rest, (3 - j) * rem, 1), 0.0) for j in range(3)]
        parts = [
            (outer_inner[:, 0:main], outer_inner[:, main:], value_rest[:, 0:main], 0),
            (rests[0], rests[1], rests[2], main),
        ]
        for outer, inner, value, first in parts:
            lanes = outer.shape[1]
            gated = inner * value
            token = lax.broadcasted_iota(jnp.int32, gated.shape, 0)
            conv = jnp.zeros_like(gated)
            for j in range(CONV_K):
                back = CONV_K - 1 - j
                moved = gated
                if back:
                    moved = jnp.where(token >= back, pltpu.roll(gated, back, 0), 0.0)
                conv = conv + tbuf[j : j + 1, first : first + lanes] * moved
            mixed[:, first : first + lanes] = (outer * conv).astype(BF16)

    for k in range(2):
        local_wait(k)
        own_z(k)
        own_y(k)
    local_wait(nff + 1)
    pack_edges()
    for k in range(2, nff + 1):
        local_wait(k)
    for q in range(3):
        across_p(q, f).start()

    @pl.when(at_end)
    def _():
        for k in range(2, KB + 1):
            own_z(k)

    local_wait(nff + 2)
    prepare_gains()
    prepare_taps()
    norm_to(xt, sum_squares(xt), 0)
    zsteps(0)

    @pl.when(at_end)
    def _():
        for q in range(3):
            start_p(q)

    @pl.when(~at_end)
    def _():
        own_z(2)

    own_y(2)
    for k in range(1, last):
        zsteps(k)
        wait_across(k - 1)
        hidden(k - 1)
    zsteps(last)

    @pl.when(~at_end)
    def _():
        start_p(0)
        steps_p((0,), True)
        own_z(K3)

    own_y(K3)
    wait_across(last - 1)
    hidden(last - 1)
    zsteps(K3)

    @pl.when(~at_end)
    def _():
        start_p(1)
        start_p(2)
        steps_p((1, 2), True)
        own_z(KB)

    own_y(KB)

    @pl.when(~at_end)
    def _():
        zsteps(KB)

    wait_across(last)
    steps_p((0,), False)
    hidden(last)
    reduce(0, ffn_pair)
    norm_to(res.at[0], update(0, xt, 1, 0.5), 2)
    wait_across(K3)
    steps_p((1, 2), False)
    unpack_edges()
    mixer()
    reduce(1, mixer_pair)
    norm_to(res.at[1], update(1, res.at[0], 3, 1.0), 4)

    def again(k, carry):
        hidden(k)
        return carry

    lax.fori_loop(0, nff, again, 0)
    reduce(2, ffn_pair)
    update(2, res.at[1], 5, 0.5)
    outs = [
        pltpu.make_async_copy(
            res.at[2, pl.ds(s * shard, part)], out_ref.at[pl.ds(s * part, part)], osem.at[s]
        )
        for s in range(n_fs)
    ]
    for copy in outs:
        copy.start()

    def done(copy):
        copy.wait_send()

    for k in range(nff + 2):
        def drain(s, carry):
            @pl.when(s <= z)
            def _():
                right(k, s, done)

            @pl.when(s >= z)
            def _():
                left(k, s, done)

            across(k, s, done)
            return carry

        lax.fori_loop(0, Z, drain, 0)
    for q in range(3):
        across_p(q, f).wait_send()

        def drain_p(s, carry):
            @pl.when(s <= z)
            def _():
                right_p(q, s, done)

            @pl.when(s >= z)
            def _():
                left_p(q, s, done)

            return carry

        lax.fori_loop(0, Z, drain_p, 0)

    for r in range(3):
        def drain_r(s, carry):
            core_copy(r, s).wait_send()
            x_copy(r, s).wait_send()
            tot_copy(r, s).wait_send()
            return carry

        lax.fori_loop(0, Z, drain_r, 0)
    for copy in outs:
        copy.wait()


def stream_form(mesh, Z):
    def local(stream_in, norm_gains, gate, up, down, outer_w, inner_w, value_w, mixer_w, conv_taps):
        rows, width = stream_in.shape
        part, hid = gate.shape
        channels = outer_w.shape[1]
        n_fs = 2 * Z
        shard = -(-part // 16) * 16
        Dp = n_fs * shard
        nff = 3
        hc = hid // nff
        main = channels // 128 * 128
        rem = channels - main
        grp = -(-part // 64) * 16
        lanes = -(-width // 128) * 128
        taps = -(-conv_taps.shape[1] // 128) * 128
        dma, vmem = pltpu.SemaphoreType.DMA, pltpu.VMEM
        out = pl.pallas_call(
            functools.partial(stream_kernel, (Z, shard, part, width, hc, nff, main, rem, grp)),
            out_shape=jax.ShapeDtypeStruct((width, rows), BF16),
            in_specs=[pl.BlockSpec(memory_space=pl.ANY)] * 8
            + [pl.BlockSpec(memory_space=pltpu.VMEM)] * 2,
            out_specs=pl.BlockSpec(memory_space=pl.ANY),
            scratch_shapes=[
                vmem((nff, Dp, 3 * hc), BF16),
                vmem((Dp, 2 * main), BF16),
                vmem((Dp, main + 128), BF16),
                vmem((Dp, main), BF16),
                vmem((n_fs * grp, 128), BF16),
                vmem((4, part, channels), BF16),
                vmem((Dp, rows), BF16),
                vmem((128, lanes), F32),
                vmem((lanes, 128), F32),
                vmem((6, Dp, 128), F32),
                vmem((8, taps), F32),
                vmem((rows, Dp), BF16),
                vmem((nff, rows, hc), BF16),
                vmem((rows, main + 128), BF16),
                vmem((3, Z, 2 * shard, rows), BF16),
                vmem((3, Z, shard, rows), BF16),
                vmem((3, Z, shard, rows), BF16),
                vmem((3, Z, shard, rows), BF16),
                vmem((3, Dp, rows), BF16),
                vmem((3, Dp, rows), BF16),
                dma((3 * nff + 8 + n_fs,)),
                dma((nff + 2, 3, n_fs)),
                dma((nff + 2, n_fs)),
                dma((3, 2, Z)),
                dma((3, Z)),
                dma((3,)),
                dma((3,)),
                dma((2, 3, Z)),
                dma((2, 3, Z)),
                dma((2, 3, Z)),
                dma((n_fs,)),
            ],
            compiler_params=pltpu.CompilerParams(
                collective_id=0, has_side_effects=True, vmem_limit_bytes=60 * 1024 * 1024
            ),
        )(gate, up, down, outer_w, inner_w, value_w, mixer_w, stream_in.T, norm_gains, conv_taps)
        return out.T

    return local


def y_count(mesh):
    try:
        found = len({d.coords[1] for d in mesh.devices.reshape(-1)})
    except AttributeError:
        found = 1
    return found if found == 2 and mesh.shape["fs"] % 2 == 0 else 1


def solution(mesh):
    n_fs, n_tp = mesh.shape["fs"], mesh.shape["tp"]
    Y = y_count(mesh)
    Z, X = n_fs // Y, n_tp // 2

    def chain_form(stream_in, norm_gains, gate, up, down, outer_w, inner_w, value_w, mixer_w, conv_taps):
        rows, width = stream_in.shape
        part, hid = gate.shape
        channels = outer_w.shape[1]
        shard = -(-part // 16) * 16
        Dp = n_fs * shard
        nff = 3 if hid % 384 == 0 else 1
        hc = hid // nff
        main = channels // 128 * 128
        rem = channels - main

        def widen(v):
            lead = v.shape[0]
            v = v.reshape(lead, n_fs, part)
            return jnp.pad(v, ((0, 0), (0, 0), (0, shard - part))).reshape(lead, Dp)

        sent = -(-part // 8) * 8

        def pack(w):
            return w if sent == part else jnp.pad(w, ((0, sent - part), (0, 0)))

        rest = [w[:, main:] for w in (outer_w, inner_w, value_w, mixer_w)]
        rest.append(jnp.zeros((part, 128 - 4 * rem), BF16))
        owns = [gate, up, down, outer_w, inner_w, value_w, mixer_w]
        owns = [pack(w) for w in owns + [jnp.concatenate(rest, axis=1)]]
        taps = lax.dynamic_slice_in_dim(
            conv_taps, lax.axis_index("tp") * channels, channels, 1
        ).astype(F32)
        taps = jnp.concatenate(
            [jnp.pad(taps[:, main:], ((0, 0), (3 * rem, 128 - 4 * rem))), taps[:, :main]], axis=1
        )
        half, quarter = rows // 2, rows // 4
        dma, vmem = pltpu.SemaphoreType.DMA, pltpu.VMEM
        out = pl.pallas_call(
            functools.partial(kernel, (Z, Y, X, shard, sent, width, hc, nff, main, rem)),
            out_shape=jax.ShapeDtypeStruct((rows, Dp), BF16),
            in_specs=[pl.BlockSpec(memory_space=pl.ANY)] * 8
            + [pl.BlockSpec(memory_space=pltpu.VMEM)] * 3,
            out_specs=pl.BlockSpec(memory_space=pltpu.VMEM),
            scratch_shapes=[
                vmem((nff, Dp, 3 * hc), BF16),
                vmem((Dp, 2 * main), BF16),
                vmem((Dp, 2 * main + 128), BF16),
                vmem((2, half, Dp), BF16),
                vmem((2, half, Dp), F32),
                vmem((2, half, main + 128), BF16),
                vmem((3, 2, quarter, Dp), BF16),
                vmem((3, 2, quarter, Dp), BF16),
                vmem((3, 2, quarter, Dp), BF16),
                vmem((3, 2, X - 1, quarter, Dp), BF16),
                vmem((3, rows, Dp), BF16),
                dma((3 * nff + 5,)),
                dma((nff + 2, 3, n_fs)),
                dma((nff + 2, n_fs)),
                dma((2, Z)),
                dma((Z,)),
                dma((2, 3, 2)),
                dma((3, 2, X - 1)),
                dma((3, 2, X - 1)),
                dma((2, 3, 2)),
            ],
            compiler_params=pltpu.CompilerParams(
                collective_id=0, has_side_effects=True, vmem_limit_bytes=60 * 1024 * 1024
            ),
        )(*owns, widen(stream_in), widen(norm_gains), taps)
        return out.reshape(rows, n_fs, shard)[:, :, :part].reshape(rows, width)

    def local(*args):
        rows, width = args[0].shape
        part, channels = args[5].shape
        rem = channels % 128
        fits = Y == 2 and X == 2 and part % 8 == 0 and 0 < rem <= 8 and rows % 128 == 0
        fits = fits and (n_fs * (-(-part // 16) * 16)) % 128 == 0 and channels > 128
        fits = fits and args[2].shape[1] % 384 == 0 and Z > 2
        return (stream_form(mesh, Z) if fits else chain_form)(*args)

    return jax.shard_map(
        local,
        mesh=mesh,
        in_specs=(P("fs", None), P()) + (P("fs", "tp"),) * 7 + (P(),),
        out_specs=P("fs", None),
        check_vma=False,
    )
```

```python
import functools

import jax
import jax.numpy as jnp
from jax import lax
from jax.experimental import pallas as pl
from jax.experimental.pallas import tpu as pltpu
from jax.sharding import PartitionSpec as P

MESH = pl.DeviceIdType.MESH
EPSILON = 1e-06
CONV_K = 3
F32, BF16 = jnp.float32, jnp.bfloat16
NT = (((1,), (1,)), ((), ()))


def kernel(cfg, *refs):
    Z, Y, X, shard, sent, width, hc, nff, main, rem = cfg
    own_refs = refs[:8]
    stream_ref, gains_ref, taps_ref, out_ref = refs[8:12]
    (ff, g3, g4, normed, acc, hidden, csend, crecv, xsend, xrecv, res,
     lsem, zsend, recv, asend, arecv, csem, xssem, xrsem, rsem) = refs[12:]
    rows, Dp = stream_ref.shape
    half, quarter = rows // 2, rows // 4
    K3, K4 = nff, nff + 1
    f, t = lax.axis_index("fs"), lax.axis_index("tp")
    z, y = f // Y, f % Y
    c, x = t % 2, t // 2
    core_peer = (f, x * 2 + 1 - c)
    x_peers = [(f, ((x + j) % X) * 2 + c) for j in range(1, X)]

    def dev_z(zz):
        return (zz * Y + y, t)

    dev_y = (z * Y + (Y - 1 - y), t)

    for s in range(Z * Y):
        tail = pl.ds(s * shard + shard - 16, 16)
        for k in range(nff):
            ff[k, tail] = jnp.zeros((16, 3 * hc), BF16)
        g3[tail] = jnp.zeros((16, 2 * main), BF16)
        g4[tail] = jnp.zeros((16, 2 * main + 128), BF16)

    barrier = pltpu.get_barrier_semaphore()

    def greet(d):
        pl.semaphore_signal(barrier, inc=1, device_id=d, device_id_type=MESH)

    always = [core_peer] + x_peers + ([dev_y] if Y == 2 else [])
    for d in always:
        greet(d)
    if Z > 1:
        @pl.when(z > 0)
        def _():
            greet(dev_z(z - 1))

        @pl.when(z < Z - 1)
        def _():
            greet(dev_z(z + 1))

    def slot(k, first, count):
        at = pl.ds(pl.multiple_of(first * shard, 16), (count - 1) * shard + sent)
        if k < nff:
            return ff.at[k, at]
        return (g3 if k == K3 else g4).at[at]

    here = pl.ds(pl.multiple_of(f * shard, 16), sent)
    moves = []
    for k in range(nff):
        for j in range(3):
            moves.append((k, own_refs[j].at[:, pl.ds(k * hc, hc)],
                          ff.at[k, here, pl.ds(j * hc, hc)]))
    ow, iw, vw, mw, rw = own_refs[3:]
    lead = pl.ds(0, main)
    moves.append((K3, ow.at[:, lead], g3.at[here, lead]))
    moves.append((K3, iw.at[:, lead], g3.at[here, pl.ds(main, main)]))
    moves.append((K4, vw.at[:, lead], g4.at[here, lead]))
    moves.append((K4, rw, g4.at[here, pl.ds(main, 128)]))
    moves.append((K4, mw.at[:, lead], g4.at[here, pl.ds(main + 128, main)]))
    local = [
        (k, pltpu.make_async_copy(src, dst, lsem.at[n])) for n, (k, src, dst) in enumerate(moves)
    ]
    for _, copy in local:
        copy.start()

    peers = len(always)
    if Z > 1:
        peers = peers + (z > 0).astype(jnp.int32) + (z < Z - 1).astype(jnp.int32)
    pl.semaphore_wait(barrier, peers)

    def remote(k, s, way, d):
        ref = slot(k, s, 1)
        return pltpu.make_async_remote_copy(
            src_ref=ref, dst_ref=ref, send_sem=zsend.at[k, way, s], recv_sem=recv.at[k, s],
            device_id=d, device_id_type=MESH,
        )

    def remote_a(s, way, d):
        ref = slot(K4, s * Y, Y)
        return pltpu.make_async_remote_copy(
            src_ref=ref, dst_ref=ref, send_sem=asend.at[way, s], recv_sem=arecv.at[s],
            device_id=d, device_id_type=MESH,
        )

    def right(k, s, act):
        @pl.when(z < Z - 1)
        def _():
            act(remote(k, s * Y + y, 0, dev_z(z + 1)))

    def left(k, s, act):
        @pl.when(z > 0)
        def _():
            act(remote(k, s * Y + y, 1, dev_z(z - 1)))

    def across(k, s, act):
        if Y == 2:
            act(remote(k, s * Y + y, 2, dev_y))

    def go(copy):
        copy.start()

    def own(k):
        right(k, z, go)
        left(k, z, go)
        across(k, z, go)

    def zsteps(k):
        def step(i, carry):
            @pl.when(z - 1 - i >= 0)
            def _():
                s = z - 1 - i
                remote(k, s * Y + y, 0, dev_z(z - 1)).wait_recv()
                right(k, s, go)
                across(k, s, go)

            @pl.when(z + 1 + i < Z)
            def _():
                s = z + 1 + i
                remote(k, s * Y + y, 0, dev_z(z + 1)).wait_recv()
                left(k, s, go)
                across(k, s, go)

            return carry

        lax.fori_loop(0, Z - 1, step, 0)

    def wait_across(k):
        if Y == 2:
            def step(s, carry):
                remote(k, s * Y + 1 - y, 2, dev_y).wait_recv()
                return carry

            lax.fori_loop(0, Z, step, 0)

    def right_a(s, act):
        @pl.when(z < Z - 1)
        def _():
            act(remote_a(s, 0, dev_z(z + 1)))

    def left_a(s, act):
        @pl.when(z > 0)
        def _():
            act(remote_a(s, 1, dev_z(z - 1)))

    def start_a():
        if Y == 2:
            remote(K4, z * Y + 1 - y, 2, dev_y).wait_recv()
        right_a(z, go)
        left_a(z, go)

    def steps_a(forward):
        def step(i, carry):
            @pl.when((z - 1 - i >= 0) & ((z < Z - 1) if forward else (z == Z - 1)))
            def _():
                s = z - 1 - i
                remote_a(s, 0, dev_z(z - 1)).wait_recv()
                if forward:
                    right_a(s, go)

            @pl.when((z + 1 + i < Z) & ((z > 0) if forward else (z == 0)))
            def _():
                s = z + 1 + i
                remote_a(s, 0, dev_z(z + 1)).wait_recv()
                if forward:
                    left_a(s, go)

            return carry

        lax.fori_loop(0, Z - 1, step, 0)

    def scaled(values, row):
        mean = jnp.sum(values * values, axis=-1, keepdims=True) * (1.0 / width)
        return values * lax.rsqrt(mean + EPSILON) * gains_ref[row : row + 1, :]

    def norm_to(source, row):
        def block(i, carry):
            at = pl.ds(pl.multiple_of(i * 32, 32), 32)
            per_half, per_quarter = half // 32, quarter // 32
            h, b = i // per_half, (i % per_half) // per_quarter
            to = pl.ds(pl.multiple_of(h * quarter + (i % per_quarter) * 32, 32), 32)
            normed[b, to] = scaled(source[at].astype(F32), row).astype(BF16)
            return carry

        lax.fori_loop(0, rows // 32, block, 0)

    def ffn_block(k, b, first):
        weights = ff.at[k]
        n = normed[b]
        gate = jnp.dot(n, weights[:, 0:hc], preferred_element_type=F32)
        up = jnp.dot(n, weights[:, hc : 2 * hc], preferred_element_type=F32)
        h = (gate / (1.0 + jnp.exp(-gate)) * up).astype(BF16)
        part = lax.dot_general(h, weights[:, 2 * hc :], NT, preferred_element_type=F32)
        acc[b] = part if first else acc[b] + part

    def ffn_chunk(k, first):
        def block(b, carry):
            ffn_block(k, b, first)
            return carry

        lax.fori_loop(0, 2, block, 0)

    mine = pl.ds(pl.multiple_of(c * quarter, 16), quarter)
    other = pl.ds(pl.multiple_of((1 - c) * quarter, 16), quarter)

    def core_copy(r, b):
        return pltpu.make_async_remote_copy(
            src_ref=csend.at[r, b], dst_ref=crecv.at[r, b], send_sem=csem.at[0, r, b],
            recv_sem=csem.at[1, r, b], device_id=core_peer, device_id_type=MESH,
        )

    def x_copy(r, b, j):
        return pltpu.make_async_remote_copy(
            src_ref=xsend.at[r, b], dst_ref=xrecv.at[r, b, j], send_sem=xssem.at[r, b, j],
            recv_sem=xrsem.at[r, b, j], device_id=x_peers[j], device_id_type=MESH,
        )

    def res_copy(r, b, core):
        at = pl.ds(pl.multiple_of(core * half + b * quarter, 16), quarter)
        return pltpu.make_async_remote_copy(
            src_ref=res.at[r, at], dst_ref=res.at[r, at], send_sem=rsem.at[0, r, b],
            recv_sem=rsem.at[1, r, b], device_id=core_peer, device_id_type=MESH,
        )

    def reduce(r, compute, source, row, factor):
        def send(b, carry):
            compute(b)
            csend[r, b] = acc[b, other].astype(BF16)
            core_copy(r, b).start()
            core_copy(r, b).wait()
            xsend[r, b] = (
                acc[b, mine].astype(BF16).astype(F32) + crecv[r, b].astype(F32)
            ).astype(BF16)
            for j in range(X - 1):
                x_copy(r, b, j).start()
            return carry

        def receive(b, carry):
            for j in range(X - 1):
                x_copy(r, b, j).wait()

            def block(i, inner_carry):
                at = pl.ds(pl.multiple_of(i * 32, 16), 32)
                full = pl.ds(pl.multiple_of(c * half + b * quarter + i * 32, 16), 32)
                total = xsend[r, b, at].astype(F32)
                for j in range(X - 1):
                    total = total + xrecv[r, b, j, at].astype(F32)
                res[r, full] = (
                    source[full].astype(F32) + factor * scaled(total, row)
                ).astype(BF16)
                return inner_carry

            lax.fori_loop(0, quarter // 32, block, 0)
            res_copy(r, b, c).start()
            return carry

        def finish(b, carry):
            res_copy(r, b, c).wait_send()
            res_copy(r, b, 1 - c).wait_recv()
            return carry

        lax.fori_loop(0, 2, send, 0)
        lax.fori_loop(0, 2, receive, 0)
        lax.fori_loop(0, 2, finish, 0)

    def swapped(v):
        q = [v[j * quarter : (j + 1) * quarter] for j in range(4)]
        return jnp.concatenate([q[0], q[2], q[1], q[3]], axis=0)

    def mixer():
        edge = main + 128
        n = swapped(normed[...].reshape(rows, Dp))
        outer_inner = jnp.dot(n, g3[...], preferred_element_type=F32)
        outer_inner = outer_inner.astype(BF16).astype(F32)
        value_rest = jnp.dot(n, g4[:, 0:edge], preferred_element_type=F32)
        value_rest = value_rest.astype(BF16).astype(F32)
        rest = value_rest[:, main:]
        if rem:
            lane = lax.broadcasted_iota(jnp.int32, rest.shape, 1)
            keep = (lane >= 3 * rem) & (lane < 4 * rem)
            rests = [
                jnp.where(keep, pltpu.roll(rest, (3 - j) * rem, 1), 0.0) for j in range(3)
            ]
        else:
            rests = [jnp.zeros_like(rest)] * 3
        outer = jnp.concatenate([rests[0], outer_inner[:, 0:main]], axis=1)
        inner = jnp.concatenate([rests[1], outer_inner[:, main:]], axis=1)
        value = jnp.concatenate([rests[2], value_rest[:, 0:main]], axis=1)
        gated = inner * value
        token = lax.broadcasted_iota(jnp.int32, gated.shape, 0)
        conv = jnp.zeros_like(gated)
        for j in range(CONV_K):
            back = CONV_K - 1 - j
            moved = gated
            if back:
                moved = jnp.where(token >= back, pltpu.roll(gated, back, 0), 0.0)
            conv = conv + taps_ref[j : j + 1, :] * moved
        hidden[...] = swapped((outer * conv).astype(BF16)).reshape(hidden.shape)

    def mixer_block(b):
        acc[b] = lax.dot_general(hidden[b], g4[:, main:], NT, preferred_element_type=F32)

    def last_chunk(b):
        ffn_block(nff - 1, b, nff == 1)

    def second(b):
        acc[b] = jnp.zeros(acc.shape[1:], F32)

        def again(k, carry):
            ffn_block(k, b, False)
            return carry

        lax.fori_loop(0, nff, again, 0)

    for k in range(nff + 2):
        for owner, copy in local:
            if owner == k:
                copy.wait()
        if k < 2:
            own(k)
    norm_to(stream_ref, 0)
    for k in range(nff):
        zsteps(k)
        if k + 2 <= K3:
            own(k + 2)
        if k + 2 == K3:
            across(K4, z, go)
        if k > 0:
            wait_across(k - 1)
            ffn_chunk(k - 1, k == 1)
    zsteps(K3)
    start_a()
    steps_a(True)
    wait_across(nff - 1)
    reduce(0, last_chunk, stream_ref, 1, 0.5)
    norm_to(res.at[0], 2)
    wait_across(K3)
    steps_a(False)
    mixer()
    reduce(1, mixer_block, res.at[0], 3, 1.0)
    norm_to(res.at[1], 4)
    reduce(2, second, res.at[1], 5, 0.5)
    out_ref[...] = res[2]

    def done(copy):
        copy.wait_send()

    for k in range(nff + 1):
        def drain(s, carry):
            @pl.when(s <= z)
            def _():
                right(k, s, done)

            @pl.when(s >= z)
            def _():
                left(k, s, done)

            across(k, s, done)
            return carry

        lax.fori_loop(0, Z, drain, 0)
    across(K4, z, done)

    def drain_a(s, carry):
        @pl.when(s <= z)
        def _():
            right_a(s, done)

        @pl.when(s >= z)
        def _():
            left_a(s, done)

        return carry

    lax.fori_loop(0, Z, drain_a, 0)


def stream_kernel(cfg, *refs):
    Z, shard, part, width, hc, nff, main, rem, grp = cfg
    own_refs = refs[:7]
    stream_ref, gains_ref, taps_ref, out_ref = refs[7:11]
    (ff, g3, gv, gb, pr, edge, xt, gtmp, gcol, gains, tbuf, normed, hid, mixed,
     part_buf, crecv, xsend, xrecv, tot, res,
     lsem, zsend, recv, psend, precv, pysend, pyrecv, csem, xsem, tsem, osem) = refs[11:]
    Y = 2
    n_fs = Z * Y
    rows = normed.shape[0]
    Dp = n_fs * shard
    groups = 128 // 32
    pair = Y * shard
    last, K3, KB = nff - 1, nff, nff + 1
    f, t = lax.axis_index("fs"), lax.axis_index("tp")
    z, y = f // Y, f % Y
    c, x = t % 2, t // 2
    core_peer = (f, x * 2 + 1 - c)
    x_peer = (f, (1 - x) * 2 + c)
    dev_y = (z * Y + (1 - y), t)

    def dev_z(zz):
        return (zz * Y + y, t)

    own_row = pl.multiple_of(f * shard, 16)
    here = pl.ds(own_row, part)
    lead = pl.ds(0, main)
    gate, up, down, ow, iw, vw, mw = own_refs
    moves = []
    for k in range(nff):
        for j, w in enumerate((gate, up, down)):
            moves.append((k, w.at[:, pl.ds(k * hc, hc)], ff.at[k, here, pl.ds(j * hc, hc)]))
    moves.append((K3, ow.at[:, lead], g3.at[here, lead]))
    moves.append((K3, iw.at[:, lead], g3.at[here, pl.ds(main, main)]))
    moves.append((K3, vw.at[:, lead], gv.at[here, lead]))
    moves.append((K3, mw.at[:, lead], gb.at[here, :]))
    for j, w in enumerate((ow, iw, vw, mw)):
        moves.append((nff + 1, w, edge.at[j]))
    for s in range(n_fs):
        moves.append((nff + 2, stream_ref.at[pl.ds(s * part, part)], xt.at[pl.ds(s * shard, part)]))
    local = [
        (k, pltpu.make_async_copy(src, dst, lsem.at[n])) for n, (k, src, dst) in enumerate(moves)
    ]

    def clear_pads():
        for s in range(n_fs):
            pad = pl.ds(s * shard + part, shard - part)
            for k in range(nff):
                ff[k, pad] = jnp.zeros((shard - part, 3 * hc), BF16)
            g3[pad] = jnp.zeros((shard - part, 2 * main), BF16)
            gv[pad] = jnp.zeros((shard - part, main + 128), BF16)
            gb[pad] = jnp.zeros((shard - part, main), BF16)
            xt[pad] = jnp.zeros((shard - part, rows), BF16)

    for _, copy in local:
        copy.start()
    clear_pads()
    barrier = pltpu.get_barrier_semaphore()

    def greet(d):
        pl.semaphore_signal(barrier, inc=1, device_id=d, device_id_type=MESH)

    for d in (core_peer, x_peer, dev_y):
        greet(d)

    @pl.when(z > 0)
    def _():
        greet(dev_z(z - 1))

    @pl.when(z < Z - 1)
    def _():
        greet(dev_z(z + 1))

    peers = 3 + (z > 0).astype(jnp.int32) + (z < Z - 1).astype(jnp.int32)
    pl.semaphore_wait(barrier, peers)

    def local_wait(k):
        for owner, copy in local:
            if owner == k:
                copy.wait()

    def remote(k, s, way, d):
        at = pl.ds(pl.multiple_of(s * shard, 16), part)
        if k < last:
            ref = ff.at[k, at]
        elif k == last:
            ref = ff.at[k, at, 0 : 2 * hc]
        else:
            ref = (g3 if k == K3 else gb).at[at]
        return pltpu.make_async_remote_copy(
            src_ref=ref, dst_ref=ref, send_sem=zsend.at[k, way, s], recv_sem=recv.at[k, s],
            device_id=d, device_id_type=MESH,
        )

    def right(k, s, act):
        @pl.when(z < Z - 1)
        def _():
            act(remote(k, s * Y + y, 0, dev_z(z + 1)))

    def left(k, s, act):
        @pl.when(z > 0)
        def _():
            act(remote(k, s * Y + y, 1, dev_z(z - 1)))

    def across(k, s, act):
        act(remote(k, s * Y + y, 2, dev_y))

    def go(copy):
        copy.start()

    near = jnp.minimum(z, Z - 1 - z)
    low = z <= Z - 1 - z
    at_end = (z == 0) | (z == Z - 1)

    def inward(go_right, go_left):
        @pl.when(low)
        def _():
            go_right()

        @pl.when(~low)
        def _():
            go_left()

    def own_in(k):
        inward(lambda: right(k, z, go), lambda: left(k, z, go))

    def own_out(k):
        inward(lambda: left(k, z, go), lambda: right(k, z, go))

    def own_y(k):
        across(k, z, go)

    def zsteps(k):
        def step(i, carry):
            @pl.when(z - 1 - i >= 0)
            def _():
                s = z - 1 - i
                remote(k, s * Y + y, 0, dev_z(z - 1)).wait_recv()
                right(k, s, go)
                across(k, s, go)

            @pl.when(z + 1 + i < Z)
            def _():
                s = z + 1 + i
                remote(k, s * Y + y, 0, dev_z(z + 1)).wait_recv()
                left(k, s, go)
                across(k, s, go)

            return carry

        lax.fori_loop(0, Z - 1, step, 0)

    def wait_across(k):
        def step(s, carry):
            remote(k, s * Y + 1 - y, 2, dev_y).wait_recv()
            return carry

        lax.fori_loop(0, Z, step, 0)

    def piece(q, first, count):
        if q == 2:
            return pr.at[pl.ds(pl.multiple_of(first * grp, 16), count * grp)]
        at = pl.ds(pl.multiple_of(first * shard, 16), (count - 1) * shard + part)
        if q == 3:
            return gb.at[at]
        return gv.at[at, lead] if q == 1 else ff.at[last, at, 2 * hc : 3 * hc]

    def across_p(q, s):
        ref = piece(q, s, 1)
        return pltpu.make_async_remote_copy(
            src_ref=ref, dst_ref=ref, send_sem=pysend.at[q], recv_sem=pyrecv.at[q],
            device_id=dev_y, device_id_type=MESH,
        )

    def remote_p(q, s, way, d):
        ref = piece(q, s * Y, Y)
        return pltpu.make_async_remote_copy(
            src_ref=ref, dst_ref=ref, send_sem=psend.at[q, way, s], recv_sem=precv.at[q, s],
            device_id=d, device_id_type=MESH,
        )

    def right_p(q, s, act):
        @pl.when(z < Z - 1)
        def _():
            act(remote_p(q, s, 0, dev_z(z + 1)))

    def left_p(q, s, act):
        @pl.when(z > 0)
        def _():
            act(remote_p(q, s, 1, dev_z(z - 1)))

    def start_in(q):
        across_p(q, z * Y + 1 - y).wait_recv()
        inward(lambda: right_p(q, z, go), lambda: left_p(q, z, go))

    def start_out(q):
        inward(lambda: left_p(q, z, go), lambda: right_p(q, z, go))

    def steps_p(qs, forward):
        def step(i, carry):
            @pl.when((z - 1 - i >= 0) & ((z < Z - 1) if forward else (z == Z - 1)))
            def _():
                s = z - 1 - i
                for q in qs:
                    remote_p(q, s, 0, dev_z(z - 1)).wait_recv()
                    if forward:
                        right_p(q, s, go)

            @pl.when((z + 1 + i < Z) & ((z > 0) if forward else (z == 0)))
            def _():
                s = z + 1 + i
                for q in qs:
                    remote_p(q, s, 0, dev_z(z + 1)).wait_recv()
                    if forward:
                        left_p(q, s, go)

            return carry

        lax.fori_loop(0, Z - 1, step, 0)

    def inside(s):
        return (s > 0) & (s < Z - 1)

    def steps_b():
        def step(i, carry):
            @pl.when(z - 1 - i >= 0)
            def _():
                s = z - 1 - i

                @pl.when(s > 0)
                def _():
                    remote(KB, s * Y + y, 0, dev_z(z - 1)).wait_recv()
                    right(KB, s, go)
                    across(KB, s, go)

                @pl.when(s == 0)
                def _():
                    remote_p(3, s, 0, dev_z(z - 1)).wait_recv()
                    right_p(3, s, go)

            @pl.when(z + 1 + i < Z)
            def _():
                s = z + 1 + i

                @pl.when(s < Z - 1)
                def _():
                    remote(KB, s * Y + y, 0, dev_z(z + 1)).wait_recv()
                    left(KB, s, go)
                    across(KB, s, go)

                @pl.when(s == Z - 1)
                def _():
                    remote_p(3, s, 0, dev_z(z + 1)).wait_recv()
                    left_p(3, s, go)

            return carry

        lax.fori_loop(0, Z - 1, step, 0)

    def pack_edges():
        packed = jnp.zeros((grp, 128), F32)
        for j in range(groups):
            count = min(grp, part - j * grp)
            if count <= 0:
                continue
            block = jnp.zeros((count, 128), F32)
            row = lax.broadcasted_iota(jnp.int32, (rem, 128), 0)
            lane = lax.broadcasted_iota(jnp.int32, (rem, 128), 1)
            for k in range(4):
                place = jnp.where(lane == row + (32 * j + rem * k), 1.0, 0.0).astype(BF16)
                source = edge[k, j * grp : j * grp + count, main : main + rem]
                block = block + jnp.dot(source, place, preferred_element_type=F32)
            if count < grp:
                block = jnp.concatenate([block, jnp.zeros((grp - count, 128), F32)], axis=0)
            packed = packed + block
        pr[pl.ds(pl.multiple_of(f * grp, 16), grp)] = packed.astype(BF16)

    def unpack_edges():
        row = lax.broadcasted_iota(jnp.int32, (128, 128), 0)
        lane = lax.broadcasted_iota(jnp.int32, (128, 128), 1)

        def body(s, carry):
            packed = pr[pl.ds(pl.multiple_of(s * grp, 16), grp)]
            for j in range(groups):
                count = min(grp, shard - j * grp)
                if count <= 0:
                    continue
                pick = jnp.where((lane < 32) & (row == lane + 32 * j), 1.0, 0.0).astype(BF16)
                block = jnp.dot(packed, pick, preferred_element_type=F32)[:count]
                at = pl.ds(pl.multiple_of(s * shard + j * grp, 16), count)
                gv[at, main : main + 128] = block.astype(BF16)
            return carry

        lax.fori_loop(0, n_fs, body, 0)

    def prepare_gains():
        gtmp[...] = jnp.zeros(gtmp.shape, F32)
        gtmp[0:6, 0:width] = gains_ref[...]
        for i in range(gtmp.shape[1] // 128):
            gcol[i * 128 : (i + 1) * 128] = gtmp[:, i * 128 : (i + 1) * 128].T

        def body(s, carry):
            for j in range(6):
                column = gcol[pl.ds(pl.multiple_of(s * part, 8), part), j : j + 1]
                at = pl.ds(pl.multiple_of(s * shard, 16), part)
                gains[j, at] = jnp.broadcast_to(column, (part, 128))
                pad = pl.ds(pl.multiple_of(s * shard + part, 8), shard - part)
                gains[j, pad] = jnp.zeros((shard - part, 128), F32)
            return carry

        lax.fori_loop(0, n_fs, body, 0)

    def prepare_taps():
        n_tp = lax.axis_size("tp")
        channels = taps_ref.shape[1] // n_tp
        lanes = tbuf.shape[1]
        tbuf[...] = jnp.zeros(tbuf.shape, F32)
        tbuf[0:CONV_K, 0 : taps_ref.shape[1]] = taps_ref[...].astype(F32)
        full = tbuf[...]
        mine = full
        for i in range(1, n_tp):
            mine = jnp.where(t == i, pltpu.roll(full, lanes - channels * i, 1), mine)
        tbuf[:, 0:main] = mine[:, 0:main]
        rest = pltpu.roll(mine[:, main : main + 128], 3 * rem, 1)
        lane = lax.broadcasted_iota(jnp.int32, rest.shape, 1)
        tbuf[:, main : main + 128] = jnp.where((lane >= 3 * rem) & (lane < 4 * rem), rest, 0.0)

    BLK = 128
    nblk = Dp // BLK

    def squares(v):
        return jnp.sum((v * v).reshape(BLK // 8, 8, rows), axis=0)

    def block_at(i):
        return pl.ds(pl.multiple_of(i * BLK, BLK), BLK)

    def inverse(sums):
        return lax.rsqrt(jnp.sum(sums, axis=0, keepdims=True) * (1.0 / width) + EPSILON)

    def gain_block(row, at):
        g = gains[row, at]
        return jnp.concatenate([g] * (rows // 128), axis=1)

    def sum_squares(source):
        def body(i, sums):
            return sums + squares(source[block_at(i)].astype(F32))

        return lax.fori_loop(0, nblk, body, jnp.zeros((8, rows), F32))

    def norm_to(source, sums, row):
        scale = inverse(sums)

        def body(i, carry):
            at = block_at(i)
            v = source[at].astype(F32) * scale * gain_block(row, at)
            normed[:, at] = v.T.astype(BF16)
            return carry

        lax.fori_loop(0, nblk, body, 0)

    def update(r, source, row, factor):
        scale = inverse(sum_squares(tot.at[r])) * factor

        def body(i, sums):
            at = block_at(i)
            v = source[at].astype(F32) + tot[r, at].astype(F32) * scale * gain_block(row, at)
            v = v.astype(BF16)
            res[r, at] = v
            return sums + squares(v.astype(F32))

        return lax.fori_loop(0, nblk, body, jnp.zeros((8, rows), F32))

    def hidden(k):
        n = normed[...]
        gate_v = jnp.dot(n, ff[k, :, 0:hc], preferred_element_type=F32)
        up_v = jnp.dot(n, ff[k, :, hc : 2 * hc], preferred_element_type=F32)
        hid[k] = (gate_v / (1.0 + jnp.exp(-gate_v)) * up_v).astype(BF16)

    def pair_at(j):
        return pl.ds(pl.multiple_of(j * pair, 16), pair)

    def ffn_pair(r, j):
        at = pair_at(j)
        total = lax.dot_general(ff[0, at, 2 * hc :], hid[0], NT, preferred_element_type=F32)
        for k in range(1, nff):
            total = total + lax.dot_general(
                ff[k, at, 2 * hc :], hid[k], NT, preferred_element_type=F32
            )
        part_buf[r, j] = total.astype(BF16)

    def mixer_pair(r, j):
        @pl.when(inside(j))
        def _():
            remote(KB, j * Y + 1 - y, 2, dev_y).wait_recv()

        at = pair_at(j)
        total = lax.dot_general(gb[at], mixed[:, 0:main], NT, preferred_element_type=F32)
        total = total + lax.dot_general(
            gv[at, main : main + 128], mixed[:, main:], NT, preferred_element_type=F32
        )
        part_buf[r, j] = total.astype(BF16)

    mine = pl.ds(pl.multiple_of(c * shard, 16), shard)
    other = pl.ds(pl.multiple_of((1 - c) * shard, 16), shard)

    def core_copy(r, j):
        return pltpu.make_async_remote_copy(
            src_ref=part_buf.at[r, j, other], dst_ref=crecv.at[r, j], send_sem=csem.at[0, r, j],
            recv_sem=csem.at[1, r, j], device_id=core_peer, device_id_type=MESH,
        )

    def x_copy(r, j):
        return pltpu.make_async_remote_copy(
            src_ref=xsend.at[r, j], dst_ref=xrecv.at[r, j], send_sem=xsem.at[0, r, j],
            recv_sem=xsem.at[1, r, j], device_id=x_peer, device_id_type=MESH,
        )

    def tot_copy(r, j):
        at = pl.ds(pl.multiple_of(j * pair + c * shard, 16), shard)
        return pltpu.make_async_remote_copy(
            src_ref=tot.at[r, at], dst_ref=tot.at[r, at], send_sem=tsem.at[0, r, j],
            recv_sem=tsem.at[1, r, j], device_id=core_peer, device_id_type=MESH,
        )

    def order(s):
        step = (s + 1) // 2
        close = jnp.where(s % 2 == 1, z - step, z + step)
        return jnp.where(s <= 2 * near, close, jnp.where(low, s, Z - 1 - s))

    def pass_on(j):
        source = dev_z(jnp.where(z == 0, z + 1, z - 1))

        @pl.when(inside(j))
        def _():
            remote(KB, j * Y + y, 0, source).wait_recv()
            across(KB, j, go)

        @pl.when(~inside(j))
        def _():
            remote_p(3, j, 0, source).wait_recv()

    def end_steps(first, stop):
        source = dev_z(jnp.where(z == 0, z + 1, z - 1))

        def step(s, carry):
            j = order(s)
            remote(K3, j * Y + y, 0, source).wait_recv()
            across(K3, j, go)
            return carry

        @pl.when(at_end)
        def _():
            lax.fori_loop(first, stop, step, 0)

    def reduce(r, compute, hooks):
        def cross(j):
            core_copy(r, j).wait_recv()
            xsend[r, j] = (
                part_buf[r, j, mine].astype(F32) + crecv[r, j].astype(F32)
            ).astype(BF16)
            x_copy(r, j).start()

        def send(s, carry):
            j = order(s)
            if r == 1:
                @pl.when(at_end & (s < Z - 1))
                def _():
                    pass_on(order(s + 1))

            compute(r, j)
            core_copy(r, j).start()

            @pl.when(s > 0)
            def _():
                cross(order(s - 1))

            return carry

        def receive(s, carry):
            j = order(s)
            x_copy(r, j).wait_recv()
            at = pl.ds(pl.multiple_of(j * pair + c * shard, 16), shard)
            tot[r, at] = (xsend[r, j].astype(F32) + xrecv[r, j].astype(F32)).astype(BF16)
            tot_copy(r, j).start()
            return carry

        def finish(s, carry):
            tot_copy(r, order(s)).wait_recv()
            return carry

        lax.fori_loop(0, Z, send, 0)
        cross(order(Z - 1))
        if hooks:
            hooks[0]()
        lax.fori_loop(0, Z // 2, receive, 0)
        if hooks:
            hooks[1]()
        lax.fori_loop(Z // 2, Z, receive, 0)
        lax.fori_loop(0, Z, finish, 0)

    def mixer():
        n = normed[...]
        outer_inner = jnp.dot(n, g3[...], preferred_element_type=F32)
        outer_inner = outer_inner.astype(BF16).astype(F32)
        value_rest = jnp.dot(n, gv[...], preferred_element_type=F32)
        value_rest = value_rest.astype(BF16).astype(F32)
        rest = value_rest[:, main:]
        lane = lax.broadcasted_iota(jnp.int32, rest.shape, 1)
        keep = (lane >= 3 * rem) & (lane < 4 * rem)
        rests = [jnp.where(keep, pltpu.roll(rest, (3 - j) * rem, 1), 0.0) for j in range(3)]
        parts = [
            (outer_inner[:, 0:main], outer_inner[:, main:], value_rest[:, 0:main], 0),
            (rests[0], rests[1], rests[2], main),
        ]
        for outer, inner, value, first in parts:
            lanes = outer.shape[1]
            gated = inner * value
            token = lax.broadcasted_iota(jnp.int32, gated.shape, 0)
            conv = jnp.zeros_like(gated)
            for j in range(CONV_K):
                back = CONV_K - 1 - j
                moved = gated
                if back:
                    moved = jnp.where(token >= back, pltpu.roll(gated, back, 0), 0.0)
                conv = conv + tbuf[j : j + 1, first : first + lanes] * moved
            mixed[:, first : first + lanes] = (outer * conv).astype(BF16)

    for k in range(2):
        local_wait(k)
        own_in(k)
        own_out(k)
        own_y(k)
    local_wait(nff + 1)
    pack_edges()
    for k in range(2, nff + 1):
        local_wait(k)
    for q in range(3):
        across_p(q, f).start()
    @pl.when(at_end)
    def _():
        across_p(3, f).start()
        for k in range(2, K3 + 1):
            own_in(k)

    own_out(2)
    own_y(2)
    local_wait(nff + 2)
    prepare_gains()
    prepare_taps()
    norm_to(xt, sum_squares(xt), 0)
    zsteps(0)

    @pl.when(~at_end)
    def _():
        own_in(2)

    start_in(0)
    start_out(0)

    @pl.when(at_end)
    def _():
        for q in range(1, 4):
            start_in(q)

    zsteps(1)
    own_out(K3)

    @pl.when(~at_end)
    def _():
        own_in(K3)
        start_in(1)
        start_in(2)
        own_in(KB)

    wait_across(0)
    hidden(0)
    zsteps(last)
    steps_p((0,), True)
    own_y(K3)

    @pl.when(~at_end)
    def _():
        zsteps(K3)
        start_out(1)
        start_out(2)
        steps_p((1, 2), True)
        own_out(KB)
        own_y(KB)
        steps_b()

    wait_across(1)
    hidden(1)
    end_steps(1, 2)
    wait_across(last)
    steps_p((0,), False)
    hidden(last)
    reduce(0, ffn_pair, (lambda: end_steps(2, Z - 1), lambda: end_steps(Z - 1, Z)))
    norm_to(res.at[0], update(0, xt, 1, 0.5), 2)
    wait_across(K3)
    steps_p((1, 2), False)
    unpack_edges()
    mixer()
    reduce(1, mixer_pair, None)
    norm_to(res.at[1], update(1, res.at[0], 3, 1.0), 4)

    def again(k, carry):
        hidden(k)
        return carry

    lax.fori_loop(0, nff, again, 0)
    reduce(2, ffn_pair, None)
    update(2, res.at[1], 5, 0.5)
    outs = [
        pltpu.make_async_copy(
            res.at[2, pl.ds(s * shard, part)], out_ref.at[pl.ds(s * part, part)], osem.at[s]
        )
        for s in range(n_fs)
    ]
    for copy in outs:
        copy.start()

    def done(copy):
        copy.wait_send()

    for k in range(nff + 2):
        def drain(s, carry):
            @pl.when(s <= z)
            def _():
                right(k, s, done)

            @pl.when(s >= z)
            def _():
                left(k, s, done)

            across(k, s, done)
            return carry

        lax.fori_loop(*((0, Z) if k < KB else (1, Z - 1)), drain, 0)
    for q in range(4):
        def drain_p(s, carry):
            @pl.when((s <= z) & ((q < 3) | ~inside(s)))
            def _():
                right_p(q, s, done)

            @pl.when((s >= z) & ((q < 3) | ~inside(s)))
            def _():
                left_p(q, s, done)

            return carry

        lax.fori_loop(0, Z, drain_p, 0)
    for q in range(3):
        across_p(q, f).wait_send()

    @pl.when(at_end)
    def _():
        across_p(3, f).wait_send()

    for r in range(3):
        def drain_r(s, carry):
            core_copy(r, s).wait_send()
            x_copy(r, s).wait_send()
            tot_copy(r, s).wait_send()
            return carry

        lax.fori_loop(0, Z, drain_r, 0)
    for copy in outs:
        copy.wait()


def stream_form(mesh, Z):
    def local(stream_in, norm_gains, gate, up, down, outer_w, inner_w, value_w, mixer_w, conv_taps):
        rows, width = stream_in.shape
        part, hid = gate.shape
        channels = outer_w.shape[1]
        n_fs = 2 * Z
        shard = -(-part // 16) * 16
        Dp = n_fs * shard
        nff = 3
        hc = hid // nff
        main = channels // 128 * 128
        rem = channels - main
        grp = -(-part // 64) * 16
        lanes = -(-width // 128) * 128
        taps = -(-conv_taps.shape[1] // 128) * 128
        dma, vmem = pltpu.SemaphoreType.DMA, pltpu.VMEM
        out = pl.pallas_call(
            functools.partial(stream_kernel, (Z, shard, part, width, hc, nff, main, rem, grp)),
            out_shape=jax.ShapeDtypeStruct((width, rows), BF16),
            in_specs=[pl.BlockSpec(memory_space=pl.ANY)] * 8
            + [pl.BlockSpec(memory_space=pltpu.VMEM)] * 2,
            out_specs=pl.BlockSpec(memory_space=pl.ANY),
            scratch_shapes=[
                vmem((nff, Dp, 3 * hc), BF16),
                vmem((Dp, 2 * main), BF16),
                vmem((Dp, main + 128), BF16),
                vmem((Dp, main), BF16),
                vmem((n_fs * grp, 128), BF16),
                vmem((4, part, channels), BF16),
                vmem((Dp, rows), BF16),
                vmem((128, lanes), F32),
                vmem((lanes, 128), F32),
                vmem((6, Dp, 128), F32),
                vmem((8, taps), F32),
                vmem((rows, Dp), BF16),
                vmem((nff, rows, hc), BF16),
                vmem((rows, main + 128), BF16),
                vmem((3, Z, 2 * shard, rows), BF16),
                vmem((3, Z, shard, rows), BF16),
                vmem((3, Z, shard, rows), BF16),
                vmem((3, Z, shard, rows), BF16),
                vmem((3, Dp, rows), BF16),
                vmem((3, Dp, rows), BF16),
                dma((3 * nff + 8 + n_fs,)),
                dma((nff + 2, 3, n_fs)),
                dma((nff + 2, n_fs)),
                dma((4, 2, Z)),
                dma((4, Z)),
                dma((4,)),
                dma((4,)),
                dma((2, 3, Z)),
                dma((2, 3, Z)),
                dma((2, 3, Z)),
                dma((n_fs,)),
            ],
            compiler_params=pltpu.CompilerParams(
                collective_id=0, has_side_effects=True, vmem_limit_bytes=60 * 1024 * 1024
            ),
        )(gate, up, down, outer_w, inner_w, value_w, mixer_w, stream_in.T, norm_gains, conv_taps)
        return out.T

    return local


def y_count(mesh):
    try:
        found = len({d.coords[1] for d in mesh.devices.reshape(-1)})
    except AttributeError:
        found = 1
    return found if found == 2 and mesh.shape["fs"] % 2 == 0 else 1


def solution(mesh):
    n_fs, n_tp = mesh.shape["fs"], mesh.shape["tp"]
    Y = y_count(mesh)
    Z, X = n_fs // Y, n_tp // 2

    def chain_form(stream_in, norm_gains, gate, up, down, outer_w, inner_w, value_w, mixer_w, conv_taps):
        rows, width = stream_in.shape
        part, hid = gate.shape
        channels = outer_w.shape[1]
        shard = -(-part // 16) * 16
        Dp = n_fs * shard
        nff = 3 if hid % 384 == 0 else 1
        hc = hid // nff
        main = channels // 128 * 128
        rem = channels - main

        def widen(v):
            lead = v.shape[0]
            v = v.reshape(lead, n_fs, part)
            return jnp.pad(v, ((0, 0), (0, 0), (0, shard - part))).reshape(lead, Dp)

        sent = -(-part // 8) * 8

        def pack(w):
            return w if sent == part else jnp.pad(w, ((0, sent - part), (0, 0)))

        rest = [w[:, main:] for w in (outer_w, inner_w, value_w, mixer_w)]
        rest.append(jnp.zeros((part, 128 - 4 * rem), BF16))
        owns = [gate, up, down, outer_w, inner_w, value_w, mixer_w]
        owns = [pack(w) for w in owns + [jnp.concatenate(rest, axis=1)]]
        taps = lax.dynamic_slice_in_dim(
            conv_taps, lax.axis_index("tp") * channels, channels, 1
        ).astype(F32)
        taps = jnp.concatenate(
            [jnp.pad(taps[:, main:], ((0, 0), (3 * rem, 128 - 4 * rem))), taps[:, :main]], axis=1
        )
        half, quarter = rows // 2, rows // 4
        dma, vmem = pltpu.SemaphoreType.DMA, pltpu.VMEM
        out = pl.pallas_call(
            functools.partial(kernel, (Z, Y, X, shard, sent, width, hc, nff, main, rem)),
            out_shape=jax.ShapeDtypeStruct((rows, Dp), BF16),
            in_specs=[pl.BlockSpec(memory_space=pl.ANY)] * 8
            + [pl.BlockSpec(memory_space=pltpu.VMEM)] * 3,
            out_specs=pl.BlockSpec(memory_space=pltpu.VMEM),
            scratch_shapes=[
                vmem((nff, Dp, 3 * hc), BF16),
                vmem((Dp, 2 * main), BF16),
                vmem((Dp, 2 * main + 128), BF16),
                vmem((2, half, Dp), BF16),
                vmem((2, half, Dp), F32),
                vmem((2, half, main + 128), BF16),
                vmem((3, 2, quarter, Dp), BF16),
                vmem((3, 2, quarter, Dp), BF16),
                vmem((3, 2, quarter, Dp), BF16),
                vmem((3, 2, X - 1, quarter, Dp), BF16),
                vmem((3, rows, Dp), BF16),
                dma((3 * nff + 5,)),
                dma((nff + 2, 3, n_fs)),
                dma((nff + 2, n_fs)),
                dma((2, Z)),
                dma((Z,)),
                dma((2, 3, 2)),
                dma((3, 2, X - 1)),
                dma((3, 2, X - 1)),
                dma((2, 3, 2)),
            ],
            compiler_params=pltpu.CompilerParams(
                collective_id=0, has_side_effects=True, vmem_limit_bytes=60 * 1024 * 1024
            ),
        )(*owns, widen(stream_in), widen(norm_gains), taps)
        return out.reshape(rows, n_fs, shard)[:, :, :part].reshape(rows, width)

    def local(*args):
        rows, width = args[0].shape
        part, channels = args[5].shape
        rem = channels % 128
        fits = Y == 2 and X == 2 and part % 8 == 0 and 0 < rem <= 8 and rows % 128 == 0
        fits = fits and (n_fs * (-(-part // 16) * 16)) % 128 == 0 and channels > 128
        fits = fits and args[2].shape[1] % 384 == 0 and Z > 2
        return (stream_form(mesh, Z) if fits else chain_form)(*args)

    return jax.shard_map(
        local,
        mesh=mesh,
        in_specs=(P("fs", None), P()) + (P("fs", "tp"),) * 7 + (P(),),
        out_specs=P("fs", None),
        check_vma=False,
    )
```

```python
import functools

import jax
import jax.numpy as jnp
from jax import lax
from jax.experimental import pallas as pl
from jax.experimental.pallas import tpu as pltpu
from jax.sharding import PartitionSpec as P

MESH = pl.DeviceIdType.MESH
EPSILON = 1e-06
CONV_K = 3
F32, BF16 = jnp.float32, jnp.bfloat16
NT = (((1,), (1,)), ((), ()))


def kernel(cfg, *refs):
    Z, Y, X, shard, sent, width, hc, nff, main, rem = cfg
    own_refs = refs[:8]
    stream_ref, gains_ref, taps_ref, out_ref = refs[8:12]
    (ff, g3, g4, normed, acc, hidden, csend, crecv, xsend, xrecv, res,
     lsem, zsend, recv, asend, arecv, csem, xssem, xrsem, rsem) = refs[12:]
    rows, Dp = stream_ref.shape
    half, quarter = rows // 2, rows // 4
    K3, K4 = nff, nff + 1
    f, t = lax.axis_index("fs"), lax.axis_index("tp")
    z, y = f // Y, f % Y
    c, x = t % 2, t // 2
    core_peer = (f, x * 2 + 1 - c)
    x_peers = [(f, ((x + j) % X) * 2 + c) for j in range(1, X)]

    def dev_z(zz):
        return (zz * Y + y, t)

    dev_y = (z * Y + (Y - 1 - y), t)

    for s in range(Z * Y):
        tail = pl.ds(s * shard + shard - 16, 16)
        for k in range(nff):
            ff[k, tail] = jnp.zeros((16, 3 * hc), BF16)
        g3[tail] = jnp.zeros((16, 2 * main), BF16)
        g4[tail] = jnp.zeros((16, 2 * main + 128), BF16)

    barrier = pltpu.get_barrier_semaphore()

    def greet(d):
        pl.semaphore_signal(barrier, inc=1, device_id=d, device_id_type=MESH)

    always = [core_peer] + x_peers + ([dev_y] if Y == 2 else [])
    for d in always:
        greet(d)
    if Z > 1:
        @pl.when(z > 0)
        def _():
            greet(dev_z(z - 1))

        @pl.when(z < Z - 1)
        def _():
            greet(dev_z(z + 1))

    def slot(k, first, count):
        at = pl.ds(pl.multiple_of(first * shard, 16), (count - 1) * shard + sent)
        if k < nff:
            return ff.at[k, at]
        return (g3 if k == K3 else g4).at[at]

    here = pl.ds(pl.multiple_of(f * shard, 16), sent)
    moves = []
    for k in range(nff):
        for j in range(3):
            moves.append((k, own_refs[j].at[:, pl.ds(k * hc, hc)],
                          ff.at[k, here, pl.ds(j * hc, hc)]))
    ow, iw, vw, mw, rw = own_refs[3:]
    lead = pl.ds(0, main)
    moves.append((K3, ow.at[:, lead], g3.at[here, lead]))
    moves.append((K3, iw.at[:, lead], g3.at[here, pl.ds(main, main)]))
    moves.append((K4, vw.at[:, lead], g4.at[here, lead]))
    moves.append((K4, rw, g4.at[here, pl.ds(main, 128)]))
    moves.append((K4, mw.at[:, lead], g4.at[here, pl.ds(main + 128, main)]))
    local = [
        (k, pltpu.make_async_copy(src, dst, lsem.at[n])) for n, (k, src, dst) in enumerate(moves)
    ]
    for _, copy in local:
        copy.start()

    peers = len(always)
    if Z > 1:
        peers = peers + (z > 0).astype(jnp.int32) + (z < Z - 1).astype(jnp.int32)
    pl.semaphore_wait(barrier, peers)

    def remote(k, s, way, d):
        ref = slot(k, s, 1)
        return pltpu.make_async_remote_copy(
            src_ref=ref, dst_ref=ref, send_sem=zsend.at[k, way, s], recv_sem=recv.at[k, s],
            device_id=d, device_id_type=MESH,
        )

    def remote_a(s, way, d):
        ref = slot(K4, s * Y, Y)
        return pltpu.make_async_remote_copy(
            src_ref=ref, dst_ref=ref, send_sem=asend.at[way, s], recv_sem=arecv.at[s],
            device_id=d, device_id_type=MESH,
        )

    def right(k, s, act):
        @pl.when(z < Z - 1)
        def _():
            act(remote(k, s * Y + y, 0, dev_z(z + 1)))

    def left(k, s, act):
        @pl.when(z > 0)
        def _():
            act(remote(k, s * Y + y, 1, dev_z(z - 1)))

    def across(k, s, act):
        if Y == 2:
            act(remote(k, s * Y + y, 2, dev_y))

    def go(copy):
        copy.start()

    def own(k):
        right(k, z, go)
        left(k, z, go)
        across(k, z, go)

    def zsteps(k):
        def step(i, carry):
            @pl.when(z - 1 - i >= 0)
            def _():
                s = z - 1 - i
                remote(k, s * Y + y, 0, dev_z(z - 1)).wait_recv()
                right(k, s, go)
                across(k, s, go)

            @pl.when(z + 1 + i < Z)
            def _():
                s = z + 1 + i
                remote(k, s * Y + y, 0, dev_z(z + 1)).wait_recv()
                left(k, s, go)
                across(k, s, go)

            return carry

        lax.fori_loop(0, Z - 1, step, 0)

    def wait_across(k):
        if Y == 2:
            def step(s, carry):
                remote(k, s * Y + 1 - y, 2, dev_y).wait_recv()
                return carry

            lax.fori_loop(0, Z, step, 0)

    def right_a(s, act):
        @pl.when(z < Z - 1)
        def _():
            act(remote_a(s, 0, dev_z(z + 1)))

    def left_a(s, act):
        @pl.when(z > 0)
        def _():
            act(remote_a(s, 1, dev_z(z - 1)))

    def start_a():
        if Y == 2:
            remote(K4, z * Y + 1 - y, 2, dev_y).wait_recv()
        right_a(z, go)
        left_a(z, go)

    def steps_a(forward):
        def step(i, carry):
            @pl.when((z - 1 - i >= 0) & ((z < Z - 1) if forward else (z == Z - 1)))
            def _():
                s = z - 1 - i
                remote_a(s, 0, dev_z(z - 1)).wait_recv()
                if forward:
                    right_a(s, go)

            @pl.when((z + 1 + i < Z) & ((z > 0) if forward else (z == 0)))
            def _():
                s = z + 1 + i
                remote_a(s, 0, dev_z(z + 1)).wait_recv()
                if forward:
                    left_a(s, go)

            return carry

        lax.fori_loop(0, Z - 1, step, 0)

    def scaled(values, row):
        mean = jnp.sum(values * values, axis=-1, keepdims=True) * (1.0 / width)
        return values * lax.rsqrt(mean + EPSILON) * gains_ref[row : row + 1, :]

    def norm_to(source, row):
        def block(i, carry):
            at = pl.ds(pl.multiple_of(i * 32, 32), 32)
            per_half, per_quarter = half // 32, quarter // 32
            h, b = i // per_half, (i % per_half) // per_quarter
            to = pl.ds(pl.multiple_of(h * quarter + (i % per_quarter) * 32, 32), 32)
            normed[b, to] = scaled(source[at].astype(F32), row).astype(BF16)
            return carry

        lax.fori_loop(0, rows // 32, block, 0)

    def ffn_block(k, b, first):
        weights = ff.at[k]
        n = normed[b]
        gate = jnp.dot(n, weights[:, 0:hc], preferred_element_type=F32)
        up = jnp.dot(n, weights[:, hc : 2 * hc], preferred_element_type=F32)
        h = (gate / (1.0 + jnp.exp(-gate)) * up).astype(BF16)
        part = lax.dot_general(h, weights[:, 2 * hc :], NT, preferred_element_type=F32)
        acc[b] = part if first else acc[b] + part

    def ffn_chunk(k, first):
        def block(b, carry):
            ffn_block(k, b, first)
            return carry

        lax.fori_loop(0, 2, block, 0)

    mine = pl.ds(pl.multiple_of(c * quarter, 16), quarter)
    other = pl.ds(pl.multiple_of((1 - c) * quarter, 16), quarter)

    def core_copy(r, b):
        return pltpu.make_async_remote_copy(
            src_ref=csend.at[r, b], dst_ref=crecv.at[r, b], send_sem=csem.at[0, r, b],
            recv_sem=csem.at[1, r, b], device_id=core_peer, device_id_type=MESH,
        )

    def x_copy(r, b, j):
        return pltpu.make_async_remote_copy(
            src_ref=xsend.at[r, b], dst_ref=xrecv.at[r, b, j], send_sem=xssem.at[r, b, j],
            recv_sem=xrsem.at[r, b, j], device_id=x_peers[j], device_id_type=MESH,
        )

    def res_copy(r, b, core):
        at = pl.ds(pl.multiple_of(core * half + b * quarter, 16), quarter)
        return pltpu.make_async_remote_copy(
            src_ref=res.at[r, at], dst_ref=res.at[r, at], send_sem=rsem.at[0, r, b],
            recv_sem=rsem.at[1, r, b], device_id=core_peer, device_id_type=MESH,
        )

    def reduce(r, compute, source, row, factor):
        def send(b, carry):
            compute(b)
            csend[r, b] = acc[b, other].astype(BF16)
            core_copy(r, b).start()
            core_copy(r, b).wait()
            xsend[r, b] = (
                acc[b, mine].astype(BF16).astype(F32) + crecv[r, b].astype(F32)
            ).astype(BF16)
            for j in range(X - 1):
                x_copy(r, b, j).start()
            return carry

        def receive(b, carry):
            for j in range(X - 1):
                x_copy(r, b, j).wait()

            def block(i, inner_carry):
                at = pl.ds(pl.multiple_of(i * 32, 16), 32)
                full = pl.ds(pl.multiple_of(c * half + b * quarter + i * 32, 16), 32)
                total = xsend[r, b, at].astype(F32)
                for j in range(X - 1):
                    total = total + xrecv[r, b, j, at].astype(F32)
                res[r, full] = (
                    source[full].astype(F32) + factor * scaled(total, row)
                ).astype(BF16)
                return inner_carry

            lax.fori_loop(0, quarter // 32, block, 0)
            res_copy(r, b, c).start()
            return carry

        def finish(b, carry):
            res_copy(r, b, c).wait_send()
            res_copy(r, b, 1 - c).wait_recv()
            return carry

        lax.fori_loop(0, 2, send, 0)
        lax.fori_loop(0, 2, receive, 0)
        lax.fori_loop(0, 2, finish, 0)

    def swapped(v):
        q = [v[j * quarter : (j + 1) * quarter] for j in range(4)]
        return jnp.concatenate([q[0], q[2], q[1], q[3]], axis=0)

    def mixer():
        edge = main + 128
        n = swapped(normed[...].reshape(rows, Dp))
        outer_inner = jnp.dot(n, g3[...], preferred_element_type=F32)
        outer_inner = outer_inner.astype(BF16).astype(F32)
        value_rest = jnp.dot(n, g4[:, 0:edge], preferred_element_type=F32)
        value_rest = value_rest.astype(BF16).astype(F32)
        rest = value_rest[:, main:]
        if rem:
            lane = lax.broadcasted_iota(jnp.int32, rest.shape, 1)
            keep = (lane >= 3 * rem) & (lane < 4 * rem)
            rests = [
                jnp.where(keep, pltpu.roll(rest, (3 - j) * rem, 1), 0.0) for j in range(3)
            ]
        else:
            rests = [jnp.zeros_like(rest)] * 3
        outer = jnp.concatenate([rests[0], outer_inner[:, 0:main]], axis=1)
        inner = jnp.concatenate([rests[1], outer_inner[:, main:]], axis=1)
        value = jnp.concatenate([rests[2], value_rest[:, 0:main]], axis=1)
        gated = inner * value
        token = lax.broadcasted_iota(jnp.int32, gated.shape, 0)
        conv = jnp.zeros_like(gated)
        for j in range(CONV_K):
            back = CONV_K - 1 - j
            moved = gated
            if back:
                moved = jnp.where(token >= back, pltpu.roll(gated, back, 0), 0.0)
            conv = conv + taps_ref[j : j + 1, :] * moved
        hidden[...] = swapped((outer * conv).astype(BF16)).reshape(hidden.shape)

    def mixer_block(b):
        acc[b] = lax.dot_general(hidden[b], g4[:, main:], NT, preferred_element_type=F32)

    def last_chunk(b):
        ffn_block(nff - 1, b, nff == 1)

    def second(b):
        acc[b] = jnp.zeros(acc.shape[1:], F32)

        def again(k, carry):
            ffn_block(k, b, False)
            return carry

        lax.fori_loop(0, nff, again, 0)

    for k in range(nff + 2):
        for owner, copy in local:
            if owner == k:
                copy.wait()
        if k < 2:
            own(k)
    norm_to(stream_ref, 0)
    for k in range(nff):
        zsteps(k)
        if k + 2 <= K3:
            own(k + 2)
        if k + 2 == K3:
            across(K4, z, go)
        if k > 0:
            wait_across(k - 1)
            ffn_chunk(k - 1, k == 1)
    zsteps(K3)
    start_a()
    steps_a(True)
    wait_across(nff - 1)
    reduce(0, last_chunk, stream_ref, 1, 0.5)
    norm_to(res.at[0], 2)
    wait_across(K3)
    steps_a(False)
    mixer()
    reduce(1, mixer_block, res.at[0], 3, 1.0)
    norm_to(res.at[1], 4)
    reduce(2, second, res.at[1], 5, 0.5)
    out_ref[...] = res[2]

    def done(copy):
        copy.wait_send()

    for k in range(nff + 1):
        def drain(s, carry):
            @pl.when(s <= z)
            def _():
                right(k, s, done)

            @pl.when(s >= z)
            def _():
                left(k, s, done)

            across(k, s, done)
            return carry

        lax.fori_loop(0, Z, drain, 0)
    across(K4, z, done)

    def drain_a(s, carry):
        @pl.when(s <= z)
        def _():
            right_a(s, done)

        @pl.when(s >= z)
        def _():
            left_a(s, done)

        return carry

    lax.fori_loop(0, Z, drain_a, 0)


def stream_kernel(cfg, *refs):
    Z, shard, part, width, hc, nff, main, rem, grp = cfg
    own_refs = refs[:7]
    stream_ref, gains_ref, taps_ref, out_ref = refs[7:11]
    (ff, g3, gv, gb, pr, edge, xt, gtmp, gcol, gains, tbuf, normed, hid, mixed,
     part_buf, crecv, xsend, xrecv, tot, res, fd, acc,
     lsem, zsend, recv, psend, precv, pysend, pyrecv, csem, xsem, tsem, osem,
     dsem, hsem) = refs[11:]
    Y = 2
    n_fs = Z * Y
    rows = normed.shape[0]
    Dp = n_fs * shard
    groups = 128 // 32
    pair = Y * shard
    last, K3, KB = nff - 1, nff + 1, nff + 2
    f, t = lax.axis_index("fs"), lax.axis_index("tp")
    z, y = f // Y, f % Y
    c, x = t % 2, t // 2
    core_peer = (f, x * 2 + 1 - c)
    x_peer = (f, (1 - x) * 2 + c)
    x_other = (f, (1 - x) * 2 + 1 - c)
    dev_y = (z * Y + (1 - y), t)

    def dev_z(zz):
        return (zz * Y + y, t)

    own_row = pl.multiple_of(f * shard, 16)
    here = pl.ds(own_row, part)
    lead = pl.ds(0, main)
    gate, up, down, ow, iw, vw, mw = own_refs
    moves = []
    for k in range(nff):
        moves.append((0, down.at[:, pl.ds(k * hc, hc)], ff.at[k, here, pl.ds(2 * hc, hc)]))
    for k in range(nff):
        for j, w in enumerate((gate, up)):
            moves.append((k + 1, w.at[:, pl.ds(k * hc, hc)], ff.at[k, here, pl.ds(j * hc, hc)]))
    moves.append((K3, ow.at[:, lead], g3.at[here, lead]))
    moves.append((K3, iw.at[:, lead], g3.at[here, pl.ds(main, main)]))
    moves.append((K3, vw.at[:, lead], gv.at[here, lead]))
    moves.append((K3, mw.at[:, lead], gb.at[here, :]))
    for j, w in enumerate((ow, iw, vw, mw)):
        moves.append((K3 + 1, w, edge.at[j]))
    for s in range(n_fs):
        moves.append((K3 + 2, stream_ref.at[pl.ds(s * part, part)], xt.at[pl.ds(s * shard, part)]))
    local = [
        (k, pltpu.make_async_copy(src, dst, lsem.at[n])) for n, (k, src, dst) in enumerate(moves)
    ]

    def clear_pads():
        for s in range(n_fs):
            pad = pl.ds(s * shard + part, shard - part)
            for k in range(nff):
                ff[k, pad] = jnp.zeros((shard - part, 3 * hc), BF16)
            g3[pad] = jnp.zeros((shard - part, 2 * main), BF16)
            gv[pad] = jnp.zeros((shard - part, main + 128), BF16)
            gb[pad] = jnp.zeros((shard - part, main), BF16)
            xt[pad] = jnp.zeros((shard - part, rows), BF16)
        for s in range(Z):
            pad = pl.ds(s * shard + part, shard - part)
            for i in range(1, 4):
                for k in range(nff):
                    fd[i, k, pad] = jnp.zeros((shard - part, hc), BF16)

    for _, copy in local:
        copy.start()
    clear_pads()
    barrier = pltpu.get_barrier_semaphore()

    def greet(d):
        pl.semaphore_signal(barrier, inc=1, device_id=d, device_id_type=MESH)

    for d in (core_peer, x_peer, x_other, dev_y):
        greet(d)

    @pl.when(z > 0)
    def _():
        greet(dev_z(z - 1))

    @pl.when(z < Z - 1)
    def _():
        greet(dev_z(z + 1))

    peers = 4 + (z > 0).astype(jnp.int32) + (z < Z - 1).astype(jnp.int32)
    pl.semaphore_wait(barrier, peers)

    def local_wait(k):
        for owner, copy in local:
            if owner == k:
                copy.wait()

    def remote(k, s, way, d):
        at = pl.ds(pl.multiple_of(s * shard, 16), part)
        if k == 0:
            ref = ff.at[:, at, 2 * hc : 3 * hc]
        elif k <= last:
            ref = ff.at[k - 1, at, 0 : 2 * hc]
        elif k == nff:
            ref = ff.at[last, at, hc : 2 * hc]
        else:
            ref = (g3 if k == K3 else gb).at[at]
        return pltpu.make_async_remote_copy(
            src_ref=ref, dst_ref=ref, send_sem=zsend.at[k, way, s], recv_sem=recv.at[k, s],
            device_id=d, device_id_type=MESH,
        )

    def right(k, s, act):
        @pl.when(z < Z - 1)
        def _():
            act(remote(k, s * Y + y, 0, dev_z(z + 1)))

    def left(k, s, act):
        @pl.when(z > 0)
        def _():
            act(remote(k, s * Y + y, 1, dev_z(z - 1)))

    def across(k, s, act):
        act(remote(k, s * Y + y, 2, dev_y))

    def go(copy):
        copy.start()

    near = jnp.minimum(z, Z - 1 - z)
    low = z <= Z - 1 - z
    at_end = (z == 0) | (z == Z - 1)

    def inward(go_right, go_left):
        @pl.when(low)
        def _():
            go_right()

        @pl.when(~low)
        def _():
            go_left()

    def own_in(k):
        inward(lambda: right(k, z, go), lambda: left(k, z, go))

    def own_out(k):
        inward(lambda: left(k, z, go), lambda: right(k, z, go))

    def own_y(k):
        across(k, z, go)

    def down_copy(kind, s, v):
        to = (core_peer, x_peer, x_other)[kind]
        return pltpu.make_async_remote_copy(
            src_ref=ff.at[:, pl.ds(pl.multiple_of((s * Y + v) * shard, 16), part), 2 * hc : 3 * hc],
            dst_ref=fd.at[kind + 1, :, pl.ds(pl.multiple_of(s * shard, 16), part)],
            send_sem=dsem.at[0, kind, s], recv_sem=dsem.at[1, kind, s],
            device_id=to, device_id_type=MESH,
        )

    def spread(s, v, act):
        @pl.when(v == c)
        def _():
            act(down_copy(1, s, v))

        @pl.when(v != c)
        def _():
            act(down_copy(2, s, v))
            act(down_copy(0, s, v))

    def zsteps(k):
        def step(i, carry):
            @pl.when(z - 1 - i >= 0)
            def _():
                s = z - 1 - i
                remote(k, s * Y + y, 0, dev_z(z - 1)).wait_recv()
                right(k, s, go)
                across(k, s, go)
                if k == 0:
                    spread(s, y, go)

            @pl.when(z + 1 + i < Z)
            def _():
                s = z + 1 + i
                remote(k, s * Y + y, 0, dev_z(z + 1)).wait_recv()
                left(k, s, go)
                across(k, s, go)
                if k == 0:
                    spread(s, y, go)

            return carry

        lax.fori_loop(0, Z - 1, step, 0)

    def wait_across(k):
        def step(s, carry):
            remote(k, s * Y + 1 - y, 2, dev_y).wait_recv()
            return carry

        lax.fori_loop(0, Z, step, 0)

    def piece(q, first, count):
        if q == 2:
            return pr.at[pl.ds(pl.multiple_of(first * grp, 16), count * grp)]
        at = pl.ds(pl.multiple_of(first * shard, 16), (count - 1) * shard + part)
        if q == 3:
            return gb.at[at]
        return gv.at[at, lead] if q == 1 else ff.at[last, at, 0:hc]

    def across_p(q, s):
        ref = piece(q, s, 1)
        return pltpu.make_async_remote_copy(
            src_ref=ref, dst_ref=ref, send_sem=pysend.at[q], recv_sem=pyrecv.at[q],
            device_id=dev_y, device_id_type=MESH,
        )

    def remote_p(q, s, way, d):
        ref = piece(q, s * Y, Y)
        return pltpu.make_async_remote_copy(
            src_ref=ref, dst_ref=ref, send_sem=psend.at[q, way, s], recv_sem=precv.at[q, s],
            device_id=d, device_id_type=MESH,
        )

    def right_p(q, s, act):
        @pl.when(z < Z - 1)
        def _():
            act(remote_p(q, s, 0, dev_z(z + 1)))

    def left_p(q, s, act):
        @pl.when(z > 0)
        def _():
            act(remote_p(q, s, 1, dev_z(z - 1)))

    def start_in(q):
        across_p(q, z * Y + 1 - y).wait_recv()
        inward(lambda: right_p(q, z, go), lambda: left_p(q, z, go))

    def start_out(q):
        inward(lambda: left_p(q, z, go), lambda: right_p(q, z, go))

    def steps_p(qs, forward):
        def step(i, carry):
            @pl.when((z - 1 - i >= 0) & ((z < Z - 1) if forward else (z == Z - 1)))
            def _():
                s = z - 1 - i
                for q in qs:
                    remote_p(q, s, 0, dev_z(z - 1)).wait_recv()
                    if forward:
                        right_p(q, s, go)

            @pl.when((z + 1 + i < Z) & ((z > 0) if forward else (z == 0)))
            def _():
                s = z + 1 + i
                for q in qs:
                    remote_p(q, s, 0, dev_z(z + 1)).wait_recv()
                    if forward:
                        left_p(q, s, go)

            return carry

        lax.fori_loop(0, Z - 1, step, 0)

    def inside(s):
        return (s > 0) & (s < Z - 1)

    def steps_b():
        def step(i, carry):
            @pl.when(z - 1 - i >= 0)
            def _():
                s = z - 1 - i

                @pl.when(s > 0)
                def _():
                    remote(KB, s * Y + y, 0, dev_z(z - 1)).wait_recv()
                    right(KB, s, go)
                    across(KB, s, go)

                @pl.when(s == 0)
                def _():
                    remote_p(3, s, 0, dev_z(z - 1)).wait_recv()
                    right_p(3, s, go)

            @pl.when(z + 1 + i < Z)
            def _():
                s = z + 1 + i

                @pl.when(s < Z - 1)
                def _():
                    remote(KB, s * Y + y, 0, dev_z(z + 1)).wait_recv()
                    left(KB, s, go)
                    across(KB, s, go)

                @pl.when(s == Z - 1)
                def _():
                    remote_p(3, s, 0, dev_z(z + 1)).wait_recv()
                    left_p(3, s, go)

            return carry

        lax.fori_loop(0, Z - 1, step, 0)

    def pack_edges():
        packed = jnp.zeros((grp, 128), F32)
        for j in range(groups):
            count = min(grp, part - j * grp)
            if count <= 0:
                continue
            block = jnp.zeros((count, 128), F32)
            row = lax.broadcasted_iota(jnp.int32, (rem, 128), 0)
            lane = lax.broadcasted_iota(jnp.int32, (rem, 128), 1)
            for k in range(4):
                place = jnp.where(lane == row + (32 * j + rem * k), 1.0, 0.0).astype(BF16)
                source = edge[k, j * grp : j * grp + count, main : main + rem]
                block = block + jnp.dot(source, place, preferred_element_type=F32)
            if count < grp:
                block = jnp.concatenate([block, jnp.zeros((grp - count, 128), F32)], axis=0)
            packed = packed + block
        pr[pl.ds(pl.multiple_of(f * grp, 16), grp)] = packed.astype(BF16)

    def unpack_edges():
        row = lax.broadcasted_iota(jnp.int32, (128, 128), 0)
        lane = lax.broadcasted_iota(jnp.int32, (128, 128), 1)

        def body(s, carry):
            packed = pr[pl.ds(pl.multiple_of(s * grp, 16), grp)]
            for j in range(groups):
                count = min(grp, shard - j * grp)
                if count <= 0:
                    continue
                pick = jnp.where((lane < 32) & (row == lane + 32 * j), 1.0, 0.0).astype(BF16)
                block = jnp.dot(packed, pick, preferred_element_type=F32)[:count]
                at = pl.ds(pl.multiple_of(s * shard + j * grp, 16), count)
                gv[at, main : main + 128] = block.astype(BF16)
            return carry

        lax.fori_loop(0, n_fs, body, 0)

    def prepare_gains():
        gtmp[...] = jnp.zeros(gtmp.shape, F32)
        gtmp[0:6, 0:width] = gains_ref[...]
        for i in range(gtmp.shape[1] // 128):
            gcol[i * 128 : (i + 1) * 128] = gtmp[:, i * 128 : (i + 1) * 128].T

        def body(s, carry):
            for j in range(6):
                column = gcol[pl.ds(pl.multiple_of(s * part, 8), part), j : j + 1]
                at = pl.ds(pl.multiple_of(s * shard, 16), part)
                gains[j, at] = jnp.broadcast_to(column, (part, 128))
                pad = pl.ds(pl.multiple_of(s * shard + part, 8), shard - part)
                gains[j, pad] = jnp.zeros((shard - part, 128), F32)
            return carry

        lax.fori_loop(0, n_fs, body, 0)

    def prepare_taps():
        n_tp = lax.axis_size("tp")
        channels = taps_ref.shape[1] // n_tp
        lanes = tbuf.shape[1]
        tbuf[...] = jnp.zeros(tbuf.shape, F32)
        tbuf[0:CONV_K, 0 : taps_ref.shape[1]] = taps_ref[...].astype(F32)
        full = tbuf[...]
        mine = full
        for i in range(1, n_tp):
            mine = jnp.where(t == i, pltpu.roll(full, lanes - channels * i, 1), mine)
        tbuf[:, 0:main] = mine[:, 0:main]
        rest = pltpu.roll(mine[:, main : main + 128], 3 * rem, 1)
        lane = lax.broadcasted_iota(jnp.int32, rest.shape, 1)
        tbuf[:, main : main + 128] = jnp.where((lane >= 3 * rem) & (lane < 4 * rem), rest, 0.0)

    BLK = 128
    nblk = Dp // BLK

    def squares(v):
        return jnp.sum((v * v).reshape(BLK // 8, 8, rows), axis=0)

    def block_at(i):
        return pl.ds(pl.multiple_of(i * BLK, BLK), BLK)

    def inverse(sums):
        return lax.rsqrt(jnp.sum(sums, axis=0, keepdims=True) * (1.0 / width) + EPSILON)

    def gain_block(row, at):
        g = gains[row, at]
        return jnp.concatenate([g] * (rows // 128), axis=1)

    def sum_squares(source):
        def body(i, sums):
            return sums + squares(source[block_at(i)].astype(F32))

        return lax.fori_loop(0, nblk, body, jnp.zeros((8, rows), F32))

    def norm_to(source, sums, row):
        scale = inverse(sums)

        def body(i, carry):
            at = block_at(i)
            v = source[at].astype(F32) * scale * gain_block(row, at)
            normed[:, at] = v.T.astype(BF16)
            return carry

        lax.fori_loop(0, nblk, body, 0)

    def update(r, source, row, factor):
        scale = inverse(sum_squares(tot.at[r])) * factor

        def body(i, sums):
            at = block_at(i)
            v = source[at].astype(F32) + tot[r, at].astype(F32) * scale * gain_block(row, at)
            v = v.astype(BF16)
            res[r, at] = v
            return sums + squares(v.astype(F32))

        return lax.fori_loop(0, nblk, body, jnp.zeros((8, rows), F32))

    def hidden_copy(u, kind, k):
        source = hid.at[u, 2 if kind == 2 else 0, k]
        return pltpu.make_async_remote_copy(
            src_ref=source, dst_ref=hid.at[u, kind + 1, k], send_sem=hsem.at[0, u, kind, k],
            recv_sem=hsem.at[1, u, kind, k], device_id=x_peer if kind == 1 else core_peer,
            device_id_type=MESH,
        )

    def hidden(u, k):
        n = normed[...]
        gate_v = jnp.dot(n, ff[k, :, 0:hc], preferred_element_type=F32)
        up_v = jnp.dot(n, ff[k, :, hc : 2 * hc], preferred_element_type=F32)
        hid[u, 0, k] = (gate_v / (1.0 + jnp.exp(-gate_v)) * up_v).astype(BF16)
        hidden_copy(u, 1, k).start()
        hidden_copy(u, 0, k).start()

    def product(u, i, k, at):
        return lax.dot_general(fd[i, k, at], hid[u, i, k], NT, preferred_element_type=F32)

    def keep_down():
        def body(s, carry):
            at = pl.ds(pl.multiple_of(s * shard, 16), shard)
            for k in range(nff):
                fd[0, k, at] = ff[
                    k, pl.ds(pl.multiple_of((s * Y + c) * shard, 16), shard), 2 * hc : 3 * hc
                ]
            return carry

        lax.fori_loop(0, Z, body, 0)

    def finish_ffn(u, r, hook):
        def rows_of(j):
            return pl.ds(pl.multiple_of(j * shard, 16), shard)

        def own_part(j, carry):
            at = rows_of(j)
            total = product(u, 0, 0, at)
            for k in range(1, nff):
                total = total + product(u, 0, k, at)
            acc[at] = total
            return carry

        def add(i, ks):
            def body(j, carry):
                at = rows_of(j)
                total = acc[at]
                for k in ks:
                    total = total + product(u, i, k, at)
                acc[at] = total
                return carry

            lax.fori_loop(0, Z, body, 0)

        lax.fori_loop(0, Z, own_part, 0)
        for k in range(nff):
            hidden_copy(u, 0, k).wait_recv()
        add(1, range(nff))
        for k in range(nff):
            hidden_copy(u, 1, k).wait_recv()
            hidden_copy(u, 2, k).start()
            if k > 0:
                hidden_copy(u, 2, k - 1).wait_recv()
                add(3, (k - 1,))
            add(2, (k,))
        if hook:
            hook()
        hidden_copy(u, 2, last).wait_recv()

        def final(j, carry):
            at = rows_of(j)
            to = pl.ds(pl.multiple_of(j * pair + c * shard, 16), shard)
            tot[r, to] = (acc[at] + product(u, 3, last, at)).astype(BF16)
            tot_copy(r, j).start()
            return carry

        def arrive(j, carry):
            tot_copy(r, j).wait_recv()
            return carry

        lax.fori_loop(0, Z, final, 0)
        lax.fori_loop(0, Z, arrive, 0)

    def pair_at(j):
        return pl.ds(pl.multiple_of(j * pair, 16), pair)

    def mixer_pair(r, j):
        @pl.when(inside(j))
        def _():
            remote(KB, j * Y + 1 - y, 2, dev_y).wait_recv()

        at = pair_at(j)
        total = lax.dot_general(gb[at], mixed[:, 0:main], NT, preferred_element_type=F32)
        total = total + lax.dot_general(
            gv[at, main : main + 128], mixed[:, main:], NT, preferred_element_type=F32
        )
        part_buf[j] = total.astype(BF16)

    mine = pl.ds(pl.multiple_of(c * shard, 16), shard)
    other = pl.ds(pl.multiple_of((1 - c) * shard, 16), shard)

    def core_copy(r, j):
        return pltpu.make_async_remote_copy(
            src_ref=part_buf.at[j, other], dst_ref=crecv.at[j], send_sem=csem.at[0, j],
            recv_sem=csem.at[1, j], device_id=core_peer, device_id_type=MESH,
        )

    def x_copy(r, j):
        return pltpu.make_async_remote_copy(
            src_ref=xsend.at[j], dst_ref=xrecv.at[j], send_sem=xsem.at[0, j],
            recv_sem=xsem.at[1, j], device_id=x_peer, device_id_type=MESH,
        )

    def tot_copy(r, j):
        at = pl.ds(pl.multiple_of(j * pair + c * shard, 16), shard)
        return pltpu.make_async_remote_copy(
            src_ref=tot.at[r, at], dst_ref=tot.at[r, at], send_sem=tsem.at[0, r, j],
            recv_sem=tsem.at[1, r, j], device_id=core_peer, device_id_type=MESH,
        )

    def order(s):
        step = (s + 1) // 2
        close = jnp.where(s % 2 == 1, z - step, z + step)
        return jnp.where(s <= 2 * near, close, jnp.where(low, s, Z - 1 - s))

    def pass_on(j):
        source = dev_z(jnp.where(z == 0, z + 1, z - 1))

        @pl.when(inside(j))
        def _():
            remote(KB, j * Y + y, 0, source).wait_recv()
            across(KB, j, go)

        @pl.when(~inside(j))
        def _():
            remote_p(3, j, 0, source).wait_recv()

    def end_steps(first, stop):
        source = dev_z(jnp.where(z == 0, z + 1, z - 1))

        def step(s, carry):
            j = order(s)
            remote(K3, j * Y + y, 0, source).wait_recv()
            across(K3, j, go)
            return carry

        @pl.when(at_end)
        def _():
            lax.fori_loop(first, stop, step, 0)

    def reduce(r, compute):
        def cross(j):
            core_copy(r, j).wait_recv()
            xsend[j] = (part_buf[j, mine].astype(F32) + crecv[j].astype(F32)).astype(BF16)
            x_copy(r, j).start()

        def send(s, carry):
            j = order(s)
            @pl.when(at_end & (s < Z - 1))
            def _():
                pass_on(order(s + 1))

            compute(r, j)
            core_copy(r, j).start()

            @pl.when(s > 0)
            def _():
                cross(order(s - 1))

            return carry

        def receive(s, carry):
            j = order(s)
            x_copy(r, j).wait_recv()
            at = pl.ds(pl.multiple_of(j * pair + c * shard, 16), shard)
            tot[r, at] = (xsend[j].astype(F32) + xrecv[j].astype(F32)).astype(BF16)
            tot_copy(r, j).start()
            return carry

        def finish(s, carry):
            tot_copy(r, order(s)).wait_recv()
            return carry

        lax.fori_loop(0, Z, send, 0)
        cross(order(Z - 1))
        lax.fori_loop(0, Z, receive, 0)
        lax.fori_loop(0, Z, finish, 0)

    def mixer():
        n = normed[...]
        outer_inner = jnp.dot(n, g3[...], preferred_element_type=F32)
        outer_inner = outer_inner.astype(BF16).astype(F32)
        value_rest = jnp.dot(n, gv[...], preferred_element_type=F32)
        value_rest = value_rest.astype(BF16).astype(F32)
        rest = value_rest[:, main:]
        lane = lax.broadcasted_iota(jnp.int32, rest.shape, 1)
        keep = (lane >= 3 * rem) & (lane < 4 * rem)
        rests = [jnp.where(keep, pltpu.roll(rest, (3 - j) * rem, 1), 0.0) for j in range(3)]
        parts = [
            (outer_inner[:, 0:main], outer_inner[:, main:], value_rest[:, 0:main], 0),
            (rests[0], rests[1], rests[2], main),
        ]
        for outer, inner, value, first in parts:
            lanes = outer.shape[1]
            gated = inner * value
            token = lax.broadcasted_iota(jnp.int32, gated.shape, 0)
            conv = jnp.zeros_like(gated)
            for j in range(CONV_K):
                back = CONV_K - 1 - j
                moved = gated
                if back:
                    moved = jnp.where(token >= back, pltpu.roll(gated, back, 0), 0.0)
                conv = conv + tbuf[j : j + 1, first : first + lanes] * moved
            mixed[:, first : first + lanes] = (outer * conv).astype(BF16)

    def spread_across(s, carry):
        j = order(s)
        remote(0, j * Y + 1 - y, 2, dev_y).wait_recv()
        spread(j, 1 - y, go)
        return carry

    for k in range(2):
        local_wait(k)
        own_in(k)
        own_out(k)
        own_y(k)
        if k == 0:
            spread(z, y, go)
    local_wait(K3 + 1)
    pack_edges()
    for k in range(2, K3 + 1):
        local_wait(k)
    for q in range(3):
        across_p(q, f).start()

    @pl.when(at_end)
    def _():
        across_p(3, f).start()
        for k in range(2, K3 + 1):
            own_in(k)

    own_out(2)
    own_y(2)
    local_wait(K3 + 2)
    prepare_gains()
    prepare_taps()
    norm_to(xt, sum_squares(xt), 0)
    zsteps(0)
    own_out(nff)
    own_y(nff)

    @pl.when(~at_end)
    def _():
        own_in(2)

    start_in(0)
    start_out(0)

    @pl.when(at_end)
    def _():
        for q in range(1, 4):
            start_in(q)

    zsteps(1)
    lax.fori_loop(0, Z // 2, spread_across, 0)

    @pl.when(~at_end)
    def _():
        own_in(nff)

    zsteps(2)
    own_out(K3)

    @pl.when(~at_end)
    def _():
        own_in(K3)
        start_in(1)
        start_in(2)
        own_in(KB)

    lax.fori_loop(Z // 2, Z, spread_across, 0)
    zsteps(nff)
    steps_p((0,), True)
    own_y(K3)
    keep_down()
    wait_across(1)
    hidden(0, 0)

    @pl.when(~at_end)
    def _():
        zsteps(K3)
        start_out(1)
        start_out(2)
        steps_p((1, 2), True)
        own_out(KB)
        own_y(KB)
        steps_b()

    wait_across(2)
    hidden(0, 1)

    def down_arrived(s, carry):
        for kind in range(3):
            down_copy(kind, s, c).wait_recv()
        return carry

    end_steps(1, 2)
    lax.fori_loop(0, Z, down_arrived, 0)
    wait_across(nff)
    steps_p((0,), False)
    hidden(0, last)
    finish_ffn(0, 0, lambda: end_steps(2, Z - 1))
    norm_to(res.at[0], update(0, xt, 1, 0.5), 2)
    end_steps(Z - 1, Z)
    wait_across(K3)
    steps_p((1, 2), False)
    unpack_edges()
    mixer()
    reduce(1, mixer_pair)
    norm_to(res.at[1], update(1, res.at[0], 3, 1.0), 4)

    def again(k, carry):
        hidden(1, k)
        return carry

    lax.fori_loop(0, nff, again, 0)
    finish_ffn(1, 2, None)
    update(2, res.at[1], 5, 0.5)
    outs = [
        pltpu.make_async_copy(
            res.at[2, pl.ds(s * shard, part)], out_ref.at[pl.ds(s * part, part)], osem.at[s]
        )
        for s in range(n_fs)
    ]
    for copy in outs:
        copy.start()

    def done(copy):
        copy.wait_send()

    for k in range(nff + 3):
        def drain(s, carry):
            @pl.when(s <= z)
            def _():
                right(k, s, done)

            @pl.when(s >= z)
            def _():
                left(k, s, done)

            across(k, s, done)
            return carry

        lax.fori_loop(*((0, Z) if k < KB else (1, Z - 1)), drain, 0)
    for q in range(4):
        def drain_p(s, carry):
            @pl.when((s <= z) & ((q < 3) | ~inside(s)))
            def _():
                right_p(q, s, done)

            @pl.when((s >= z) & ((q < 3) | ~inside(s)))
            def _():
                left_p(q, s, done)

            return carry

        lax.fori_loop(0, Z, drain_p, 0)
    for q in range(3):
        across_p(q, f).wait_send()

    @pl.when(at_end)
    def _():
        across_p(3, f).wait_send()

    def drain_r(s, carry):
        core_copy(1, s).wait_send()
        x_copy(1, s).wait_send()
        for r in range(3):
            tot_copy(r, s).wait_send()
        for v in range(Y):
            spread(s, v, done)
        return carry

    lax.fori_loop(0, Z, drain_r, 0)
    for u in range(2):
        for kind in range(3):
            for k in range(nff):
                hidden_copy(u, kind, k).wait_send()
    for copy in outs:
        copy.wait()


def stream_form(mesh, Z):
    def local(stream_in, norm_gains, gate, up, down, outer_w, inner_w, value_w, mixer_w, conv_taps):
        rows, width = stream_in.shape
        part, hid = gate.shape
        channels = outer_w.shape[1]
        n_fs = 2 * Z
        shard = -(-part // 16) * 16
        Dp = n_fs * shard
        nff = 3
        hc = hid // nff
        main = channels // 128 * 128
        rem = channels - main
        grp = -(-part // 64) * 16
        lanes = -(-width // 128) * 128
        taps = -(-conv_taps.shape[1] // 128) * 128
        dma, vmem = pltpu.SemaphoreType.DMA, pltpu.VMEM
        out = pl.pallas_call(
            functools.partial(stream_kernel, (Z, shard, part, width, hc, nff, main, rem, grp)),
            out_shape=jax.ShapeDtypeStruct((width, rows), BF16),
            in_specs=[pl.BlockSpec(memory_space=pl.ANY)] * 8
            + [pl.BlockSpec(memory_space=pltpu.VMEM)] * 2,
            out_specs=pl.BlockSpec(memory_space=pl.ANY),
            scratch_shapes=[
                vmem((nff, Dp, 3 * hc), BF16),
                vmem((Dp, 2 * main), BF16),
                vmem((Dp, main + 128), BF16),
                vmem((Dp, main), BF16),
                vmem((n_fs * grp, 128), BF16),
                vmem((4, part, channels), BF16),
                vmem((Dp, rows), BF16),
                vmem((128, lanes), F32),
                vmem((lanes, 128), F32),
                vmem((6, Dp, 128), F32),
                vmem((8, taps), F32),
                vmem((rows, Dp), BF16),
                vmem((2, 4, nff, rows, hc), BF16),
                vmem((rows, main + 128), BF16),
                vmem((Z, 2 * shard, rows), BF16),
                vmem((Z, shard, rows), BF16),
                vmem((Z, shard, rows), BF16),
                vmem((Z, shard, rows), BF16),
                vmem((3, Dp, rows), BF16),
                vmem((3, Dp, rows), BF16),
                vmem((4, nff, Z * shard, hc), BF16),
                vmem((Z * shard, rows), F32),
                dma((3 * nff + 8 + n_fs,)),
                dma((nff + 3, 3, n_fs)),
                dma((nff + 3, n_fs)),
                dma((4, 2, Z)),
                dma((4, Z)),
                dma((4,)),
                dma((4,)),
                dma((2, Z)),
                dma((2, Z)),
                dma((2, 3, Z)),
                dma((n_fs,)),
                dma((2, 3, Z)),
                dma((2, 2, 3, nff)),
            ],
            compiler_params=pltpu.CompilerParams(
                collective_id=0, has_side_effects=True, vmem_limit_bytes=60 * 1024 * 1024
            ),
        )(gate, up, down, outer_w, inner_w, value_w, mixer_w, stream_in.T, norm_gains, conv_taps)
        return out.T

    return local


def y_count(mesh):
    try:
        found = len({d.coords[1] for d in mesh.devices.reshape(-1)})
    except AttributeError:
        found = 1
    return found if found == 2 and mesh.shape["fs"] % 2 == 0 else 1


def solution(mesh):
    n_fs, n_tp = mesh.shape["fs"], mesh.shape["tp"]
    Y = y_count(mesh)
    Z, X = n_fs // Y, n_tp // 2

    def chain_form(stream_in, norm_gains, gate, up, down, outer_w, inner_w, value_w, mixer_w, conv_taps):
        rows, width = stream_in.shape
        part, hid = gate.shape
        channels = outer_w.shape[1]
        shard = -(-part // 16) * 16
        Dp = n_fs * shard
        nff = 3 if hid % 384 == 0 else 1
        hc = hid // nff
        main = channels // 128 * 128
        rem = channels - main

        def widen(v):
            lead = v.shape[0]
            v = v.reshape(lead, n_fs, part)
            return jnp.pad(v, ((0, 0), (0, 0), (0, shard - part))).reshape(lead, Dp)

        sent = -(-part // 8) * 8

        def pack(w):
            return w if sent == part else jnp.pad(w, ((0, sent - part), (0, 0)))

        rest = [w[:, main:] for w in (outer_w, inner_w, value_w, mixer_w)]
        rest.append(jnp.zeros((part, 128 - 4 * rem), BF16))
        owns = [gate, up, down, outer_w, inner_w, value_w, mixer_w]
        owns = [pack(w) for w in owns + [jnp.concatenate(rest, axis=1)]]
        taps = lax.dynamic_slice_in_dim(
            conv_taps, lax.axis_index("tp") * channels, channels, 1
        ).astype(F32)
        taps = jnp.concatenate(
            [jnp.pad(taps[:, main:], ((0, 0), (3 * rem, 128 - 4 * rem))), taps[:, :main]], axis=1
        )
        half, quarter = rows // 2, rows // 4
        dma, vmem = pltpu.SemaphoreType.DMA, pltpu.VMEM
        out = pl.pallas_call(
            functools.partial(kernel, (Z, Y, X, shard, sent, width, hc, nff, main, rem)),
            out_shape=jax.ShapeDtypeStruct((rows, Dp), BF16),
            in_specs=[pl.BlockSpec(memory_space=pl.ANY)] * 8
            + [pl.BlockSpec(memory_space=pltpu.VMEM)] * 3,
            out_specs=pl.BlockSpec(memory_space=pltpu.VMEM),
            scratch_shapes=[
                vmem((nff, Dp, 3 * hc), BF16),
                vmem((Dp, 2 * main), BF16),
                vmem((Dp, 2 * main + 128), BF16),
                vmem((2, half, Dp), BF16),
                vmem((2, half, Dp), F32),
                vmem((2, half, main + 128), BF16),
                vmem((3, 2, quarter, Dp), BF16),
                vmem((3, 2, quarter, Dp), BF16),
                vmem((3, 2, quarter, Dp), BF16),
                vmem((3, 2, X - 1, quarter, Dp), BF16),
                vmem((3, rows, Dp), BF16),
                dma((3 * nff + 5,)),
                dma((nff + 2, 3, n_fs)),
                dma((nff + 2, n_fs)),
                dma((2, Z)),
                dma((Z,)),
                dma((2, 3, 2)),
                dma((3, 2, X - 1)),
                dma((3, 2, X - 1)),
                dma((2, 3, 2)),
            ],
            compiler_params=pltpu.CompilerParams(
                collective_id=0, has_side_effects=True, vmem_limit_bytes=60 * 1024 * 1024
            ),
        )(*owns, widen(stream_in), widen(norm_gains), taps)
        return out.reshape(rows, n_fs, shard)[:, :, :part].reshape(rows, width)

    def local(*args):
        rows, width = args[0].shape
        part, channels = args[5].shape
        rem = channels % 128
        fits = Y == 2 and X == 2 and part % 8 == 0 and 0 < rem <= 8 and rows % 128 == 0
        fits = fits and (n_fs * (-(-part // 16) * 16)) % 128 == 0 and channels > 128
        fits = fits and args[2].shape[1] % 384 == 0 and Z > 2
        return (stream_form(mesh, Z) if fits else chain_form)(*args)

    return jax.shard_map(
        local,
        mesh=mesh,
        in_specs=(P("fs", None), P()) + (P("fs", "tp"),) * 7 + (P(),),
        out_specs=P("fs", None),
        check_vma=False,
    )
```

```python
import functools

import jax
import jax.numpy as jnp
from jax import lax
from jax.experimental import pallas as pl
from jax.experimental.pallas import tpu as pltpu
from jax.sharding import PartitionSpec as P

MESH = pl.DeviceIdType.MESH
EPSILON = 1e-06
CONV_K = 3
F32, BF16 = jnp.float32, jnp.bfloat16
NT = (((1,), (1,)), ((), ()))


def kernel(cfg, *refs):
    Z, Y, X, shard, sent, width, hc, nff, main, rem = cfg
    own_refs = refs[:8]
    stream_ref, gains_ref, taps_ref, out_ref = refs[8:12]
    (ff, g3, g4, normed, acc, hidden, csend, crecv, xsend, xrecv, res,
     lsem, zsend, recv, asend, arecv, csem, xssem, xrsem, rsem) = refs[12:]
    rows, Dp = stream_ref.shape
    half, quarter = rows // 2, rows // 4
    K3, K4 = nff, nff + 1
    f, t = lax.axis_index("fs"), lax.axis_index("tp")
    z, y = f // Y, f % Y
    c, x = t % 2, t // 2
    core_peer = (f, x * 2 + 1 - c)
    x_peers = [(f, ((x + j) % X) * 2 + c) for j in range(1, X)]

    def dev_z(zz):
        return (zz * Y + y, t)

    dev_y = (z * Y + (Y - 1 - y), t)

    for s in range(Z * Y):
        tail = pl.ds(s * shard + shard - 16, 16)
        for k in range(nff):
            ff[k, tail] = jnp.zeros((16, 3 * hc), BF16)
        g3[tail] = jnp.zeros((16, 2 * main), BF16)
        g4[tail] = jnp.zeros((16, 2 * main + 128), BF16)

    barrier = pltpu.get_barrier_semaphore()

    def greet(d):
        pl.semaphore_signal(barrier, inc=1, device_id=d, device_id_type=MESH)

    always = [core_peer] + x_peers + ([dev_y] if Y == 2 else [])
    for d in always:
        greet(d)
    if Z > 1:
        @pl.when(z > 0)
        def _():
            greet(dev_z(z - 1))

        @pl.when(z < Z - 1)
        def _():
            greet(dev_z(z + 1))

    def slot(k, first, count):
        at = pl.ds(pl.multiple_of(first * shard, 16), (count - 1) * shard + sent)
        if k < nff:
            return ff.at[k, at]
        return (g3 if k == K3 else g4).at[at]

    here = pl.ds(pl.multiple_of(f * shard, 16), sent)
    moves = []
    for k in range(nff):
        for j in range(3):
            moves.append((k, own_refs[j].at[:, pl.ds(k * hc, hc)],
                          ff.at[k, here, pl.ds(j * hc, hc)]))
    ow, iw, vw, mw, rw = own_refs[3:]
    lead = pl.ds(0, main)
    moves.append((K3, ow.at[:, lead], g3.at[here, lead]))
    moves.append((K3, iw.at[:, lead], g3.at[here, pl.ds(main, main)]))
    moves.append((K4, vw.at[:, lead], g4.at[here, lead]))
    moves.append((K4, rw, g4.at[here, pl.ds(main, 128)]))
    moves.append((K4, mw.at[:, lead], g4.at[here, pl.ds(main + 128, main)]))
    local = [
        (k, pltpu.make_async_copy(src, dst, lsem.at[n])) for n, (k, src, dst) in enumerate(moves)
    ]
    for _, copy in local:
        copy.start()

    peers = len(always)
    if Z > 1:
        peers = peers + (z > 0).astype(jnp.int32) + (z < Z - 1).astype(jnp.int32)
    pl.semaphore_wait(barrier, peers)

    def remote(k, s, way, d):
        ref = slot(k, s, 1)
        return pltpu.make_async_remote_copy(
            src_ref=ref, dst_ref=ref, send_sem=zsend.at[k, way, s], recv_sem=recv.at[k, s],
            device_id=d, device_id_type=MESH,
        )

    def remote_a(s, way, d):
        ref = slot(K4, s * Y, Y)
        return pltpu.make_async_remote_copy(
            src_ref=ref, dst_ref=ref, send_sem=asend.at[way, s], recv_sem=arecv.at[s],
            device_id=d, device_id_type=MESH,
        )

    def right(k, s, act):
        @pl.when(z < Z - 1)
        def _():
            act(remote(k, s * Y + y, 0, dev_z(z + 1)))

    def left(k, s, act):
        @pl.when(z > 0)
        def _():
            act(remote(k, s * Y + y, 1, dev_z(z - 1)))

    def across(k, s, act):
        if Y == 2:
            act(remote(k, s * Y + y, 2, dev_y))

    def go(copy):
        copy.start()

    def own(k):
        right(k, z, go)
        left(k, z, go)
        across(k, z, go)

    def zsteps(k):
        def step(i, carry):
            @pl.when(z - 1 - i >= 0)
            def _():
                s = z - 1 - i
                remote(k, s * Y + y, 0, dev_z(z - 1)).wait_recv()
                right(k, s, go)
                across(k, s, go)

            @pl.when(z + 1 + i < Z)
            def _():
                s = z + 1 + i
                remote(k, s * Y + y, 0, dev_z(z + 1)).wait_recv()
                left(k, s, go)
                across(k, s, go)

            return carry

        lax.fori_loop(0, Z - 1, step, 0)

    def wait_across(k):
        if Y == 2:
            def step(s, carry):
                remote(k, s * Y + 1 - y, 2, dev_y).wait_recv()
                return carry

            lax.fori_loop(0, Z, step, 0)

    def right_a(s, act):
        @pl.when(z < Z - 1)
        def _():
            act(remote_a(s, 0, dev_z(z + 1)))

    def left_a(s, act):
        @pl.when(z > 0)
        def _():
            act(remote_a(s, 1, dev_z(z - 1)))

    def start_a():
        if Y == 2:
            remote(K4, z * Y + 1 - y, 2, dev_y).wait_recv()
        right_a(z, go)
        left_a(z, go)

    def steps_a(forward):
        def step(i, carry):
            @pl.when((z - 1 - i >= 0) & ((z < Z - 1) if forward else (z == Z - 1)))
            def _():
                s = z - 1 - i
                remote_a(s, 0, dev_z(z - 1)).wait_recv()
                if forward:
                    right_a(s, go)

            @pl.when((z + 1 + i < Z) & ((z > 0) if forward else (z == 0)))
            def _():
                s = z + 1 + i
                remote_a(s, 0, dev_z(z + 1)).wait_recv()
                if forward:
                    left_a(s, go)

            return carry

        lax.fori_loop(0, Z - 1, step, 0)

    def scaled(values, row):
        mean = jnp.sum(values * values, axis=-1, keepdims=True) * (1.0 / width)
        return values * lax.rsqrt(mean + EPSILON) * gains_ref[row : row + 1, :]

    def norm_to(source, row):
        def block(i, carry):
            at = pl.ds(pl.multiple_of(i * 32, 32), 32)
            per_half, per_quarter = half // 32, quarter // 32
            h, b = i // per_half, (i % per_half) // per_quarter
            to = pl.ds(pl.multiple_of(h * quarter + (i % per_quarter) * 32, 32), 32)
            normed[b, to] = scaled(source[at].astype(F32), row).astype(BF16)
            return carry

        lax.fori_loop(0, rows // 32, block, 0)

    def ffn_block(k, b, first):
        weights = ff.at[k]
        n = normed[b]
        gate = jnp.dot(n, weights[:, 0:hc], preferred_element_type=F32)
        up = jnp.dot(n, weights[:, hc : 2 * hc], preferred_element_type=F32)
        h = (gate / (1.0 + jnp.exp(-gate)) * up).astype(BF16)
        part = lax.dot_general(h, weights[:, 2 * hc :], NT, preferred_element_type=F32)
        acc[b] = part if first else acc[b] + part

    def ffn_chunk(k, first):
        def block(b, carry):
            ffn_block(k, b, first)
            return carry

        lax.fori_loop(0, 2, block, 0)

    mine = pl.ds(pl.multiple_of(c * quarter, 16), quarter)
    other = pl.ds(pl.multiple_of((1 - c) * quarter, 16), quarter)

    def core_copy(r, b):
        return pltpu.make_async_remote_copy(
            src_ref=csend.at[r, b], dst_ref=crecv.at[r, b], send_sem=csem.at[0, r, b],
            recv_sem=csem.at[1, r, b], device_id=core_peer, device_id_type=MESH,
        )

    def x_copy(r, b, j):
        return pltpu.make_async_remote_copy(
            src_ref=xsend.at[r, b], dst_ref=xrecv.at[r, b, j], send_sem=xssem.at[r, b, j],
            recv_sem=xrsem.at[r, b, j], device_id=x_peers[j], device_id_type=MESH,
        )

    def res_copy(r, b, core):
        at = pl.ds(pl.multiple_of(core * half + b * quarter, 16), quarter)
        return pltpu.make_async_remote_copy(
            src_ref=res.at[r, at], dst_ref=res.at[r, at], send_sem=rsem.at[0, r, b],
            recv_sem=rsem.at[1, r, b], device_id=core_peer, device_id_type=MESH,
        )

    def reduce(r, compute, source, row, factor):
        def send(b, carry):
            compute(b)
            csend[r, b] = acc[b, other].astype(BF16)
            core_copy(r, b).start()
            core_copy(r, b).wait()
            xsend[r, b] = (
                acc[b, mine].astype(BF16).astype(F32) + crecv[r, b].astype(F32)
            ).astype(BF16)
            for j in range(X - 1):
                x_copy(r, b, j).start()
            return carry

        def receive(b, carry):
            for j in range(X - 1):
                x_copy(r, b, j).wait()

            def block(i, inner_carry):
                at = pl.ds(pl.multiple_of(i * 32, 16), 32)
                full = pl.ds(pl.multiple_of(c * half + b * quarter + i * 32, 16), 32)
                total = xsend[r, b, at].astype(F32)
                for j in range(X - 1):
                    total = total + xrecv[r, b, j, at].astype(F32)
                res[r, full] = (
                    source[full].astype(F32) + factor * scaled(total, row)
                ).astype(BF16)
                return inner_carry

            lax.fori_loop(0, quarter // 32, block, 0)
            res_copy(r, b, c).start()
            return carry

        def finish(b, carry):
            res_copy(r, b, c).wait_send()
            res_copy(r, b, 1 - c).wait_recv()
            return carry

        lax.fori_loop(0, 2, send, 0)
        lax.fori_loop(0, 2, receive, 0)
        lax.fori_loop(0, 2, finish, 0)

    def swapped(v):
        q = [v[j * quarter : (j + 1) * quarter] for j in range(4)]
        return jnp.concatenate([q[0], q[2], q[1], q[3]], axis=0)

    def mixer():
        edge = main + 128
        n = swapped(normed[...].reshape(rows, Dp))
        outer_inner = jnp.dot(n, g3[...], preferred_element_type=F32)
        outer_inner = outer_inner.astype(BF16).astype(F32)
        value_rest = jnp.dot(n, g4[:, 0:edge], preferred_element_type=F32)
        value_rest = value_rest.astype(BF16).astype(F32)
        rest = value_rest[:, main:]
        if rem:
            lane = lax.broadcasted_iota(jnp.int32, rest.shape, 1)
            keep = (lane >= 3 * rem) & (lane < 4 * rem)
            rests = [
                jnp.where(keep, pltpu.roll(rest, (3 - j) * rem, 1), 0.0) for j in range(3)
            ]
        else:
            rests = [jnp.zeros_like(rest)] * 3
        outer = jnp.concatenate([rests[0], outer_inner[:, 0:main]], axis=1)
        inner = jnp.concatenate([rests[1], outer_inner[:, main:]], axis=1)
        value = jnp.concatenate([rests[2], value_rest[:, 0:main]], axis=1)
        gated = inner * value
        token = lax.broadcasted_iota(jnp.int32, gated.shape, 0)
        conv = jnp.zeros_like(gated)
        for j in range(CONV_K):
            back = CONV_K - 1 - j
            moved = gated
            if back:
                moved = jnp.where(token >= back, pltpu.roll(gated, back, 0), 0.0)
            conv = conv + taps_ref[j : j + 1, :] * moved
        hidden[...] = swapped((outer * conv).astype(BF16)).reshape(hidden.shape)

    def mixer_block(b):
        acc[b] = lax.dot_general(hidden[b], g4[:, main:], NT, preferred_element_type=F32)

    def last_chunk(b):
        ffn_block(nff - 1, b, nff == 1)

    def second(b):
        acc[b] = jnp.zeros(acc.shape[1:], F32)

        def again(k, carry):
            ffn_block(k, b, False)
            return carry

        lax.fori_loop(0, nff, again, 0)

    for k in range(nff + 2):
        for owner, copy in local:
            if owner == k:
                copy.wait()
        if k < 2:
            own(k)
    norm_to(stream_ref, 0)
    for k in range(nff):
        zsteps(k)
        if k + 2 <= K3:
            own(k + 2)
        if k + 2 == K3:
            across(K4, z, go)
        if k > 0:
            wait_across(k - 1)
            ffn_chunk(k - 1, k == 1)
    zsteps(K3)
    start_a()
    steps_a(True)
    wait_across(nff - 1)
    reduce(0, last_chunk, stream_ref, 1, 0.5)
    norm_to(res.at[0], 2)
    wait_across(K3)
    steps_a(False)
    mixer()
    reduce(1, mixer_block, res.at[0], 3, 1.0)
    norm_to(res.at[1], 4)
    reduce(2, second, res.at[1], 5, 0.5)
    out_ref[...] = res[2]

    def done(copy):
        copy.wait_send()

    for k in range(nff + 1):
        def drain(s, carry):
            @pl.when(s <= z)
            def _():
                right(k, s, done)

            @pl.when(s >= z)
            def _():
                left(k, s, done)

            across(k, s, done)
            return carry

        lax.fori_loop(0, Z, drain, 0)
    across(K4, z, done)

    def drain_a(s, carry):
        @pl.when(s <= z)
        def _():
            right_a(s, done)

        @pl.when(s >= z)
        def _():
            left_a(s, done)

        return carry

    lax.fori_loop(0, Z, drain_a, 0)


def stream_kernel(cfg, *refs):
    Z, shard, part, width, hc, nff, main, rem, grp = cfg
    own_refs = refs[:7]
    stream_ref, gains_ref, taps_ref, out_ref = refs[7:11]
    (ff, g3, gv, gb, pr, edge, xt, gains_in, taps_in, gtmp, gcol, gains, tbuf, normed, hid, mixed,
     part_buf, crecv, xsend, xrecv, tot, res, fd, acc,
     lsem, zsend, recv, psend, precv, pysend, pyrecv, csem, xsem, tsem,
     dsem, hsem) = refs[11:]
    Y = 2
    n_fs = Z * Y
    rows = normed.shape[0]
    Dp = n_fs * shard
    groups = 128 // 32
    pair = Y * shard
    last, K3, KB = nff - 1, nff + 1, nff + 2
    f, t = lax.axis_index("fs"), lax.axis_index("tp")
    z, y = f // Y, f % Y
    c, x = t % 2, t // 2
    core_peer = (f, x * 2 + 1 - c)
    x_peer = (f, (1 - x) * 2 + c)
    x_other = (f, (1 - x) * 2 + 1 - c)
    dev_y = (z * Y + (1 - y), t)

    def dev_z(zz):
        return (zz * Y + y, t)

    own_row = pl.multiple_of(f * shard, 16)
    here = pl.ds(own_row, part)
    lead = pl.ds(0, main)
    gate, up, down, ow, iw, vw, mw = own_refs
    moves = []
    for k in range(nff):
        moves.append((0, down.at[:, pl.ds(k * hc, hc)], ff.at[k, here, pl.ds(2 * hc, hc)]))
    for k in range(nff):
        for j, w in enumerate((gate, up)):
            moves.append((k + 1, w.at[:, pl.ds(k * hc, hc)], ff.at[k, here, pl.ds(j * hc, hc)]))
    moves.append((K3, ow.at[:, lead], g3.at[here, lead]))
    moves.append((K3, iw.at[:, lead], g3.at[here, pl.ds(main, main)]))
    moves.append((K3, vw.at[:, lead], gv.at[here, lead]))
    moves.append((K3, mw.at[:, lead], gb.at[here, :]))
    for j, w in enumerate((ow, iw, vw, mw)):
        moves.append((K3 + 1, w, edge.at[j]))
    moves.append((K3 + 2, gains_ref, gains_in))
    moves.append((K3 + 2, taps_ref, taps_in))
    for s in range(n_fs):
        moves.append((K3 + 2, stream_ref.at[pl.ds(s * part, part)], xt.at[pl.ds(s * shard, part)]))
    local = [
        (k, pltpu.make_async_copy(src, dst, lsem.at[n])) for n, (k, src, dst) in enumerate(moves)
    ]

    def pads(count):
        return [pl.ds(s * shard + part, shard - part) for s in range(count)]

    def clear(ref, index):
        ref[index] = jnp.zeros(ref.at[index].shape, ref.dtype)

    def clear_pairs():
        for pad in pads(n_fs):
            clear(ff, (last, pad, pl.ds(0, hc)))
            clear(gv, (pad, lead))
            clear(gb, (pad,))

    def clear_rest():
        for pad in pads(n_fs):
            for k in range(nff):
                clear(ff, (k, pad, pl.ds(0 if k < last else hc, 3 * hc if k < last else 2 * hc)))
            clear(g3, (pad,))
            clear(gv, (pad, pl.ds(main, 128)))
            clear(xt, (pad,))
        for pad in pads(Z):
            for i in range(1, 4):
                for k in range(nff):
                    clear(fd, (i, k, pad))

    for owner, copy in local:
        if owner < 2:
            copy.start()
    clear_pairs()
    barrier = pltpu.get_barrier_semaphore()

    def greet(d):
        pl.semaphore_signal(barrier, inc=1, device_id=d, device_id_type=MESH)

    for d in (core_peer, x_peer, x_other, dev_y):
        greet(d)

    @pl.when(z > 0)
    def _():
        greet(dev_z(z - 1))

    @pl.when(z < Z - 1)
    def _():
        greet(dev_z(z + 1))

    for owner, copy in local:
        if owner >= 2:
            copy.start()
    clear_rest()
    peers = 4 + (z > 0).astype(jnp.int32) + (z < Z - 1).astype(jnp.int32)
    pl.semaphore_wait(barrier, peers)

    def local_wait(k):
        for owner, copy in local:
            if owner == k:
                copy.wait()

    def remote(k, s, way, d):
        at = pl.ds(pl.multiple_of(s * shard, 16), part)
        if k == 0:
            ref = ff.at[:, at, 2 * hc : 3 * hc]
        elif k <= last:
            ref = ff.at[k - 1, at, 0 : 2 * hc]
        elif k == nff:
            ref = ff.at[last, at, hc : 2 * hc]
        else:
            ref = (g3 if k == K3 else gb).at[at]
        return pltpu.make_async_remote_copy(
            src_ref=ref, dst_ref=ref, send_sem=zsend.at[k, way, s], recv_sem=recv.at[k, s],
            device_id=d, device_id_type=MESH,
        )

    def right(k, s, act):
        @pl.when(z < Z - 1)
        def _():
            act(remote(k, s * Y + y, 0, dev_z(z + 1)))

    def left(k, s, act):
        @pl.when(z > 0)
        def _():
            act(remote(k, s * Y + y, 1, dev_z(z - 1)))

    def across(k, s, act):
        act(remote(k, s * Y + y, 2, dev_y))

    def go(copy):
        copy.start()

    near = jnp.minimum(z, Z - 1 - z)
    low = z <= Z - 1 - z
    at_end = (z == 0) | (z == Z - 1)

    def inward(go_right, go_left):
        @pl.when(low)
        def _():
            go_right()

        @pl.when(~low)
        def _():
            go_left()

    def own_in(k):
        inward(lambda: right(k, z, go), lambda: left(k, z, go))

    def own_out(k):
        inward(lambda: left(k, z, go), lambda: right(k, z, go))

    def own_y(k):
        across(k, z, go)

    def down_copy(kind, s, v):
        to = (core_peer, x_peer, x_other)[kind]
        return pltpu.make_async_remote_copy(
            src_ref=ff.at[:, pl.ds(pl.multiple_of((s * Y + v) * shard, 16), part), 2 * hc : 3 * hc],
            dst_ref=fd.at[kind + 1, :, pl.ds(pl.multiple_of(s * shard, 16), part)],
            send_sem=dsem.at[0, kind, s], recv_sem=dsem.at[1, kind, s],
            device_id=to, device_id_type=MESH,
        )

    def spread(s, v, act):
        @pl.when(v == c)
        def _():
            act(down_copy(1, s, v))

        @pl.when(v != c)
        def _():
            act(down_copy(2, s, v))
            act(down_copy(0, s, v))

    def zsteps(k):
        def step(i, carry):
            @pl.when(z - 1 - i >= 0)
            def _():
                s = z - 1 - i
                remote(k, s * Y + y, 0, dev_z(z - 1)).wait_recv()
                right(k, s, go)
                across(k, s, go)
                if k == 0:
                    spread(s, y, go)

            @pl.when(z + 1 + i < Z)
            def _():
                s = z + 1 + i
                remote(k, s * Y + y, 0, dev_z(z + 1)).wait_recv()
                left(k, s, go)
                across(k, s, go)
                if k == 0:
                    spread(s, y, go)

            return carry

        lax.fori_loop(0, Z - 1, step, 0)

    def wait_across(k):
        def step(s, carry):
            remote(k, s * Y + 1 - y, 2, dev_y).wait_recv()
            return carry

        lax.fori_loop(0, Z, step, 0)

    def piece(q, first, count):
        if q == 2:
            return pr.at[pl.ds(pl.multiple_of(first * grp, 16), count * grp)]
        at = pl.ds(pl.multiple_of(first * shard, 16), (count - 1) * shard + part)
        if q == 3:
            return gb.at[at]
        return gv.at[at, lead] if q == 1 else ff.at[last, at, 0:hc]

    def across_p(q, s):
        ref = piece(q, s, 1)
        return pltpu.make_async_remote_copy(
            src_ref=ref, dst_ref=ref, send_sem=pysend.at[q], recv_sem=pyrecv.at[q],
            device_id=dev_y, device_id_type=MESH,
        )

    def remote_p(q, s, way, d):
        ref = piece(q, s * Y, Y)
        return pltpu.make_async_remote_copy(
            src_ref=ref, dst_ref=ref, send_sem=psend.at[q, way, s], recv_sem=precv.at[q, s],
            device_id=d, device_id_type=MESH,
        )

    def right_p(q, s, act):
        @pl.when(z < Z - 1)
        def _():
            act(remote_p(q, s, 0, dev_z(z + 1)))

    def left_p(q, s, act):
        @pl.when(z > 0)
        def _():
            act(remote_p(q, s, 1, dev_z(z - 1)))

    def start_in(q):
        across_p(q, z * Y + 1 - y).wait_recv()
        inward(lambda: right_p(q, z, go), lambda: left_p(q, z, go))

    def start_out(q):
        inward(lambda: left_p(q, z, go), lambda: right_p(q, z, go))

    def steps_p(qs, forward):
        def step(i, carry):
            @pl.when((z - 1 - i >= 0) & ((z < Z - 1) if forward else (z == Z - 1)))
            def _():
                s = z - 1 - i
                for q in qs:
                    remote_p(q, s, 0, dev_z(z - 1)).wait_recv()
                    if forward:
                        right_p(q, s, go)

            @pl.when((z + 1 + i < Z) & ((z > 0) if forward else (z == 0)))
            def _():
                s = z + 1 + i
                for q in qs:
                    remote_p(q, s, 0, dev_z(z + 1)).wait_recv()
                    if forward:
                        left_p(q, s, go)

            return carry

        lax.fori_loop(0, Z - 1, step, 0)

    def inside(s):
        return (s > 0) & (s < Z - 1)

    def steps_b():
        def step(i, carry):
            @pl.when(z - 1 - i >= 0)
            def _():
                s = z - 1 - i

                @pl.when(s > 0)
                def _():
                    remote(KB, s * Y + y, 0, dev_z(z - 1)).wait_recv()
                    right(KB, s, go)
                    across(KB, s, go)

                @pl.when(s == 0)
                def _():
                    remote_p(3, s, 0, dev_z(z - 1)).wait_recv()
                    right_p(3, s, go)

            @pl.when(z + 1 + i < Z)
            def _():
                s = z + 1 + i

                @pl.when(s < Z - 1)
                def _():
                    remote(KB, s * Y + y, 0, dev_z(z + 1)).wait_recv()
                    left(KB, s, go)
                    across(KB, s, go)

                @pl.when(s == Z - 1)
                def _():
                    remote_p(3, s, 0, dev_z(z + 1)).wait_recv()
                    left_p(3, s, go)

            return carry

        lax.fori_loop(0, Z - 1, step, 0)

    def pack_edges():
        packed = jnp.zeros((grp, 128), F32)
        for j in range(groups):
            count = min(grp, part - j * grp)
            if count <= 0:
                continue
            block = jnp.zeros((count, 128), F32)
            row = lax.broadcasted_iota(jnp.int32, (rem, 128), 0)
            lane = lax.broadcasted_iota(jnp.int32, (rem, 128), 1)
            for k in range(4):
                place = jnp.where(lane == row + (32 * j + rem * k), 1.0, 0.0).astype(BF16)
                source = edge[k, j * grp : j * grp + count, main : main + rem]
                block = block + jnp.dot(source, place, preferred_element_type=F32)
            if count < grp:
                block = jnp.concatenate([block, jnp.zeros((grp - count, 128), F32)], axis=0)
            packed = packed + block
        pr[pl.ds(pl.multiple_of(f * grp, 16), grp)] = packed.astype(BF16)

    def unpack_edges():
        row = lax.broadcasted_iota(jnp.int32, (128, 128), 0)
        lane = lax.broadcasted_iota(jnp.int32, (128, 128), 1)

        def unpack(s):
            packed = pr[pl.ds(pl.multiple_of(s * grp, 16), grp)]
            for j in range(groups):
                count = min(grp, shard - j * grp)
                if count <= 0:
                    continue
                pick = jnp.where((lane < 32) & (row == lane + 32 * j), 1.0, 0.0).astype(BF16)
                block = jnp.dot(packed, pick, preferred_element_type=F32)[:count]
                at = pl.ds(pl.multiple_of(s * shard + j * grp, 16), count)
                gv[at, main : main + 128] = block.astype(BF16)

        def body(i, carry):
            j = order(i)

            @pl.when(at_end & (i > 0))
            def _():
                remote_p(2, j, 0, toward()).wait_recv()

            for v in range(Y):
                unpack(j * Y + v)
            return carry

        lax.fori_loop(0, Z, body, 0)

    def prepare_gains():
        gtmp[...] = jnp.zeros(gtmp.shape, F32)
        gtmp[0:6, 0:width] = gains_in[...]
        for i in range(gtmp.shape[1] // 128):
            gcol[i * 128 : (i + 1) * 128] = gtmp[:, i * 128 : (i + 1) * 128].T

        def body(s, carry):
            for j in range(6):
                column = gcol[pl.ds(pl.multiple_of(s * part, 8), part), j : j + 1]
                at = pl.ds(pl.multiple_of(s * shard, 16), part)
                gains[j, at] = jnp.broadcast_to(column, (part, 128))
                pad = pl.ds(pl.multiple_of(s * shard + part, 8), shard - part)
                gains[j, pad] = jnp.zeros((shard - part, 128), F32)
            return carry

        lax.fori_loop(0, n_fs, body, 0)

    def prepare_taps():
        n_tp = lax.axis_size("tp")
        channels = taps_in.shape[1] // n_tp
        lanes = tbuf.shape[1]
        tbuf[...] = jnp.zeros(tbuf.shape, F32)
        tbuf[0:CONV_K, 0 : taps_in.shape[1]] = taps_in[...].astype(F32)
        full = tbuf[...]
        mine = full
        for i in range(1, n_tp):
            mine = jnp.where(t == i, pltpu.roll(full, lanes - channels * i, 1), mine)
        tbuf[:, 0:main] = mine[:, 0:main]
        rest = pltpu.roll(mine[:, main : main + 128], 3 * rem, 1)
        lane = lax.broadcasted_iota(jnp.int32, rest.shape, 1)
        tbuf[:, main : main + 128] = jnp.where((lane >= 3 * rem) & (lane < 4 * rem), rest, 0.0)

    BLK = 128
    nblk = Dp // BLK

    def squares(v):
        return jnp.sum((v * v).reshape(v.shape[0] // 8, 8, rows), axis=0)

    def block_at(i):
        return pl.ds(pl.multiple_of(i * BLK, BLK), BLK)

    def inverse(sums):
        return lax.rsqrt(jnp.sum(sums, axis=0, keepdims=True) * (1.0 / width) + EPSILON)

    def gain_block(row, at):
        g = gains[row, at]
        return jnp.concatenate([g] * (rows // 128), axis=1)

    def sum_squares(source):
        def body(i, sums):
            return sums + squares(source[block_at(i)].astype(F32))

        return lax.fori_loop(0, nblk, body, jnp.zeros((8, rows), F32))

    def norm_to(source, sums, row):
        scale = inverse(sums)

        def body(i, carry):
            at = block_at(i)
            v = source[at].astype(F32) * scale * gain_block(row, at)
            normed[:, at] = v.T.astype(BF16)
            return carry

        lax.fori_loop(0, nblk, body, 0)

    def update(r, sums, source, row, factor):
        scale = inverse(sums) * factor

        def body(i, sums):
            at = block_at(i)
            v = source[at].astype(F32) + tot[r, at].astype(F32) * scale * gain_block(row, at)
            v = v.astype(BF16)
            res[r, at] = v
            return sums + squares(v.astype(F32))

        return lax.fori_loop(0, nblk, body, jnp.zeros((8, rows), F32))

    def hidden_copy(u, kind, k):
        source = hid.at[u, 2 if kind == 2 else 0, k]
        return pltpu.make_async_remote_copy(
            src_ref=source, dst_ref=hid.at[u, kind + 1, k], send_sem=hsem.at[0, u, kind, k],
            recv_sem=hsem.at[1, u, kind, k], device_id=x_peer if kind == 1 else core_peer,
            device_id_type=MESH,
        )

    def hidden(u, k):
        n = normed[...]
        gate_v = jnp.dot(n, ff[k, :, 0:hc], preferred_element_type=F32)
        up_v = jnp.dot(n, ff[k, :, hc : 2 * hc], preferred_element_type=F32)
        hid[u, 0, k] = (gate_v / (1.0 + jnp.exp(-gate_v)) * up_v).astype(BF16)
        hidden_copy(u, 1, k).start()
        hidden_copy(u, 0, k).start()

    def product(u, i, k, at):
        return lax.dot_general(fd[i, k, at], hid[u, i, k], NT, preferred_element_type=F32)

    def keep_down():
        def body(s, carry):
            at = pl.ds(pl.multiple_of(s * shard, 16), shard)
            for k in range(nff):
                fd[0, k, at] = ff[
                    k, pl.ds(pl.multiple_of((s * Y + c) * shard, 16), shard), 2 * hc : 3 * hc
                ]
            return carry

        lax.fori_loop(0, Z, body, 0)

    def finish_ffn(u, r, hook, idle):
        def rows_of(j):
            return pl.ds(pl.multiple_of(j * shard, 16), shard)

        def own_part(j, carry):
            at = rows_of(j)
            total = product(u, 0, 0, at)
            for k in range(1, nff):
                total = total + product(u, 0, k, at)
            acc[at] = total
            return carry

        def add(i, ks):
            def body(j, carry):
                at = rows_of(j)
                total = acc[at]
                for k in ks:
                    total = total + product(u, i, k, at)
                acc[at] = total
                return carry

            lax.fori_loop(0, Z, body, 0)

        lax.fori_loop(0, Z, own_part, 0)
        for k in range(nff):
            hidden_copy(u, 0, k).wait_recv()
        add(1, range(nff))
        if idle:
            idle()
        for k in range(nff):
            hidden_copy(u, 1, k).wait_recv()
            hidden_copy(u, 2, k).start()
            if k > 0:
                hidden_copy(u, 2, k - 1).wait_recv()
                add(3, (k - 1,))
            add(2, (k,))
        if hook:
            hook()
        hidden_copy(u, 2, last).wait_recv()

        def final(j, sums):
            at = rows_of(j)
            v = (acc[at] + product(u, 3, last, at)).astype(BF16)
            tot[r, column(j, c)] = v
            tot_copy(r, j).start()
            return sums + squares(v.astype(F32))

        return both_squares(r, lax.fori_loop(0, Z, final, jnp.zeros((8, rows), F32)), lambda j: j)

    def pair_at(j):
        return pl.ds(pl.multiple_of(j * pair, 16), pair)

    def mixer_pair(r, j):
        @pl.when(inside(j))
        def _():
            remote(KB, j * Y + 1 - y, 2, dev_y).wait_recv()

        at = pair_at(j)
        total = lax.dot_general(gb[at], mixed[:, 0:main], NT, preferred_element_type=F32)
        total = total + lax.dot_general(
            gv[at, main : main + 128], mixed[:, main:], NT, preferred_element_type=F32
        )
        part_buf[j] = total.astype(BF16)

    mine = pl.ds(pl.multiple_of(c * shard, 16), shard)
    other = pl.ds(pl.multiple_of((1 - c) * shard, 16), shard)

    def core_copy(r, j):
        return pltpu.make_async_remote_copy(
            src_ref=part_buf.at[j, other], dst_ref=crecv.at[j], send_sem=csem.at[0, j],
            recv_sem=csem.at[1, j], device_id=core_peer, device_id_type=MESH,
        )

    def x_copy(r, j):
        return pltpu.make_async_remote_copy(
            src_ref=xsend.at[j], dst_ref=xrecv.at[j], send_sem=xsem.at[0, j],
            recv_sem=xsem.at[1, j], device_id=x_peer, device_id_type=MESH,
        )

    def column(j, v):
        return pl.ds(pl.multiple_of(j * pair + v * shard, 16), shard)

    def both_squares(r, mine_sums, at):
        def arrive(s, sums):
            tot_copy(r, at(s)).wait_recv()
            return sums + squares(tot[r, column(at(s), 1 - c)].astype(F32))

        return mine_sums + lax.fori_loop(0, Z, arrive, jnp.zeros((8, rows), F32))

    def tot_copy(r, j):
        at = column(j, c)
        return pltpu.make_async_remote_copy(
            src_ref=tot.at[r, at], dst_ref=tot.at[r, at], send_sem=tsem.at[0, r, j],
            recv_sem=tsem.at[1, r, j], device_id=core_peer, device_id_type=MESH,
        )

    def toward():
        return dev_z(jnp.where(z == 0, z + 1, z - 1))

    def order(s):
        step = (s + 1) // 2
        close = jnp.where(s % 2 == 1, z - step, z + step)
        return jnp.where(s <= 2 * near, close, jnp.where(low, s, Z - 1 - s))

    def pass_on(j):
        source = toward()

        @pl.when(inside(j))
        def _():
            remote(KB, j * Y + y, 0, source).wait_recv()
            across(KB, j, go)

        @pl.when(~inside(j))
        def _():
            remote_p(3, j, 0, source).wait_recv()

    def end_steps(first, stop):
        source = toward()

        def step(s, carry):
            j = order(s)
            remote(K3, j * Y + y, 0, source).wait_recv()
            across(K3, j, go)
            return carry

        @pl.when(at_end)
        def _():
            lax.fori_loop(first, stop, step, 0)

    def reduce(r, compute):
        def cross(j):
            core_copy(r, j).wait_recv()
            xsend[j] = (part_buf[j, mine].astype(F32) + crecv[j].astype(F32)).astype(BF16)
            x_copy(r, j).start()

        def send(s, carry):
            j = order(s)
            @pl.when(at_end & (s > 0) & (s < Z - 1))
            def _():
                pass_on(order(s + 1))

            compute(r, j)
            core_copy(r, j).start()

            @pl.when(s > 0)
            def _():
                cross(order(s - 1))

            return carry

        def receive(s, sums):
            j = order(s)
            x_copy(r, j).wait_recv()
            v = (xsend[j].astype(F32) + xrecv[j].astype(F32)).astype(BF16)
            tot[r, column(j, c)] = v
            tot_copy(r, j).start()
            return sums + squares(v.astype(F32))

        lax.fori_loop(0, Z, send, 0)
        cross(order(Z - 1))
        return both_squares(r, lax.fori_loop(0, Z, receive, jnp.zeros((8, rows), F32)), order)

    def mixer():
        n = normed[...]
        outer_inner = jnp.dot(n, g3[...], preferred_element_type=F32)
        outer_inner = outer_inner.astype(BF16).astype(F32)
        value_rest = jnp.dot(n, gv[...], preferred_element_type=F32)
        value_rest = value_rest.astype(BF16).astype(F32)

        @pl.when(at_end)
        def _():
            pass_on(order(1))

        rest = value_rest[:, main:]
        lane = lax.broadcasted_iota(jnp.int32, rest.shape, 1)
        keep = (lane >= 3 * rem) & (lane < 4 * rem)
        rests = [jnp.where(keep, pltpu.roll(rest, (3 - j) * rem, 1), 0.0) for j in range(3)]
        parts = [
            (outer_inner[:, 0:main], outer_inner[:, main:], value_rest[:, 0:main], 0),
            (rests[0], rests[1], rests[2], main),
        ]
        for outer, inner, value, first in parts:
            lanes = outer.shape[1]
            gated = inner * value
            token = lax.broadcasted_iota(jnp.int32, gated.shape, 0)
            conv = jnp.zeros_like(gated)
            for j in range(CONV_K):
                back = CONV_K - 1 - j
                moved = gated
                if back:
                    moved = jnp.where(token >= back, pltpu.roll(gated, back, 0), 0.0)
                conv = conv + tbuf[j : j + 1, first : first + lanes] * moved
            mixed[:, first : first + lanes] = (outer * conv).astype(BF16)

    def drain_all():
        def done(copy):
            copy.wait_send()

        for k in range(nff + 3):
            def drain(s, carry):
                @pl.when(s <= z)
                def _():
                    right(k, s, done)

                @pl.when(s >= z)
                def _():
                    left(k, s, done)

                across(k, s, done)
                return carry

            lax.fori_loop(*((0, Z) if k < KB else (1, Z - 1)), drain, 0)
        for q in range(4):
            def drain_p(s, carry):
                @pl.when((s <= z) & ((q < 3) | ~inside(s)))
                def _():
                    right_p(q, s, done)

                @pl.when((s >= z) & ((q < 3) | ~inside(s)))
                def _():
                    left_p(q, s, done)

                return carry

            lax.fori_loop(0, Z, drain_p, 0)
        for q in range(3):
            across_p(q, f).wait_send()

        @pl.when(at_end)
        def _():
            across_p(3, f).wait_send()

        def drain_r(s, carry):
            core_copy(1, s).wait_send()
            x_copy(1, s).wait_send()
            for r in range(2):
                tot_copy(r, s).wait_send()
            for v in range(Y):
                spread(s, v, done)
            return carry

        lax.fori_loop(0, Z, drain_r, 0)
        for kind in range(3):
            for k in range(nff):
                hidden_copy(0, kind, k).wait_send()

    def spread_across(s, carry):
        j = order(s)
        remote(0, j * Y + 1 - y, 2, dev_y).wait_recv()
        spread(j, 1 - y, go)
        return carry

    for k in range(2):
        local_wait(k)
        own_in(k)
        own_out(k)
        own_y(k)
        if k == 0:
            spread(z, y, go)
    local_wait(K3 + 1)
    pack_edges()
    for k in range(2, K3 + 1):
        local_wait(k)
    for q in range(3):
        across_p(q, f).start()

    @pl.when(at_end)
    def _():
        across_p(3, f).start()
        for k in range(2, K3 + 1):
            own_in(k)

    own_out(2)
    own_y(2)
    local_wait(K3 + 2)
    prepare_gains()
    prepare_taps()
    norm_to(xt, sum_squares(xt), 0)
    zsteps(0)
    own_out(nff)
    own_y(nff)

    @pl.when(~at_end)
    def _():
        own_in(2)

    start_in(0)
    start_out(0)

    @pl.when(at_end)
    def _():
        for q in range(1, 4):
            start_in(q)

    zsteps(1)
    lax.fori_loop(0, Z // 2, spread_across, 0)

    @pl.when(~at_end)
    def _():
        own_in(nff)

    zsteps(2)
    own_out(K3)

    @pl.when(~at_end)
    def _():
        own_in(K3)
        start_in(1)
        start_in(2)
        own_in(KB)

    lax.fori_loop(Z // 2, Z, spread_across, 0)
    zsteps(nff)
    steps_p((0,), True)
    own_y(K3)
    keep_down()
    wait_across(1)
    hidden(0, 0)

    @pl.when(~at_end)
    def _():
        zsteps(K3)
        start_out(1)
        start_out(2)
        steps_p((1, 2), True)
        own_out(KB)
        own_y(KB)
        steps_b()

    wait_across(2)
    hidden(0, 1)

    def down_arrived(s, carry):
        for kind in range(3):
            down_copy(kind, s, c).wait_recv()
        return carry

    end_steps(1, 2)
    lax.fori_loop(0, Z, down_arrived, 0)
    wait_across(nff)
    steps_p((0,), False)
    hidden(0, last)
    sums = finish_ffn(0, 0, lambda: end_steps(2, Z - 1), None)
    norm_to(res.at[0], update(0, sums, xt, 1, 0.5), 2)
    end_steps(Z - 1, Z)
    wait_across(K3)
    unpack_edges()
    steps_p((1,), False)
    mixer()
    sums = reduce(1, mixer_pair)
    norm_to(res.at[1], update(1, sums, res.at[0], 3, 1.0), 4)

    def again(k, carry):
        hidden(1, k)
        return carry

    lax.fori_loop(0, nff, again, 0)
    scale = inverse(finish_ffn(1, 2, None, drain_all)) * 0.5
    for s in range(n_fs):
        at = pl.ds(s * shard, part)
        v = res[1, at].astype(F32) + tot[2, at].astype(F32) * scale * gain_block(5, at)
        out_ref[s * part : (s + 1) * part] = v.astype(BF16)
    def drain_last(j, carry):
        tot_copy(2, j).wait_send()
        return carry

    lax.fori_loop(0, Z, drain_last, 0)
    for kind in range(3):
        for k in range(nff):
            hidden_copy(1, kind, k).wait_send()


def stream_form(mesh, Z):
    def local(stream_in, norm_gains, gate, up, down, outer_w, inner_w, value_w, mixer_w, conv_taps):
        rows, width = stream_in.shape
        part, hid = gate.shape
        channels = outer_w.shape[1]
        n_fs = 2 * Z
        shard = -(-part // 16) * 16
        Dp = n_fs * shard
        nff = 3
        hc = hid // nff
        main = channels // 128 * 128
        rem = channels - main
        grp = -(-part // 64) * 16
        lanes = -(-width // 128) * 128
        taps = -(-conv_taps.shape[1] // 128) * 128
        dma, vmem = pltpu.SemaphoreType.DMA, pltpu.VMEM
        out = pl.pallas_call(
            functools.partial(stream_kernel, (Z, shard, part, width, hc, nff, main, rem, grp)),
            out_shape=pltpu.VMEM((width, rows), BF16),
            in_specs=[pl.BlockSpec(memory_space=pl.ANY)] * 10,
            out_specs=pl.BlockSpec(memory_space=pltpu.VMEM),
            scratch_shapes=[
                vmem((nff, Dp, 3 * hc), BF16),
                vmem((Dp, 2 * main), BF16),
                vmem((Dp, main + 128), BF16),
                vmem((Dp, main), BF16),
                vmem((n_fs * grp, 128), BF16),
                vmem((4, part, channels), BF16),
                vmem((Dp, rows), BF16),
                vmem(norm_gains.shape, F32),
                vmem(conv_taps.shape, BF16),
                vmem((128, lanes), F32),
                vmem((lanes, 128), F32),
                vmem((6, Dp, 128), F32),
                vmem((8, taps), F32),
                vmem((rows, Dp), BF16),
                vmem((2, 4, nff, rows, hc), BF16),
                vmem((rows, main + 128), BF16),
                vmem((Z, 2 * shard, rows), BF16),
                vmem((Z, shard, rows), BF16),
                vmem((Z, shard, rows), BF16),
                vmem((Z, shard, rows), BF16),
                vmem((3, Dp, rows), BF16),
                vmem((2, Dp, rows), BF16),
                vmem((4, nff, Z * shard, hc), BF16),
                vmem((Z * shard, rows), F32),
                dma((3 * nff + 10 + n_fs,)),
                dma((nff + 3, 3, n_fs)),
                dma((nff + 3, n_fs)),
                dma((4, 2, Z)),
                dma((4, Z)),
                dma((4,)),
                dma((4,)),
                dma((2, Z)),
                dma((2, Z)),
                dma((2, 3, Z)),
                dma((2, 3, Z)),
                dma((2, 2, 3, nff)),
            ],
            compiler_params=pltpu.CompilerParams(
                collective_id=0, has_side_effects=True, vmem_limit_bytes=60 * 1024 * 1024
            ),
        )(gate, up, down, outer_w, inner_w, value_w, mixer_w, stream_in.T, norm_gains, conv_taps)
        return out.T

    return local


def y_count(mesh):
    try:
        found = len({d.coords[1] for d in mesh.devices.reshape(-1)})
    except AttributeError:
        found = 1
    return found if found == 2 and mesh.shape["fs"] % 2 == 0 else 1


def solution(mesh):
    n_fs, n_tp = mesh.shape["fs"], mesh.shape["tp"]
    Y = y_count(mesh)
    Z, X = n_fs // Y, n_tp // 2

    def chain_form(stream_in, norm_gains, gate, up, down, outer_w, inner_w, value_w, mixer_w, conv_taps):
        rows, width = stream_in.shape
        part, hid = gate.shape
        channels = outer_w.shape[1]
        shard = -(-part // 16) * 16
        Dp = n_fs * shard
        nff = 3 if hid % 384 == 0 else 1
        hc = hid // nff
        main = channels // 128 * 128
        rem = channels - main

        def widen(v):
            lead = v.shape[0]
            v = v.reshape(lead, n_fs, part)
            return jnp.pad(v, ((0, 0), (0, 0), (0, shard - part))).reshape(lead, Dp)

        sent = -(-part // 8) * 8

        def pack(w):
            return w if sent == part else jnp.pad(w, ((0, sent - part), (0, 0)))

        rest = [w[:, main:] for w in (outer_w, inner_w, value_w, mixer_w)]
        rest.append(jnp.zeros((part, 128 - 4 * rem), BF16))
        owns = [gate, up, down, outer_w, inner_w, value_w, mixer_w]
        owns = [pack(w) for w in owns + [jnp.concatenate(rest, axis=1)]]
        taps = lax.dynamic_slice_in_dim(
            conv_taps, lax.axis_index("tp") * channels, channels, 1
        ).astype(F32)
        taps = jnp.concatenate(
            [jnp.pad(taps[:, main:], ((0, 0), (3 * rem, 128 - 4 * rem))), taps[:, :main]], axis=1
        )
        half, quarter = rows // 2, rows // 4
        dma, vmem = pltpu.SemaphoreType.DMA, pltpu.VMEM
        out = pl.pallas_call(
            functools.partial(kernel, (Z, Y, X, shard, sent, width, hc, nff, main, rem)),
            out_shape=jax.ShapeDtypeStruct((rows, Dp), BF16),
            in_specs=[pl.BlockSpec(memory_space=pl.ANY)] * 8
            + [pl.BlockSpec(memory_space=pltpu.VMEM)] * 3,
            out_specs=pl.BlockSpec(memory_space=pltpu.VMEM),
            scratch_shapes=[
                vmem((nff, Dp, 3 * hc), BF16),
                vmem((Dp, 2 * main), BF16),
                vmem((Dp, 2 * main + 128), BF16),
                vmem((2, half, Dp), BF16),
                vmem((2, half, Dp), F32),
                vmem((2, half, main + 128), BF16),
                vmem((3, 2, quarter, Dp), BF16),
                vmem((3, 2, quarter, Dp), BF16),
                vmem((3, 2, quarter, Dp), BF16),
                vmem((3, 2, X - 1, quarter, Dp), BF16),
                vmem((3, rows, Dp), BF16),
                dma((3 * nff + 5,)),
                dma((nff + 2, 3, n_fs)),
                dma((nff + 2, n_fs)),
                dma((2, Z)),
                dma((Z,)),
                dma((2, 3, 2)),
                dma((3, 2, X - 1)),
                dma((3, 2, X - 1)),
                dma((2, 3, 2)),
            ],
            compiler_params=pltpu.CompilerParams(
                collective_id=0, has_side_effects=True, vmem_limit_bytes=60 * 1024 * 1024
            ),
        )(*owns, widen(stream_in), widen(norm_gains), taps)
        return out.reshape(rows, n_fs, shard)[:, :, :part].reshape(rows, width)

    def local(*args):
        rows, width = args[0].shape
        part, channels = args[5].shape
        rem = channels % 128
        fits = Y == 2 and X == 2 and part % 8 == 0 and 0 < rem <= 8 and rows % 128 == 0
        fits = fits and (n_fs * (-(-part // 16) * 16)) % 128 == 0 and channels > 128
        fits = fits and args[2].shape[1] % 384 == 0 and Z > 2
        return (stream_form(mesh, Z) if fits else chain_form)(*args)

    return jax.shard_map(
        local,
        mesh=mesh,
        in_specs=(P("fs", None), P()) + (P("fs", "tp"),) * 7 + (P(),),
        out_specs=P("fs", None),
        check_vma=False,
    )
```

```python
import functools

import jax
import jax.numpy as jnp
from jax import lax
from jax.experimental import pallas as pl
from jax.experimental.pallas import tpu as pltpu
from jax.sharding import PartitionSpec as P

MESH = pl.DeviceIdType.MESH
EPSILON = 1e-06
CONV_K = 3
F32, BF16 = jnp.float32, jnp.bfloat16
NT = (((1,), (1,)), ((), ()))


def kernel(cfg, *refs):
    Z, Y, X, shard, sent, width, hc, nff, main, rem = cfg
    own_refs = refs[:8]
    stream_ref, gains_ref, taps_ref, out_ref = refs[8:12]
    (ff, g3, g4, normed, acc, hidden, csend, crecv, xsend, xrecv, res,
     lsem, zsend, recv, asend, arecv, csem, xssem, xrsem, rsem) = refs[12:]
    rows, Dp = stream_ref.shape
    half, quarter = rows // 2, rows // 4
    K3, K4 = nff, nff + 1
    f, t = lax.axis_index("fs"), lax.axis_index("tp")
    z, y = f // Y, f % Y
    c, x = t % 2, t // 2
    core_peer = (f, x * 2 + 1 - c)
    x_peers = [(f, ((x + j) % X) * 2 + c) for j in range(1, X)]

    def dev_z(zz):
        return (zz * Y + y, t)

    dev_y = (z * Y + (Y - 1 - y), t)

    for s in range(Z * Y):
        tail = pl.ds(s * shard + shard - 16, 16)
        for k in range(nff):
            ff[k, tail] = jnp.zeros((16, 3 * hc), BF16)
        g3[tail] = jnp.zeros((16, 2 * main), BF16)
        g4[tail] = jnp.zeros((16, 2 * main + 128), BF16)

    barrier = pltpu.get_barrier_semaphore()

    def greet(d):
        pl.semaphore_signal(barrier, inc=1, device_id=d, device_id_type=MESH)

    always = [core_peer] + x_peers + ([dev_y] if Y == 2 else [])
    for d in always:
        greet(d)
    if Z > 1:
        @pl.when(z > 0)
        def _():
            greet(dev_z(z - 1))

        @pl.when(z < Z - 1)
        def _():
            greet(dev_z(z + 1))

    def slot(k, first, count):
        at = pl.ds(pl.multiple_of(first * shard, 16), (count - 1) * shard + sent)
        if k < nff:
            return ff.at[k, at]
        return (g3 if k == K3 else g4).at[at]

    here = pl.ds(pl.multiple_of(f * shard, 16), sent)
    moves = []
    for k in range(nff):
        for j in range(3):
            moves.append((k, own_refs[j].at[:, pl.ds(k * hc, hc)],
                          ff.at[k, here, pl.ds(j * hc, hc)]))
    ow, iw, vw, mw, rw = own_refs[3:]
    lead = pl.ds(0, main)
    moves.append((K3, ow.at[:, lead], g3.at[here, lead]))
    moves.append((K3, iw.at[:, lead], g3.at[here, pl.ds(main, main)]))
    moves.append((K4, vw.at[:, lead], g4.at[here, lead]))
    moves.append((K4, rw, g4.at[here, pl.ds(main, 128)]))
    moves.append((K4, mw.at[:, lead], g4.at[here, pl.ds(main + 128, main)]))
    local = [
        (k, pltpu.make_async_copy(src, dst, lsem.at[n])) for n, (k, src, dst) in enumerate(moves)
    ]
    for _, copy in local:
        copy.start()

    peers = len(always)
    if Z > 1:
        peers = peers + (z > 0).astype(jnp.int32) + (z < Z - 1).astype(jnp.int32)
    pl.semaphore_wait(barrier, peers)

    def remote(k, s, way, d):
        ref = slot(k, s, 1)
        return pltpu.make_async_remote_copy(
            src_ref=ref, dst_ref=ref, send_sem=zsend.at[k, way, s], recv_sem=recv.at[k, s],
            device_id=d, device_id_type=MESH,
        )

    def remote_a(s, way, d):
        ref = slot(K4, s * Y, Y)
        return pltpu.make_async_remote_copy(
            src_ref=ref, dst_ref=ref, send_sem=asend.at[way, s], recv_sem=arecv.at[s],
            device_id=d, device_id_type=MESH,
        )

    def right(k, s, act):
        @pl.when(z < Z - 1)
        def _():
            act(remote(k, s * Y + y, 0, dev_z(z + 1)))

    def left(k, s, act):
        @pl.when(z > 0)
        def _():
            act(remote(k, s * Y + y, 1, dev_z(z - 1)))

    def across(k, s, act):
        if Y == 2:
            act(remote(k, s * Y + y, 2, dev_y))

    def go(copy):
        copy.start()

    def own(k):
        right(k, z, go)
        left(k, z, go)
        across(k, z, go)

    def zsteps(k):
        def step(i, carry):
            @pl.when(z - 1 - i >= 0)
            def _():
                s = z - 1 - i
                remote(k, s * Y + y, 0, dev_z(z - 1)).wait_recv()
                right(k, s, go)
                across(k, s, go)

            @pl.when(z + 1 + i < Z)
            def _():
                s = z + 1 + i
                remote(k, s * Y + y, 0, dev_z(z + 1)).wait_recv()
                left(k, s, go)
                across(k, s, go)

            return carry

        lax.fori_loop(0, Z - 1, step, 0)

    def wait_across(k):
        if Y == 2:
            def step(s, carry):
                remote(k, s * Y + 1 - y, 2, dev_y).wait_recv()
                return carry

            lax.fori_loop(0, Z, step, 0)

    def right_a(s, act):
        @pl.when(z < Z - 1)
        def _():
            act(remote_a(s, 0, dev_z(z + 1)))

    def left_a(s, act):
        @pl.when(z > 0)
        def _():
            act(remote_a(s, 1, dev_z(z - 1)))

    def start_a():
        if Y == 2:
            remote(K4, z * Y + 1 - y, 2, dev_y).wait_recv()
        right_a(z, go)
        left_a(z, go)

    def steps_a(forward):
        def step(i, carry):
            @pl.when((z - 1 - i >= 0) & ((z < Z - 1) if forward else (z == Z - 1)))
            def _():
                s = z - 1 - i
                remote_a(s, 0, dev_z(z - 1)).wait_recv()
                if forward:
                    right_a(s, go)

            @pl.when((z + 1 + i < Z) & ((z > 0) if forward else (z == 0)))
            def _():
                s = z + 1 + i
                remote_a(s, 0, dev_z(z + 1)).wait_recv()
                if forward:
                    left_a(s, go)

            return carry

        lax.fori_loop(0, Z - 1, step, 0)

    def scaled(values, row):
        mean = jnp.sum(values * values, axis=-1, keepdims=True) * (1.0 / width)
        return values * lax.rsqrt(mean + EPSILON) * gains_ref[row : row + 1, :]

    def norm_to(source, row):
        def block(i, carry):
            at = pl.ds(pl.multiple_of(i * 32, 32), 32)
            per_half, per_quarter = half // 32, quarter // 32
            h, b = i // per_half, (i % per_half) // per_quarter
            to = pl.ds(pl.multiple_of(h * quarter + (i % per_quarter) * 32, 32), 32)
            normed[b, to] = scaled(source[at].astype(F32), row).astype(BF16)
            return carry

        lax.fori_loop(0, rows // 32, block, 0)

    def ffn_block(k, b, first):
        weights = ff.at[k]
        n = normed[b]
        gate = jnp.dot(n, weights[:, 0:hc], preferred_element_type=F32)
        up = jnp.dot(n, weights[:, hc : 2 * hc], preferred_element_type=F32)
        h = (gate / (1.0 + jnp.exp(-gate)) * up).astype(BF16)
        part = lax.dot_general(h, weights[:, 2 * hc :], NT, preferred_element_type=F32)
        acc[b] = part if first else acc[b] + part

    def ffn_chunk(k, first):
        def block(b, carry):
            ffn_block(k, b, first)
            return carry

        lax.fori_loop(0, 2, block, 0)

    mine = pl.ds(pl.multiple_of(c * quarter, 16), quarter)
    other = pl.ds(pl.multiple_of((1 - c) * quarter, 16), quarter)

    def core_copy(r, b):
        return pltpu.make_async_remote_copy(
            src_ref=csend.at[r, b], dst_ref=crecv.at[r, b], send_sem=csem.at[0, r, b],
            recv_sem=csem.at[1, r, b], device_id=core_peer, device_id_type=MESH,
        )

    def x_copy(r, b, j):
        return pltpu.make_async_remote_copy(
            src_ref=xsend.at[r, b], dst_ref=xrecv.at[r, b, j], send_sem=xssem.at[r, b, j],
            recv_sem=xrsem.at[r, b, j], device_id=x_peers[j], device_id_type=MESH,
        )

    def res_copy(r, b, core):
        at = pl.ds(pl.multiple_of(core * half + b * quarter, 16), quarter)
        return pltpu.make_async_remote_copy(
            src_ref=res.at[r, at], dst_ref=res.at[r, at], send_sem=rsem.at[0, r, b],
            recv_sem=rsem.at[1, r, b], device_id=core_peer, device_id_type=MESH,
        )

    def reduce(r, compute, source, row, factor):
        def send(b, carry):
            compute(b)
            csend[r, b] = acc[b, other].astype(BF16)
            core_copy(r, b).start()
            core_copy(r, b).wait()
            xsend[r, b] = (
                acc[b, mine].astype(BF16).astype(F32) + crecv[r, b].astype(F32)
            ).astype(BF16)
            for j in range(X - 1):
                x_copy(r, b, j).start()
            return carry

        def receive(b, carry):
            for j in range(X - 1):
                x_copy(r, b, j).wait()

            def block(i, inner_carry):
                at = pl.ds(pl.multiple_of(i * 32, 16), 32)
                full = pl.ds(pl.multiple_of(c * half + b * quarter + i * 32, 16), 32)
                total = xsend[r, b, at].astype(F32)
                for j in range(X - 1):
                    total = total + xrecv[r, b, j, at].astype(F32)
                res[r, full] = (
                    source[full].astype(F32) + factor * scaled(total, row)
                ).astype(BF16)
                return inner_carry

            lax.fori_loop(0, quarter // 32, block, 0)
            res_copy(r, b, c).start()
            return carry

        def finish(b, carry):
            res_copy(r, b, c).wait_send()
            res_copy(r, b, 1 - c).wait_recv()
            return carry

        lax.fori_loop(0, 2, send, 0)
        lax.fori_loop(0, 2, receive, 0)
        lax.fori_loop(0, 2, finish, 0)

    def swapped(v):
        q = [v[j * quarter : (j + 1) * quarter] for j in range(4)]
        return jnp.concatenate([q[0], q[2], q[1], q[3]], axis=0)

    def mixer():
        edge = main + 128
        n = swapped(normed[...].reshape(rows, Dp))
        outer_inner = jnp.dot(n, g3[...], preferred_element_type=F32)
        outer_inner = outer_inner.astype(BF16).astype(F32)
        value_rest = jnp.dot(n, g4[:, 0:edge], preferred_element_type=F32)
        value_rest = value_rest.astype(BF16).astype(F32)
        rest = value_rest[:, main:]
        if rem:
            lane = lax.broadcasted_iota(jnp.int32, rest.shape, 1)
            keep = (lane >= 3 * rem) & (lane < 4 * rem)
            rests = [
                jnp.where(keep, pltpu.roll(rest, (3 - j) * rem, 1), 0.0) for j in range(3)
            ]
        else:
            rests = [jnp.zeros_like(rest)] * 3
        outer = jnp.concatenate([rests[0], outer_inner[:, 0:main]], axis=1)
        inner = jnp.concatenate([rests[1], outer_inner[:, main:]], axis=1)
        value = jnp.concatenate([rests[2], value_rest[:, 0:main]], axis=1)
        gated = inner * value
        token = lax.broadcasted_iota(jnp.int32, gated.shape, 0)
        conv = jnp.zeros_like(gated)
        for j in range(CONV_K):
            back = CONV_K - 1 - j
            moved = gated
            if back:
                moved = jnp.where(token >= back, pltpu.roll(gated, back, 0), 0.0)
            conv = conv + taps_ref[j : j + 1, :] * moved
        hidden[...] = swapped((outer * conv).astype(BF16)).reshape(hidden.shape)

    def mixer_block(b):
        acc[b] = lax.dot_general(hidden[b], g4[:, main:], NT, preferred_element_type=F32)

    def last_chunk(b):
        ffn_block(nff - 1, b, nff == 1)

    def second(b):
        acc[b] = jnp.zeros(acc.shape[1:], F32)

        def again(k, carry):
            ffn_block(k, b, False)
            return carry

        lax.fori_loop(0, nff, again, 0)

    for k in range(nff + 2):
        for owner, copy in local:
            if owner == k:
                copy.wait()
        if k < 2:
            own(k)
    norm_to(stream_ref, 0)
    for k in range(nff):
        zsteps(k)
        if k + 2 <= K3:
            own(k + 2)
        if k + 2 == K3:
            across(K4, z, go)
        if k > 0:
            wait_across(k - 1)
            ffn_chunk(k - 1, k == 1)
    zsteps(K3)
    start_a()
    steps_a(True)
    wait_across(nff - 1)
    reduce(0, last_chunk, stream_ref, 1, 0.5)
    norm_to(res.at[0], 2)
    wait_across(K3)
    steps_a(False)
    mixer()
    reduce(1, mixer_block, res.at[0], 3, 1.0)
    norm_to(res.at[1], 4)
    reduce(2, second, res.at[1], 5, 0.5)
    out_ref[...] = res[2]

    def done(copy):
        copy.wait_send()

    for k in range(nff + 1):
        def drain(s, carry):
            @pl.when(s <= z)
            def _():
                right(k, s, done)

            @pl.when(s >= z)
            def _():
                left(k, s, done)

            across(k, s, done)
            return carry

        lax.fori_loop(0, Z, drain, 0)
    across(K4, z, done)

    def drain_a(s, carry):
        @pl.when(s <= z)
        def _():
            right_a(s, done)

        @pl.when(s >= z)
        def _():
            left_a(s, done)

        return carry

    lax.fori_loop(0, Z, drain_a, 0)


def stream_kernel(cfg, *refs):
    Z, shard, part, width, hc, nff, main, rem, grp = cfg
    own_refs = refs[:7]
    stream_ref, gains_ref, taps_ref, out_ref = refs[7:11]
    (ff, g3, gv, gb, pr, edge, xt, gains_in, taps_in, gtmp, gcol, gains, tbuf, normed, hid, mixed,
     part_buf, crecv, xsend, xrecv, tot, res, fd, acc,
     lsem, zsend, recv, psend, precv, pysend, pyrecv, csem, xsem, tsem,
     dsem, hsem) = refs[11:]
    Y = 2
    n_fs = Z * Y
    rows = normed.shape[0]
    Dp = n_fs * shard
    groups = 128 // 32
    pair = Y * shard
    last, K3, KB = nff - 1, nff + 1, nff + 2
    f, t = lax.axis_index("fs"), lax.axis_index("tp")
    z, y = f // Y, f % Y
    c, x = t % 2, t // 2
    core_peer = (f, x * 2 + 1 - c)
    x_peer = (f, (1 - x) * 2 + c)
    x_other = (f, (1 - x) * 2 + 1 - c)
    dev_y = (z * Y + (1 - y), t)

    def dev_z(zz):
        return (zz * Y + y, t)

    own_row = pl.multiple_of(f * shard, 16)
    here = pl.ds(own_row, part)
    lead = pl.ds(0, main)
    gate, up, down, ow, iw, vw, mw = own_refs
    moves = []
    for k in range(nff):
        moves.append((0, down.at[:, pl.ds(k * hc, hc)], ff.at[k, here, pl.ds(2 * hc, hc)]))
    for k in range(nff):
        for j, w in enumerate((gate, up)):
            moves.append((k + 1, w.at[:, pl.ds(k * hc, hc)], ff.at[k, here, pl.ds(j * hc, hc)]))
    moves.append((K3, ow.at[:, lead], g3.at[here, lead]))
    moves.append((K3, iw.at[:, lead], g3.at[here, pl.ds(main, main)]))
    moves.append((K3, vw.at[:, lead], gv.at[here, lead]))
    moves.append((K3, mw.at[:, lead], gb.at[here, :]))
    for j, w in enumerate((ow, iw, vw, mw)):
        moves.append((K3 + 1, w, edge.at[j]))
    moves.append((K3 + 2, gains_ref, gains_in))
    moves.append((K3 + 2, taps_ref, taps_in))
    for s in range(n_fs):
        moves.append((K3 + 2, stream_ref.at[pl.ds(s * part, part)], xt.at[pl.ds(s * shard, part)]))
    local = [
        (k, pltpu.make_async_copy(src, dst, lsem.at[n])) for n, (k, src, dst) in enumerate(moves)
    ]

    def pads(count):
        return [pl.ds(s * shard + part, shard - part) for s in range(count)]

    def clear(ref, index):
        ref[index] = jnp.zeros(ref.at[index].shape, ref.dtype)

    def clear_pairs():
        for pad in pads(n_fs):
            clear(ff, (last, pad, pl.ds(0, hc)))
            clear(gv, (pad, lead))
            clear(gb, (pad,))

    def clear_rest():
        for pad in pads(n_fs):
            for k in range(nff):
                clear(ff, (k, pad, pl.ds(0 if k < last else hc, 3 * hc if k < last else 2 * hc)))
            clear(g3, (pad,))
            clear(gv, (pad, pl.ds(main, 128)))
            clear(xt, (pad,))
        for pad in pads(Z):
            for i in range(1, 4):
                for k in range(nff):
                    clear(fd, (i, k, pad))

    for owner, copy in local:
        if owner < 2:
            copy.start()
    clear_pairs()
    barrier = pltpu.get_barrier_semaphore()

    def greet(d):
        pl.semaphore_signal(barrier, inc=1, device_id=d, device_id_type=MESH)

    for d in (core_peer, x_peer, x_other, dev_y):
        greet(d)

    @pl.when(z > 0)
    def _():
        greet(dev_z(z - 1))

    @pl.when(z < Z - 1)
    def _():
        greet(dev_z(z + 1))

    for owner, copy in local:
        if owner >= 2:
            copy.start()
    clear_rest()
    peers = 4 + (z > 0).astype(jnp.int32) + (z < Z - 1).astype(jnp.int32)
    pl.semaphore_wait(barrier, peers)

    def local_wait(k):
        for owner, copy in local:
            if owner == k:
                copy.wait()

    def remote(k, s, way, d):
        slot = s // Y + (0, 1, Z + 1)[way]
        at = pl.ds(pl.multiple_of(s * shard, 16), part)
        if k == 0:
            ref = ff.at[:, at, 2 * hc : 3 * hc]
        elif k <= last:
            ref = ff.at[k - 1, at, 0 : 2 * hc]
        elif k == nff:
            ref = ff.at[last, at, hc : 2 * hc]
        else:
            ref = (g3 if k == K3 else gb).at[at]
        return pltpu.make_async_remote_copy(
            src_ref=ref, dst_ref=ref, send_sem=zsend.at[k, slot], recv_sem=recv.at[k, s],
            device_id=d, device_id_type=MESH,
        )

    def right(k, s, act):
        @pl.when(z < Z - 1)
        def _():
            act(remote(k, s * Y + y, 0, dev_z(z + 1)))

    def left(k, s, act):
        @pl.when(z > 0)
        def _():
            act(remote(k, s * Y + y, 1, dev_z(z - 1)))

    def across(k, s, act):
        act(remote(k, s * Y + y, 2, dev_y))

    def go(copy):
        copy.start()

    near = jnp.minimum(z, Z - 1 - z)
    low = z <= Z - 1 - z
    at_end = (z == 0) | (z == Z - 1)

    def inward(go_right, go_left):
        @pl.when(low)
        def _():
            go_right()

        @pl.when(~low)
        def _():
            go_left()

    def own_in(k):
        inward(lambda: right(k, z, go), lambda: left(k, z, go))

    def own_out(k):
        inward(lambda: left(k, z, go), lambda: right(k, z, go))

    def own_y(k):
        across(k, z, go)

    def down_copy(kind, s, v):
        to = (core_peer, x_peer, x_other)[kind]
        return pltpu.make_async_remote_copy(
            src_ref=ff.at[:, pl.ds(pl.multiple_of((s * Y + v) * shard, 16), part), 2 * hc : 3 * hc],
            dst_ref=fd.at[kind + 1, :, pl.ds(pl.multiple_of(s * shard, 16), part)],
            send_sem=dsem.at[0, kind, s], recv_sem=dsem.at[1, kind, s],
            device_id=to, device_id_type=MESH,
        )

    def spread(s, v, act):
        @pl.when(v == c)
        def _():
            act(down_copy(1, s, v))

        @pl.when(v != c)
        def _():
            act(down_copy(2, s, v))
            act(down_copy(0, s, v))

    def zsteps(k):
        def step(i, carry):
            @pl.when(z - 1 - i >= 0)
            def _():
                s = z - 1 - i
                remote(k, s * Y + y, 0, dev_z(z - 1)).wait_recv()
                right(k, s, go)
                across(k, s, go)
                if k == 0:
                    spread(s, y, go)

            @pl.when(z + 1 + i < Z)
            def _():
                s = z + 1 + i
                remote(k, s * Y + y, 0, dev_z(z + 1)).wait_recv()
                left(k, s, go)
                across(k, s, go)
                if k == 0:
                    spread(s, y, go)

            return carry

        lax.fori_loop(0, Z - 1, step, 0)

    def wait_across(k):
        def step(s, carry):
            remote(k, s * Y + 1 - y, 2, dev_y).wait_recv()
            return carry

        lax.fori_loop(0, Z, step, 0)

    def piece(q, first, count):
        if q == 2:
            return pr.at[pl.ds(pl.multiple_of(first * grp, 16), count * grp)]
        at = pl.ds(pl.multiple_of(first * shard, 16), (count - 1) * shard + part)
        return gv.at[at, lead] if q == 1 else ff.at[last, at, 0:hc]

    def across_p(q, s):
        ref = piece(q, s, 1)
        return pltpu.make_async_remote_copy(
            src_ref=ref, dst_ref=ref, send_sem=pysend.at[q], recv_sem=pyrecv.at[q],
            device_id=dev_y, device_id_type=MESH,
        )

    def remote_p(q, s, way, d):
        ref = piece(q, s * Y, Y)
        return pltpu.make_async_remote_copy(
            src_ref=ref, dst_ref=ref, send_sem=psend.at[q, s + way], recv_sem=precv.at[q, s],
            device_id=d, device_id_type=MESH,
        )

    def right_p(q, s, act):
        @pl.when(z < Z - 1)
        def _():
            act(remote_p(q, s, 0, dev_z(z + 1)))

    def left_p(q, s, act):
        @pl.when(z > 0)
        def _():
            act(remote_p(q, s, 1, dev_z(z - 1)))

    def start_in(q):
        across_p(q, z * Y + 1 - y).wait_recv()
        inward(lambda: right_p(q, z, go), lambda: left_p(q, z, go))

    def start_out(q):
        inward(lambda: left_p(q, z, go), lambda: right_p(q, z, go))

    def steps_p(qs, forward, first=0):
        def step(i, carry):
            @pl.when((z - 1 - i >= 0) & ((z < Z - 1) if forward else (z == Z - 1)))
            def _():
                s = z - 1 - i
                for q in qs:
                    remote_p(q, s, 0, dev_z(z - 1)).wait_recv()
                    if forward:
                        right_p(q, s, go)

            @pl.when((z + 1 + i < Z) & ((z > 0) if forward else (z == 0)))
            def _():
                s = z + 1 + i
                for q in qs:
                    remote_p(q, s, 0, dev_z(z + 1)).wait_recv()
                    if forward:
                        left_p(q, s, go)

            return carry

        lax.fori_loop(first, Z - 1, step, 0)

    beside = jnp.where(low, 1, Z - 2)

    def value_z(d):
        ref = piece(1, beside * Y + y, 1)
        return pltpu.make_async_remote_copy(
            src_ref=ref, dst_ref=ref, send_sem=psend.at[1, jnp.where(low, beside + 1, beside)],
            recv_sem=precv.at[1, beside], device_id=d, device_id_type=MESH,
        )

    def value_y(column):
        ref = piece(1, beside * Y + column, 1)
        return pltpu.make_async_remote_copy(
            src_ref=ref, dst_ref=ref, send_sem=pysend.at[3], recv_sem=pyrecv.at[3],
            device_id=dev_y, device_id_type=MESH,
        )

    def to_end():
        return dev_z(jnp.where(low, 0, Z - 1))

    def pack_edges():
        packed = jnp.zeros((grp, 128), F32)
        for j in range(groups):
            count = min(grp, part - j * grp)
            if count <= 0:
                continue
            block = jnp.zeros((count, 128), F32)
            row = lax.broadcasted_iota(jnp.int32, (rem, 128), 0)
            lane = lax.broadcasted_iota(jnp.int32, (rem, 128), 1)
            for k in range(4):
                place = jnp.where(lane == row + (32 * j + rem * k), 1.0, 0.0).astype(BF16)
                source = edge[k, j * grp : j * grp + count, main : main + rem]
                block = block + jnp.dot(source, place, preferred_element_type=F32)
            if count < grp:
                block = jnp.concatenate([block, jnp.zeros((grp - count, 128), F32)], axis=0)
            packed = packed + block
        pr[pl.ds(pl.multiple_of(f * grp, 16), grp)] = packed.astype(BF16)

    def unpack_edges():
        row = lax.broadcasted_iota(jnp.int32, (128, 128), 0)
        lane = lax.broadcasted_iota(jnp.int32, (128, 128), 1)

        def unpack(s):
            packed = pr[pl.ds(pl.multiple_of(s * grp, 16), grp)]
            for j in range(groups):
                count = min(grp, shard - j * grp)
                if count <= 0:
                    continue
                pick = jnp.where((lane < 32) & (row == lane + 32 * j), 1.0, 0.0).astype(BF16)
                block = jnp.dot(packed, pick, preferred_element_type=F32)[:count]
                at = pl.ds(pl.multiple_of(s * shard + j * grp, 16), count)
                gv[at, main : main + 128] = block.astype(BF16)

        def body(i, carry):
            j = order(i)

            @pl.when(at_end & (i > 0))
            def _():
                remote_p(2, j, 0, toward()).wait_recv()

            for v in range(Y):
                unpack(j * Y + v)
            return carry

        lax.fori_loop(0, Z, body, 0)

    def prepare_gains():
        gtmp[...] = jnp.zeros(gtmp.shape, F32)
        gtmp[0:6, 0:width] = gains_in[...]
        for i in range(gtmp.shape[1] // 128):
            gcol[i * 128 : (i + 1) * 128] = gtmp[:, i * 128 : (i + 1) * 128].T

        def body(s, carry):
            for j in range(6):
                column = gcol[pl.ds(pl.multiple_of(s * part, 8), part), j : j + 1]
                at = pl.ds(pl.multiple_of(s * shard, 16), part)
                gains[j, at] = jnp.broadcast_to(column, (part, 128))
                pad = pl.ds(pl.multiple_of(s * shard + part, 8), shard - part)
                gains[j, pad] = jnp.zeros((shard - part, 128), F32)
            return carry

        lax.fori_loop(0, n_fs, body, 0)

    def prepare_taps():
        n_tp = lax.axis_size("tp")
        channels = taps_in.shape[1] // n_tp
        lanes = tbuf.shape[1]
        tbuf[...] = jnp.zeros(tbuf.shape, F32)
        tbuf[0:CONV_K, 0 : taps_in.shape[1]] = taps_in[...].astype(F32)
        full = tbuf[...]
        mine = full
        for i in range(1, n_tp):
            mine = jnp.where(t == i, pltpu.roll(full, lanes - channels * i, 1), mine)
        tbuf[:, 0:main] = mine[:, 0:main]
        rest = pltpu.roll(mine[:, main : main + 128], 3 * rem, 1)
        lane = lax.broadcasted_iota(jnp.int32, rest.shape, 1)
        tbuf[:, main : main + 128] = jnp.where((lane >= 3 * rem) & (lane < 4 * rem), rest, 0.0)

    BLK = 128
    nblk = Dp // BLK

    def squares(v):
        return jnp.sum((v * v).reshape(v.shape[0] // 8, 8, rows), axis=0)

    def block_at(i):
        return pl.ds(pl.multiple_of(i * BLK, BLK), BLK)

    def inverse(sums):
        return lax.rsqrt(jnp.sum(sums, axis=0, keepdims=True) * (1.0 / width) + EPSILON)

    def gain_block(row, at):
        g = gains[row, at]
        return jnp.concatenate([g] * (rows // 128), axis=1)

    def sum_squares(source):
        def body(i, sums):
            return sums + squares(source[block_at(i)].astype(F32))

        return lax.fori_loop(0, nblk, body, jnp.zeros((8, rows), F32))

    def norm_to(source, sums, row):
        scale = inverse(sums)

        def body(i, carry):
            at = block_at(i)
            v = source[at].astype(F32) * scale * gain_block(row, at)
            normed[:, at] = v.T.astype(BF16)
            return carry

        lax.fori_loop(0, nblk, body, 0)

    def update(r, sums, source, row, factor):
        scale = inverse(sums) * factor

        def body(i, sums):
            at = block_at(i)
            v = source[at].astype(F32) + tot[r, at].astype(F32) * scale * gain_block(row, at)
            v = v.astype(BF16)
            res[r, at] = v
            return sums + squares(v.astype(F32))

        return lax.fori_loop(0, nblk, body, jnp.zeros((8, rows), F32))

    def hidden_copy(u, kind, k):
        source = hid.at[u, 2 if kind == 2 else 0, k]
        return pltpu.make_async_remote_copy(
            src_ref=source, dst_ref=hid.at[u, kind + 1, k], send_sem=hsem.at[0, kind, k],
            recv_sem=hsem.at[1, kind, k], device_id=x_peer if kind == 1 else core_peer,
            device_id_type=MESH,
        )

    def hidden(u, k):
        n = normed[...]
        gate_v = jnp.dot(n, ff[k, :, 0:hc], preferred_element_type=F32)
        up_v = jnp.dot(n, ff[k, :, hc : 2 * hc], preferred_element_type=F32)
        hid[u, 0, k] = (gate_v / (1.0 + jnp.exp(-gate_v)) * up_v).astype(BF16)
        hidden_copy(u, 1, k).start()
        hidden_copy(u, 0, k).start()

    def hidden_sent(u):
        for kind in range(3):
            for k in range(nff):
                hidden_copy(u, kind, k).wait_send()

    def product(u, i, k, at):
        return lax.dot_general(fd[i, k, at], hid[u, i, k], NT, preferred_element_type=F32)

    def keep_down():
        def body(s, carry):
            at = pl.ds(pl.multiple_of(s * shard, 16), shard)
            for k in range(nff):
                fd[0, k, at] = ff[
                    k, pl.ds(pl.multiple_of((s * Y + c) * shard, 16), shard), 2 * hc : 3 * hc
                ]
            return carry

        lax.fori_loop(0, Z, body, 0)

    def finish_ffn(u, r, hook, idle):
        def rows_of(j):
            return pl.ds(pl.multiple_of(j * shard, 16), shard)

        def own_part(j, carry):
            at = rows_of(j)
            total = product(u, 0, 0, at)
            for k in range(1, nff):
                total = total + product(u, 0, k, at)
            acc[at] = total
            return carry

        def add(i, ks):
            def body(j, carry):
                at = rows_of(j)
                total = acc[at]
                for k in ks:
                    total = total + product(u, i, k, at)
                acc[at] = total
                return carry

            lax.fori_loop(0, Z, body, 0)

        lax.fori_loop(0, Z, own_part, 0)
        for k in range(nff):
            hidden_copy(u, 0, k).wait_recv()
        add(1, range(nff))
        if idle:
            idle()
        for k in range(nff):
            hidden_copy(u, 1, k).wait_recv()
            hidden_copy(u, 2, k).start()
            if k > 0:
                hidden_copy(u, 2, k - 1).wait_recv()
                add(3, (k - 1,))
            add(2, (k,))
        if hook:
            hook()
        hidden_copy(u, 2, last).wait_recv()

        def final(j, sums):
            at = rows_of(j)
            v = (acc[at] + product(u, 3, last, at)).astype(BF16)
            tot[r, column(j, c)] = v
            tot_copy(r, j).start()
            return sums + squares(v.astype(F32))

        return both_squares(r, lax.fori_loop(0, Z, final, jnp.zeros((8, rows), F32)), lambda j: j)

    def pair_at(j):
        return pl.ds(pl.multiple_of(j * pair, 16), pair)

    def mixer_pair(r, j):
        remote(KB, j * Y + 1 - y, 2, dev_y).wait_recv()
        at = pair_at(j)
        total = lax.dot_general(gb[at], mixed[:, 0:main], NT, preferred_element_type=F32)
        total = total + lax.dot_general(
            gv[at, main : main + 128], mixed[:, main:], NT, preferred_element_type=F32
        )
        part_buf[j] = total.astype(BF16)

    mine = pl.ds(pl.multiple_of(c * shard, 16), shard)
    other = pl.ds(pl.multiple_of((1 - c) * shard, 16), shard)

    def core_copy(r, j):
        return pltpu.make_async_remote_copy(
            src_ref=part_buf.at[j, other], dst_ref=crecv.at[j], send_sem=csem.at[0, j],
            recv_sem=csem.at[1, j], device_id=core_peer, device_id_type=MESH,
        )

    def x_copy(r, j):
        return pltpu.make_async_remote_copy(
            src_ref=xsend.at[j], dst_ref=xrecv.at[j], send_sem=xsem.at[0, j],
            recv_sem=xsem.at[1, j], device_id=x_peer, device_id_type=MESH,
        )

    def column(j, v):
        return pl.ds(pl.multiple_of(j * pair + v * shard, 16), shard)

    def both_squares(r, mine_sums, at):
        def arrive(s, sums):
            tot_copy(r, at(s)).wait()
            return sums + squares(tot[r, column(at(s), 1 - c)].astype(F32))

        return mine_sums + lax.fori_loop(0, Z, arrive, jnp.zeros((8, rows), F32))

    def tot_copy(r, j):
        at = column(j, c)
        return pltpu.make_async_remote_copy(
            src_ref=tot.at[r, at], dst_ref=tot.at[r, at], send_sem=tsem.at[0, j],
            recv_sem=tsem.at[1, j], device_id=core_peer, device_id_type=MESH,
        )

    def toward():
        return dev_z(jnp.where(z == 0, z + 1, z - 1))

    def order(s):
        step = (s + 1) // 2
        close = jnp.where(s % 2 == 1, z - step, z + step)
        return jnp.where(s <= 2 * near, close, jnp.where(low, s, Z - 1 - s))

    def pass_on(j):
        remote(KB, j * Y + y, 0, toward()).wait_recv()
        across(KB, j, go)

    def end_steps(first, stop):
        source = toward()

        def step(s, carry):
            j = order(s)
            remote(K3, j * Y + y, 0, source).wait_recv()
            across(K3, j, go)
            return carry

        @pl.when(at_end)
        def _():
            lax.fori_loop(first, stop, step, 0)

    def reduce(r, compute):
        def cross(j):
            core_copy(r, j).wait_recv()
            xsend[j] = (part_buf[j, mine].astype(F32) + crecv[j].astype(F32)).astype(BF16)
            x_copy(r, j).start()

        def send(s, carry):
            j = order(s)
            @pl.when(at_end & (s > 0) & (s < Z - 1))
            def _():
                pass_on(order(s + 1))

            compute(r, j)
            core_copy(r, j).start()

            @pl.when(s > 0)
            def _():
                cross(order(s - 1))

            return carry

        def receive(s, sums):
            j = order(s)
            x_copy(r, j).wait_recv()
            v = (xsend[j].astype(F32) + xrecv[j].astype(F32)).astype(BF16)
            tot[r, column(j, c)] = v
            tot_copy(r, j).start()
            return sums + squares(v.astype(F32))

        lax.fori_loop(0, Z, send, 0)
        cross(order(Z - 1))
        return both_squares(r, lax.fori_loop(0, Z, receive, jnp.zeros((8, rows), F32)), order)

    def mixer():
        n = normed[...]
        outer_inner = jnp.dot(n, g3[...], preferred_element_type=F32)
        outer_inner = outer_inner.astype(BF16).astype(F32)
        value_rest = jnp.dot(n, gv[...], preferred_element_type=F32)
        value_rest = value_rest.astype(BF16).astype(F32)

        @pl.when(at_end)
        def _():
            pass_on(order(1))

        rest = value_rest[:, main:]
        lane = lax.broadcasted_iota(jnp.int32, rest.shape, 1)
        keep = (lane >= 3 * rem) & (lane < 4 * rem)
        rests = [jnp.where(keep, pltpu.roll(rest, (3 - j) * rem, 1), 0.0) for j in range(3)]
        parts = [
            (outer_inner[:, 0:main], outer_inner[:, main:], value_rest[:, 0:main], 0),
            (rests[0], rests[1], rests[2], main),
        ]
        for outer, inner, value, first in parts:
            lanes = outer.shape[1]
            gated = inner * value
            token = lax.broadcasted_iota(jnp.int32, gated.shape, 0)
            conv = jnp.zeros_like(gated)
            for j in range(CONV_K):
                back = CONV_K - 1 - j
                moved = gated
                if back:
                    moved = jnp.where(token >= back, pltpu.roll(gated, back, 0), 0.0)
                conv = conv + tbuf[j : j + 1, first : first + lanes] * moved
            mixed[:, first : first + lanes] = (outer * conv).astype(BF16)

    def drain_all():
        def done(copy):
            copy.wait_send()

        for k in range(nff + 3):
            def drain(s, carry):
                @pl.when(s <= z)
                def _():
                    right(k, s, done)

                @pl.when(s >= z)
                def _():
                    left(k, s, done)

                across(k, s, done)
                return carry

            lax.fori_loop(0, Z, drain, 0)
        for q in range(3):
            def drain_p(s, carry):
                alone = (s == z) & ~at_end if q == 1 else s < 0

                @pl.when((s <= z) & ~(alone & ~low))
                def _():
                    right_p(q, s, done)

                @pl.when((s >= z) & ~(alone & low))
                def _():
                    left_p(q, s, done)

                return carry

            lax.fori_loop(0, Z, drain_p, 0)
            across_p(q, f).wait_send()

        @pl.when(at_end)
        def _():
            value_y(y).wait_send()

        @pl.when(~at_end)
        def _():
            value_z(to_end()).wait_send()

        def drain_r(s, carry):
            core_copy(1, s).wait_send()
            x_copy(1, s).wait_send()
            for v in range(Y):
                spread(s, v, done)
            return carry

        lax.fori_loop(0, Z, drain_r, 0)

    def spread_across(s, carry):
        j = order(s)
        remote(0, j * Y + 1 - y, 2, dev_y).wait_recv()
        spread(j, 1 - y, go)
        return carry

    for k in range(2):
        local_wait(k)
        own_in(k)
        own_out(k)
        own_y(k)
        if k == 0:
            spread(z, y, go)
    local_wait(K3 + 1)
    pack_edges()
    for k in range(2, K3 + 1):
        local_wait(k)
    for q in range(3):
        across_p(q, f).start()

    @pl.when(at_end)
    def _():
        for k in range(2, KB + 1):
            own_in(k)

    own_out(2)
    own_y(2)
    local_wait(K3 + 2)
    prepare_gains()
    prepare_taps()
    norm_to(xt, sum_squares(xt), 0)
    zsteps(0)
    own_out(nff)
    own_y(nff)

    @pl.when(~at_end)
    def _():
        own_in(2)

    start_in(0)
    start_out(0)

    @pl.when(at_end)
    def _():
        for q in range(1, 3):
            start_in(q)

    zsteps(1)
    lax.fori_loop(0, Z // 2, spread_across, 0)

    @pl.when(~at_end)
    def _():
        own_in(nff)

    zsteps(2)
    own_out(K3)

    @pl.when(~at_end)
    def _():
        own_in(K3)
        start_in(1)
        start_in(2)
        own_in(KB)

    lax.fori_loop(Z // 2, Z, spread_across, 0)
    zsteps(nff)
    steps_p((0,), True)
    own_y(K3)
    keep_down()
    wait_across(1)
    hidden(0, 0)

    @pl.when(~at_end)
    def _():
        zsteps(K3)
        value_z(to_end()).start()
        start_out(2)
        steps_p((1, 2), True)
        own_out(KB)
        own_y(KB)
        zsteps(KB)

    wait_across(2)
    hidden(0, 1)

    def down_arrived(s, carry):
        for kind in range(3):
            down_copy(kind, s, c).wait_recv()
        return carry

    end_steps(1, 2)
    lax.fori_loop(0, Z, down_arrived, 0)
    wait_across(nff)
    steps_p((0,), False)
    hidden(0, last)
    sums = finish_ffn(0, 0, lambda: end_steps(2, Z - 1), None)
    norm_to(res.at[0], update(0, sums, xt, 1, 0.5), 2)
    end_steps(Z - 1, Z)

    @pl.when(at_end)
    def _():
        value_z(toward()).wait_recv()
        value_y(y).start()
        own_y(KB)

    hidden_sent(0)
    wait_across(K3)
    unpack_edges()
    steps_p((1,), False, 1)

    @pl.when(at_end)
    def _():
        value_y(1 - y).wait_recv()

    mixer()
    sums = reduce(1, mixer_pair)
    norm_to(res.at[1], update(1, sums, res.at[0], 3, 1.0), 4)

    def again(k, carry):
        hidden(1, k)
        return carry

    lax.fori_loop(0, nff, again, 0)
    scale = inverse(finish_ffn(1, 2, None, drain_all)) * 0.5
    for s in range(n_fs):
        at = pl.ds(s * shard, part)
        v = res[1, at].astype(F32) + tot[2, at].astype(F32) * scale * gain_block(5, at)
        out_ref[s * part : (s + 1) * part] = v.astype(BF16)
    hidden_sent(1)


def stream_form(mesh, Z):
    def local(stream_in, norm_gains, gate, up, down, outer_w, inner_w, value_w, mixer_w, conv_taps):
        rows, width = stream_in.shape
        part, hid = gate.shape
        channels = outer_w.shape[1]
        n_fs = 2 * Z
        shard = -(-part // 16) * 16
        Dp = n_fs * shard
        nff = 3
        hc = hid // nff
        main = channels // 128 * 128
        rem = channels - main
        grp = -(-part // 64) * 16
        lanes = -(-width // 128) * 128
        taps = -(-conv_taps.shape[1] // 128) * 128
        dma, vmem = pltpu.SemaphoreType.DMA, pltpu.VMEM
        out = pl.pallas_call(
            functools.partial(stream_kernel, (Z, shard, part, width, hc, nff, main, rem, grp)),
            out_shape=pltpu.VMEM((width, rows), BF16),
            in_specs=[pl.BlockSpec(memory_space=pl.ANY)] * 10,
            out_specs=pl.BlockSpec(memory_space=pltpu.VMEM),
            scratch_shapes=[
                vmem((nff, Dp, 3 * hc), BF16),
                vmem((Dp, 2 * main), BF16),
                vmem((Dp, main + 128), BF16),
                vmem((Dp, main), BF16),
                vmem((n_fs * grp, 128), BF16),
                vmem((4, part, channels), BF16),
                vmem((Dp, rows), BF16),
                vmem(norm_gains.shape, F32),
                vmem(conv_taps.shape, BF16),
                vmem((128, lanes), F32),
                vmem((lanes, 128), F32),
                vmem((6, Dp, 128), F32),
                vmem((8, taps), F32),
                vmem((rows, Dp), BF16),
                vmem((2, 4, nff, rows, hc), BF16),
                vmem((rows, main + 128), BF16),
                vmem((Z, 2 * shard, rows), BF16),
                vmem((Z, shard, rows), BF16),
                vmem((Z, shard, rows), BF16),
                vmem((Z, shard, rows), BF16),
                vmem((3, Dp, rows), BF16),
                vmem((2, Dp, rows), BF16),
                vmem((4, nff, Z * shard, hc), BF16),
                vmem((Z * shard, rows), F32),
                dma((3 * nff + 10 + n_fs,)),
                dma((nff + 3, 2 * Z + 1)),
                dma((nff + 3, n_fs)),
                dma((4, Z + 1)),
                dma((4, Z)),
                dma((4,)),
                dma((4,)),
                dma((2, Z)),
                dma((2, Z)),
                dma((2, Z)),
                dma((2, 3, Z)),
                dma((2, 3, nff)),
            ],
            compiler_params=pltpu.CompilerParams(
                collective_id=0, has_side_effects=True, vmem_limit_bytes=60 * 1024 * 1024
            ),
        )(gate, up, down, outer_w, inner_w, value_w, mixer_w, stream_in.T, norm_gains, conv_taps)
        return out.T

    return local


def y_count(mesh):
    try:
        found = len({d.coords[1] for d in mesh.devices.reshape(-1)})
    except AttributeError:
        found = 1
    return found if found == 2 and mesh.shape["fs"] % 2 == 0 else 1


def solution(mesh):
    n_fs, n_tp = mesh.shape["fs"], mesh.shape["tp"]
    Y = y_count(mesh)
    Z, X = n_fs // Y, n_tp // 2

    def chain_form(stream_in, norm_gains, gate, up, down, outer_w, inner_w, value_w, mixer_w, conv_taps):
        rows, width = stream_in.shape
        part, hid = gate.shape
        channels = outer_w.shape[1]
        shard = -(-part // 16) * 16
        Dp = n_fs * shard
        nff = 3 if hid % 384 == 0 else 1
        hc = hid // nff
        main = channels // 128 * 128
        rem = channels - main

        def widen(v):
            lead = v.shape[0]
            v = v.reshape(lead, n_fs, part)
            return jnp.pad(v, ((0, 0), (0, 0), (0, shard - part))).reshape(lead, Dp)

        sent = -(-part // 8) * 8

        def pack(w):
            return w if sent == part else jnp.pad(w, ((0, sent - part), (0, 0)))

        rest = [w[:, main:] for w in (outer_w, inner_w, value_w, mixer_w)]
        rest.append(jnp.zeros((part, 128 - 4 * rem), BF16))
        owns = [gate, up, down, outer_w, inner_w, value_w, mixer_w]
        owns = [pack(w) for w in owns + [jnp.concatenate(rest, axis=1)]]
        taps = lax.dynamic_slice_in_dim(
            conv_taps, lax.axis_index("tp") * channels, channels, 1
        ).astype(F32)
        taps = jnp.concatenate(
            [jnp.pad(taps[:, main:], ((0, 0), (3 * rem, 128 - 4 * rem))), taps[:, :main]], axis=1
        )
        half, quarter = rows // 2, rows // 4
        dma, vmem = pltpu.SemaphoreType.DMA, pltpu.VMEM
        out = pl.pallas_call(
            functools.partial(kernel, (Z, Y, X, shard, sent, width, hc, nff, main, rem)),
            out_shape=jax.ShapeDtypeStruct((rows, Dp), BF16),
            in_specs=[pl.BlockSpec(memory_space=pl.ANY)] * 8
            + [pl.BlockSpec(memory_space=pltpu.VMEM)] * 3,
            out_specs=pl.BlockSpec(memory_space=pltpu.VMEM),
            scratch_shapes=[
                vmem((nff, Dp, 3 * hc), BF16),
                vmem((Dp, 2 * main), BF16),
                vmem((Dp, 2 * main + 128), BF16),
                vmem((2, half, Dp), BF16),
                vmem((2, half, Dp), F32),
                vmem((2, half, main + 128), BF16),
                vmem((3, 2, quarter, Dp), BF16),
                vmem((3, 2, quarter, Dp), BF16),
                vmem((3, 2, quarter, Dp), BF16),
                vmem((3, 2, X - 1, quarter, Dp), BF16),
                vmem((3, rows, Dp), BF16),
                dma((3 * nff + 5,)),
                dma((nff + 2, 3, n_fs)),
                dma((nff + 2, n_fs)),
                dma((2, Z)),
                dma((Z,)),
                dma((2, 3, 2)),
                dma((3, 2, X - 1)),
                dma((3, 2, X - 1)),
                dma((2, 3, 2)),
            ],
            compiler_params=pltpu.CompilerParams(
                collective_id=0, has_side_effects=True, vmem_limit_bytes=60 * 1024 * 1024
            ),
        )(*owns, widen(stream_in), widen(norm_gains), taps)
        return out.reshape(rows, n_fs, shard)[:, :, :part].reshape(rows, width)

    def local(*args):
        rows, width = args[0].shape
        part, channels = args[5].shape
        rem = channels % 128
        fits = Y == 2 and X == 2 and part % 8 == 0 and 0 < rem <= 8 and rows % 128 == 0
        fits = fits and (n_fs * (-(-part // 16) * 16)) % 128 == 0 and channels > 128
        fits = fits and args[2].shape[1] % 384 == 0 and Z == 4
        return (stream_form(mesh, Z) if fits else chain_form)(*args)

    return jax.shard_map(
        local,
        mesh=mesh,
        in_specs=(P("fs", None), P()) + (P("fs", "tp"),) * 7 + (P(),),
        out_specs=P("fs", None),
        check_vma=False,
    )
```

```python
import functools

import jax
import jax.numpy as jnp
from jax import lax
from jax.experimental import pallas as pl
from jax.experimental.pallas import tpu as pltpu
from jax.sharding import PartitionSpec as P

MESH = pl.DeviceIdType.MESH
EPSILON = 1e-06
CONV_K = 3
F32, BF16 = jnp.float32, jnp.bfloat16
NT = (((1,), (1,)), ((), ()))


def kernel(cfg, *refs):
    Z, Y, X, shard, sent, width, hc, nff, main, rem = cfg
    own_refs = refs[:8]
    stream_ref, gains_ref, taps_ref, out_ref = refs[8:12]
    (ff, g3, g4, normed, acc, hidden, csend, crecv, xsend, xrecv, res,
     lsem, zsend, recv, asend, arecv, csem, xssem, xrsem, rsem) = refs[12:]
    rows, Dp = stream_ref.shape
    half, quarter = rows // 2, rows // 4
    K3, K4 = nff, nff + 1
    f, t = lax.axis_index("fs"), lax.axis_index("tp")
    z, y = f // Y, f % Y
    c, x = t % 2, t // 2
    core_peer = (f, x * 2 + 1 - c)
    x_peers = [(f, ((x + j) % X) * 2 + c) for j in range(1, X)]

    def dev_z(zz):
        return (zz * Y + y, t)

    dev_y = (z * Y + (Y - 1 - y), t)

    for s in range(Z * Y):
        tail = pl.ds(s * shard + shard - 16, 16)
        for k in range(nff):
            ff[k, tail] = jnp.zeros((16, 3 * hc), BF16)
        g3[tail] = jnp.zeros((16, 2 * main), BF16)
        g4[tail] = jnp.zeros((16, 2 * main + 128), BF16)

    barrier = pltpu.get_barrier_semaphore()

    def greet(d):
        pl.semaphore_signal(barrier, inc=1, device_id=d, device_id_type=MESH)

    always = [core_peer] + x_peers + ([dev_y] if Y == 2 else [])
    for d in always:
        greet(d)
    if Z > 1:
        @pl.when(z > 0)
        def _():
            greet(dev_z(z - 1))

        @pl.when(z < Z - 1)
        def _():
            greet(dev_z(z + 1))

    def slot(k, first, count):
        at = pl.ds(pl.multiple_of(first * shard, 16), (count - 1) * shard + sent)
        if k < nff:
            return ff.at[k, at]
        return (g3 if k == K3 else g4).at[at]

    here = pl.ds(pl.multiple_of(f * shard, 16), sent)
    moves = []
    for k in range(nff):
        for j in range(3):
            moves.append((k, own_refs[j].at[:, pl.ds(k * hc, hc)],
                          ff.at[k, here, pl.ds(j * hc, hc)]))
    ow, iw, vw, mw, rw = own_refs[3:]
    lead = pl.ds(0, main)
    moves.append((K3, ow.at[:, lead], g3.at[here, lead]))
    moves.append((K3, iw.at[:, lead], g3.at[here, pl.ds(main, main)]))
    moves.append((K4, vw.at[:, lead], g4.at[here, lead]))
    moves.append((K4, rw, g4.at[here, pl.ds(main, 128)]))
    moves.append((K4, mw.at[:, lead], g4.at[here, pl.ds(main + 128, main)]))
    local = [
        (k, pltpu.make_async_copy(src, dst, lsem.at[n])) for n, (k, src, dst) in enumerate(moves)
    ]
    for _, copy in local:
        copy.start()

    peers = len(always)
    if Z > 1:
        peers = peers + (z > 0).astype(jnp.int32) + (z < Z - 1).astype(jnp.int32)
    pl.semaphore_wait(barrier, peers)

    def remote(k, s, way, d):
        ref = slot(k, s, 1)
        return pltpu.make_async_remote_copy(
            src_ref=ref, dst_ref=ref, send_sem=zsend.at[k, way, s], recv_sem=recv.at[k, s],
            device_id=d, device_id_type=MESH,
        )

    def remote_a(s, way, d):
        ref = slot(K4, s * Y, Y)
        return pltpu.make_async_remote_copy(
            src_ref=ref, dst_ref=ref, send_sem=asend.at[way, s], recv_sem=arecv.at[s],
            device_id=d, device_id_type=MESH,
        )

    def right(k, s, act):
        @pl.when(z < Z - 1)
        def _():
            act(remote(k, s * Y + y, 0, dev_z(z + 1)))

    def left(k, s, act):
        @pl.when(z > 0)
        def _():
            act(remote(k, s * Y + y, 1, dev_z(z - 1)))

    def across(k, s, act):
        if Y == 2:
            act(remote(k, s * Y + y, 2, dev_y))

    def go(copy):
        copy.start()

    def own(k):
        right(k, z, go)
        left(k, z, go)
        across(k, z, go)

    def zsteps(k):
        def step(i, carry):
            @pl.when(z - 1 - i >= 0)
            def _():
                s = z - 1 - i
                remote(k, s * Y + y, 0, dev_z(z - 1)).wait_recv()
                right(k, s, go)
                across(k, s, go)

            @pl.when(z + 1 + i < Z)
            def _():
                s = z + 1 + i
                remote(k, s * Y + y, 0, dev_z(z + 1)).wait_recv()
                left(k, s, go)
                across(k, s, go)

            return carry

        lax.fori_loop(0, Z - 1, step, 0)

    def wait_across(k):
        if Y == 2:
            def step(s, carry):
                remote(k, s * Y + 1 - y, 2, dev_y).wait_recv()
                return carry

            lax.fori_loop(0, Z, step, 0)

    def right_a(s, act):
        @pl.when(z < Z - 1)
        def _():
            act(remote_a(s, 0, dev_z(z + 1)))

    def left_a(s, act):
        @pl.when(z > 0)
        def _():
            act(remote_a(s, 1, dev_z(z - 1)))

    def start_a():
        if Y == 2:
            remote(K4, z * Y + 1 - y, 2, dev_y).wait_recv()
        right_a(z, go)
        left_a(z, go)

    def steps_a(forward):
        def step(i, carry):
            @pl.when((z - 1 - i >= 0) & ((z < Z - 1) if forward else (z == Z - 1)))
            def _():
                s = z - 1 - i
                remote_a(s, 0, dev_z(z - 1)).wait_recv()
                if forward:
                    right_a(s, go)

            @pl.when((z + 1 + i < Z) & ((z > 0) if forward else (z == 0)))
            def _():
                s = z + 1 + i
                remote_a(s, 0, dev_z(z + 1)).wait_recv()
                if forward:
                    left_a(s, go)

            return carry

        lax.fori_loop(0, Z - 1, step, 0)

    def scaled(values, row):
        mean = jnp.sum(values * values, axis=-1, keepdims=True) * (1.0 / width)
        return values * lax.rsqrt(mean + EPSILON) * gains_ref[row : row + 1, :]

    def norm_to(source, row):
        def block(i, carry):
            at = pl.ds(pl.multiple_of(i * 32, 32), 32)
            per_half, per_quarter = half // 32, quarter // 32
            h, b = i // per_half, (i % per_half) // per_quarter
            to = pl.ds(pl.multiple_of(h * quarter + (i % per_quarter) * 32, 32), 32)
            normed[b, to] = scaled(source[at].astype(F32), row).astype(BF16)
            return carry

        lax.fori_loop(0, rows // 32, block, 0)

    def ffn_block(k, b, first):
        weights = ff.at[k]
        n = normed[b]
        gate = jnp.dot(n, weights[:, 0:hc], preferred_element_type=F32)
        up = jnp.dot(n, weights[:, hc : 2 * hc], preferred_element_type=F32)
        h = (gate / (1.0 + jnp.exp(-gate)) * up).astype(BF16)
        part = lax.dot_general(h, weights[:, 2 * hc :], NT, preferred_element_type=F32)
        acc[b] = part if first else acc[b] + part

    def ffn_chunk(k, first):
        def block(b, carry):
            ffn_block(k, b, first)
            return carry

        lax.fori_loop(0, 2, block, 0)

    mine = pl.ds(pl.multiple_of(c * quarter, 16), quarter)
    other = pl.ds(pl.multiple_of((1 - c) * quarter, 16), quarter)

    def core_copy(r, b):
        return pltpu.make_async_remote_copy(
            src_ref=csend.at[r, b], dst_ref=crecv.at[r, b], send_sem=csem.at[0, r, b],
            recv_sem=csem.at[1, r, b], device_id=core_peer, device_id_type=MESH,
        )

    def x_copy(r, b, j):
        return pltpu.make_async_remote_copy(
            src_ref=xsend.at[r, b], dst_ref=xrecv.at[r, b, j], send_sem=xssem.at[r, b, j],
            recv_sem=xrsem.at[r, b, j], device_id=x_peers[j], device_id_type=MESH,
        )

    def res_copy(r, b, core):
        at = pl.ds(pl.multiple_of(core * half + b * quarter, 16), quarter)
        return pltpu.make_async_remote_copy(
            src_ref=res.at[r, at], dst_ref=res.at[r, at], send_sem=rsem.at[0, r, b],
            recv_sem=rsem.at[1, r, b], device_id=core_peer, device_id_type=MESH,
        )

    def reduce(r, compute, source, row, factor):
        def send(b, carry):
            compute(b)
            csend[r, b] = acc[b, other].astype(BF16)
            core_copy(r, b).start()
            core_copy(r, b).wait()
            xsend[r, b] = (
                acc[b, mine].astype(BF16).astype(F32) + crecv[r, b].astype(F32)
            ).astype(BF16)
            for j in range(X - 1):
                x_copy(r, b, j).start()
            return carry

        def receive(b, carry):
            for j in range(X - 1):
                x_copy(r, b, j).wait()

            def block(i, inner_carry):
                at = pl.ds(pl.multiple_of(i * 32, 16), 32)
                full = pl.ds(pl.multiple_of(c * half + b * quarter + i * 32, 16), 32)
                total = xsend[r, b, at].astype(F32)
                for j in range(X - 1):
                    total = total + xrecv[r, b, j, at].astype(F32)
                res[r, full] = (
                    source[full].astype(F32) + factor * scaled(total, row)
                ).astype(BF16)
                return inner_carry

            lax.fori_loop(0, quarter // 32, block, 0)
            res_copy(r, b, c).start()
            return carry

        def finish(b, carry):
            res_copy(r, b, c).wait_send()
            res_copy(r, b, 1 - c).wait_recv()
            return carry

        lax.fori_loop(0, 2, send, 0)
        lax.fori_loop(0, 2, receive, 0)
        lax.fori_loop(0, 2, finish, 0)

    def swapped(v):
        q = [v[j * quarter : (j + 1) * quarter] for j in range(4)]
        return jnp.concatenate([q[0], q[2], q[1], q[3]], axis=0)

    def mixer():
        edge = main + 128
        n = swapped(normed[...].reshape(rows, Dp))
        outer_inner = jnp.dot(n, g3[...], preferred_element_type=F32)
        outer_inner = outer_inner.astype(BF16).astype(F32)
        value_rest = jnp.dot(n, g4[:, 0:edge], preferred_element_type=F32)
        value_rest = value_rest.astype(BF16).astype(F32)
        rest = value_rest[:, main:]
        if rem:
            lane = lax.broadcasted_iota(jnp.int32, rest.shape, 1)
            keep = (lane >= 3 * rem) & (lane < 4 * rem)
            rests = [
                jnp.where(keep, pltpu.roll(rest, (3 - j) * rem, 1), 0.0) for j in range(3)
            ]
        else:
            rests = [jnp.zeros_like(rest)] * 3
        outer = jnp.concatenate([rests[0], outer_inner[:, 0:main]], axis=1)
        inner = jnp.concatenate([rests[1], outer_inner[:, main:]], axis=1)
        value = jnp.concatenate([rests[2], value_rest[:, 0:main]], axis=1)
        gated = inner * value
        token = lax.broadcasted_iota(jnp.int32, gated.shape, 0)
        conv = jnp.zeros_like(gated)
        for j in range(CONV_K):
            back = CONV_K - 1 - j
            moved = gated
            if back:
                moved = jnp.where(token >= back, pltpu.roll(gated, back, 0), 0.0)
            conv = conv + taps_ref[j : j + 1, :] * moved
        hidden[...] = swapped((outer * conv).astype(BF16)).reshape(hidden.shape)

    def mixer_block(b):
        acc[b] = lax.dot_general(hidden[b], g4[:, main:], NT, preferred_element_type=F32)

    def last_chunk(b):
        ffn_block(nff - 1, b, nff == 1)

    def second(b):
        acc[b] = jnp.zeros(acc.shape[1:], F32)

        def again(k, carry):
            ffn_block(k, b, False)
            return carry

        lax.fori_loop(0, nff, again, 0)

    for k in range(nff + 2):
        for owner, copy in local:
            if owner == k:
                copy.wait()
        if k < 2:
            own(k)
    norm_to(stream_ref, 0)
    for k in range(nff):
        zsteps(k)
        if k + 2 <= K3:
            own(k + 2)
        if k + 2 == K3:
            across(K4, z, go)
        if k > 0:
            wait_across(k - 1)
            ffn_chunk(k - 1, k == 1)
    zsteps(K3)
    start_a()
    steps_a(True)
    wait_across(nff - 1)
    reduce(0, last_chunk, stream_ref, 1, 0.5)
    norm_to(res.at[0], 2)
    wait_across(K3)
    steps_a(False)
    mixer()
    reduce(1, mixer_block, res.at[0], 3, 1.0)
    norm_to(res.at[1], 4)
    reduce(2, second, res.at[1], 5, 0.5)
    out_ref[...] = res[2]

    def done(copy):
        copy.wait_send()

    for k in range(nff + 1):
        def drain(s, carry):
            @pl.when(s <= z)
            def _():
                right(k, s, done)

            @pl.when(s >= z)
            def _():
                left(k, s, done)

            across(k, s, done)
            return carry

        lax.fori_loop(0, Z, drain, 0)
    across(K4, z, done)

    def drain_a(s, carry):
        @pl.when(s <= z)
        def _():
            right_a(s, done)

        @pl.when(s >= z)
        def _():
            left_a(s, done)

        return carry

    lax.fori_loop(0, Z, drain_a, 0)


def stream_kernel(cfg, *refs):
    Z, shard, part, width, hc, nff, main, rem, grp = cfg
    own_refs = refs[:7]
    stream_ref, gains_ref, taps_ref, out_ref = refs[7:11]
    (ff, g3, gv, gb, pr, edge, xt, gains_in, taps_in, gtmp, gcol, gains, tbuf, normed, hid, mixed,
     part_buf, crecv, xsend, xrecv, tot, res, fd, acc,
     lsem, zsend, recv, psend, precv, pysend, pyrecv, csem, xsem, tsem,
     dsem, hsem) = refs[11:]
    Y = 2
    n_fs = Z * Y
    rows = normed.shape[0]
    Dp = n_fs * shard
    groups = 128 // 32
    pair = Y * shard
    last, K3, KB = nff - 1, nff + 1, nff + 2
    f, t = lax.axis_index("fs"), lax.axis_index("tp")
    z, y = f // Y, f % Y
    c, x = t % 2, t // 2
    core_peer = (f, x * 2 + 1 - c)
    x_peer = (f, (1 - x) * 2 + c)
    x_other = (f, (1 - x) * 2 + 1 - c)
    dev_y = (z * Y + (1 - y), t)

    def dev_z(zz):
        return (zz * Y + y, t)

    own_row = pl.multiple_of(f * shard, 16)
    here = pl.ds(own_row, part)
    lead = pl.ds(0, main)
    gate, up, down, ow, iw, vw, mw = own_refs
    moves = []
    for k in range(nff):
        moves.append((0, down.at[:, pl.ds(k * hc, hc)], ff.at[k, here, pl.ds(2 * hc, hc)]))
    for k in range(nff):
        for j, w in enumerate((gate, up)):
            moves.append((k + 1, w.at[:, pl.ds(k * hc, hc)], ff.at[k, here, pl.ds(j * hc, hc)]))
    moves.append((K3, ow.at[:, lead], g3.at[here, lead]))
    moves.append((K3, iw.at[:, lead], g3.at[here, pl.ds(main, main)]))
    moves.append((K3, vw.at[:, lead], gv.at[here, lead]))
    moves.append((K3, mw.at[:, lead], gb.at[here, :]))
    for j, w in enumerate((ow, iw, vw, mw)):
        moves.append((K3 + 1, w, edge.at[j]))
    moves.append((K3 + 2, gains_ref, gains_in))
    moves.append((K3 + 2, taps_ref, taps_in))
    for s in range(n_fs):
        moves.append((K3 + 2, stream_ref.at[pl.ds(s * part, part)], xt.at[pl.ds(s * shard, part)]))
    local = [
        (k, pltpu.make_async_copy(src, dst, lsem.at[n])) for n, (k, src, dst) in enumerate(moves)
    ]

    def pads(count):
        return [pl.ds(s * shard + part, shard - part) for s in range(count)]

    def clear(ref, index):
        ref[index] = jnp.zeros(ref.at[index].shape, ref.dtype)

    def clear_pairs():
        for pad in pads(n_fs):
            clear(ff, (last, pad, pl.ds(0, hc)))
            clear(gv, (pad, lead))
            clear(gb, (pad,))

    def clear_rest():
        for pad in pads(n_fs):
            for k in range(nff):
                clear(ff, (k, pad, pl.ds(0 if k < last else hc, 3 * hc if k < last else 2 * hc)))
            clear(g3, (pad,))
            clear(gv, (pad, pl.ds(main, 128)))
            clear(xt, (pad,))
        for pad in pads(Z):
            for i in range(1, 4):
                for k in range(nff):
                    clear(fd, (i, k, pad))

    clear_pairs()
    barrier = pltpu.get_barrier_semaphore()

    def greet(d):
        pl.semaphore_signal(barrier, inc=1, device_id=d, device_id_type=MESH)

    for d in (core_peer, x_peer, x_other, dev_y):
        greet(d)

    @pl.when(z > 0)
    def _():
        greet(dev_z(z - 1))

    @pl.when(z < Z - 1)
    def _():
        greet(dev_z(z + 1))

    for _, copy in local:
        copy.start()
    clear_rest()
    peers = 4 + (z > 0).astype(jnp.int32) + (z < Z - 1).astype(jnp.int32)
    pl.semaphore_wait(barrier, peers)

    def local_wait(k):
        for owner, copy in local:
            if owner == k:
                copy.wait()

    def remote(k, s, way, d):
        slot = s // Y + (0, 1, Z + 1)[way]
        at = pl.ds(pl.multiple_of(s * shard, 16), part)
        if k == 0:
            ref = ff.at[:, at, 2 * hc : 3 * hc]
        elif k <= last:
            ref = ff.at[k - 1, at, 0 : 2 * hc]
        elif k == nff:
            ref = ff.at[last, at, hc : 2 * hc]
        else:
            ref = (g3 if k == K3 else gb).at[at]
        return pltpu.make_async_remote_copy(
            src_ref=ref, dst_ref=ref, send_sem=zsend.at[k, slot], recv_sem=recv.at[k, s],
            device_id=d, device_id_type=MESH,
        )

    def right(k, s, act):
        @pl.when(z < Z - 1)
        def _():
            act(remote(k, s * Y + y, 0, dev_z(z + 1)))

    def left(k, s, act):
        @pl.when(z > 0)
        def _():
            act(remote(k, s * Y + y, 1, dev_z(z - 1)))

    def across(k, s, act):
        act(remote(k, s * Y + y, 2, dev_y))

    def go(copy):
        copy.start()

    near = jnp.minimum(z, Z - 1 - z)
    low = z <= Z - 1 - z
    at_end = (z == 0) | (z == Z - 1)

    def inward(go_right, go_left):
        @pl.when(low)
        def _():
            go_right()

        @pl.when(~low)
        def _():
            go_left()

    def own_in(k):
        inward(lambda: right(k, z, go), lambda: left(k, z, go))

    def own_out(k):
        inward(lambda: left(k, z, go), lambda: right(k, z, go))

    def own_y(k):
        across(k, z, go)

    def down_copy(kind, s, v):
        to = (core_peer, x_peer, x_other)[kind]
        return pltpu.make_async_remote_copy(
            src_ref=ff.at[:, pl.ds(pl.multiple_of((s * Y + v) * shard, 16), part), 2 * hc : 3 * hc],
            dst_ref=fd.at[kind + 1, :, pl.ds(pl.multiple_of(s * shard, 16), part)],
            send_sem=dsem.at[0, kind, s], recv_sem=dsem.at[1, kind, s],
            device_id=to, device_id_type=MESH,
        )

    def spread(s, v, act):
        @pl.when(v == c)
        def _():
            act(down_copy(1, s, v))

        @pl.when(v != c)
        def _():
            act(down_copy(2, s, v))
            act(down_copy(0, s, v))

    def zsteps(k):
        def step(i, carry):
            @pl.when(z - 1 - i >= 0)
            def _():
                s = z - 1 - i
                remote(k, s * Y + y, 0, dev_z(z - 1)).wait_recv()
                right(k, s, go)
                across(k, s, go)
                if k == 0:
                    spread(s, y, go)

            @pl.when(z + 1 + i < Z)
            def _():
                s = z + 1 + i
                remote(k, s * Y + y, 0, dev_z(z + 1)).wait_recv()
                left(k, s, go)
                across(k, s, go)
                if k == 0:
                    spread(s, y, go)

            return carry

        lax.fori_loop(0, Z - 1, step, 0)

    def wait_across(k):
        def step(s, carry):
            remote(k, s * Y + 1 - y, 2, dev_y).wait_recv()
            return carry

        lax.fori_loop(0, Z, step, 0)

    def piece(q, first, count):
        if q == 2:
            return pr.at[pl.ds(pl.multiple_of(first * grp, 16), count * grp)]
        at = pl.ds(pl.multiple_of(first * shard, 16), (count - 1) * shard + part)
        return gv.at[at, lead] if q == 1 else ff.at[last, at, 0:hc]

    def across_p(q, s):
        ref = piece(q, s, 1)
        return pltpu.make_async_remote_copy(
            src_ref=ref, dst_ref=ref, send_sem=pysend.at[q], recv_sem=pyrecv.at[q],
            device_id=dev_y, device_id_type=MESH,
        )

    def remote_p(q, s, way, d):
        ref = piece(q, s * Y, Y)
        return pltpu.make_async_remote_copy(
            src_ref=ref, dst_ref=ref, send_sem=psend.at[q, s + way], recv_sem=precv.at[q, s],
            device_id=d, device_id_type=MESH,
        )

    def right_p(q, s, act):
        @pl.when(z < Z - 1)
        def _():
            act(remote_p(q, s, 0, dev_z(z + 1)))

    def left_p(q, s, act):
        @pl.when(z > 0)
        def _():
            act(remote_p(q, s, 1, dev_z(z - 1)))

    def start_in(q):
        across_p(q, z * Y + 1 - y).wait_recv()
        inward(lambda: right_p(q, z, go), lambda: left_p(q, z, go))

    def start_out(q):
        inward(lambda: left_p(q, z, go), lambda: right_p(q, z, go))

    def steps_p(qs, forward, first=0):
        def step(i, carry):
            @pl.when((z - 1 - i >= 0) & ((z < Z - 1) if forward else (z == Z - 1)))
            def _():
                s = z - 1 - i
                for q in qs:
                    remote_p(q, s, 0, dev_z(z - 1)).wait_recv()
                    if forward:
                        right_p(q, s, go)

            @pl.when((z + 1 + i < Z) & ((z > 0) if forward else (z == 0)))
            def _():
                s = z + 1 + i
                for q in qs:
                    remote_p(q, s, 0, dev_z(z + 1)).wait_recv()
                    if forward:
                        left_p(q, s, go)

            return carry

        lax.fori_loop(first, Z - 1, step, 0)

    beside = jnp.where(low, 1, Z - 2)

    def value_z(d):
        ref = piece(1, beside * Y + y, 1)
        return pltpu.make_async_remote_copy(
            src_ref=ref, dst_ref=ref, send_sem=psend.at[1, jnp.where(low, beside + 1, beside)],
            recv_sem=precv.at[1, beside], device_id=d, device_id_type=MESH,
        )

    def value_y(column):
        ref = piece(1, beside * Y + column, 1)
        return pltpu.make_async_remote_copy(
            src_ref=ref, dst_ref=ref, send_sem=pysend.at[3], recv_sem=pyrecv.at[3],
            device_id=dev_y, device_id_type=MESH,
        )

    def to_end():
        return dev_z(jnp.where(low, 0, Z - 1))

    def pack_edges():
        packed = jnp.zeros((grp, 128), F32)
        for j in range(groups):
            count = min(grp, part - j * grp)
            if count <= 0:
                continue
            block = jnp.zeros((count, 128), F32)
            row = lax.broadcasted_iota(jnp.int32, (rem, 128), 0)
            lane = lax.broadcasted_iota(jnp.int32, (rem, 128), 1)
            for k in range(4):
                place = jnp.where(lane == row + (32 * j + rem * k), 1.0, 0.0).astype(BF16)
                source = edge[k, j * grp : j * grp + count, main : main + rem]
                block = block + jnp.dot(source, place, preferred_element_type=F32)
            if count < grp:
                block = jnp.concatenate([block, jnp.zeros((grp - count, 128), F32)], axis=0)
            packed = packed + block
        pr[pl.ds(pl.multiple_of(f * grp, 16), grp)] = packed.astype(BF16)

    def unpack_edges():
        row = lax.broadcasted_iota(jnp.int32, (128, 128), 0)
        lane = lax.broadcasted_iota(jnp.int32, (128, 128), 1)

        def unpack(s):
            packed = pr[pl.ds(pl.multiple_of(s * grp, 16), grp)]
            for j in range(groups):
                count = min(grp, shard - j * grp)
                if count <= 0:
                    continue
                pick = jnp.where((lane < 32) & (row == lane + 32 * j), 1.0, 0.0).astype(BF16)
                block = jnp.dot(packed, pick, preferred_element_type=F32)[:count]
                at = pl.ds(pl.multiple_of(s * shard + j * grp, 16), count)
                gv[at, main : main + 128] = block.astype(BF16)

        def body(i, carry):
            j = order(i)

            @pl.when(at_end & (i > 0))
            def _():
                remote_p(2, j, 0, toward()).wait_recv()

            for v in range(Y):
                unpack(j * Y + v)
            return carry

        lax.fori_loop(0, Z, body, 0)

    def prepare_gains():
        gtmp[...] = jnp.zeros(gtmp.shape, F32)
        gtmp[0:6, 0:width] = gains_in[...]
        for i in range(gtmp.shape[1] // 128):
            gcol[i * 128 : (i + 1) * 128] = gtmp[:, i * 128 : (i + 1) * 128].T

        def body(s, carry):
            for j in range(6):
                column = gcol[pl.ds(pl.multiple_of(s * part, 8), part), j : j + 1]
                at = pl.ds(pl.multiple_of(s * shard, 16), part)
                gains[j, at] = jnp.broadcast_to(column, (part, 128))
                pad = pl.ds(pl.multiple_of(s * shard + part, 8), shard - part)
                gains[j, pad] = jnp.zeros((shard - part, 128), F32)
            return carry

        lax.fori_loop(0, n_fs, body, 0)

    def prepare_taps():
        n_tp = lax.axis_size("tp")
        channels = taps_in.shape[1] // n_tp
        lanes = tbuf.shape[1]
        tbuf[...] = jnp.zeros(tbuf.shape, F32)
        tbuf[0:CONV_K, 0 : taps_in.shape[1]] = taps_in[...].astype(F32)
        full = tbuf[...]
        mine = full
        for i in range(1, n_tp):
            mine = jnp.where(t == i, pltpu.roll(full, lanes - channels * i, 1), mine)
        tbuf[:, 0:main] = mine[:, 0:main]
        rest = pltpu.roll(mine[:, main : main + 128], 3 * rem, 1)
        lane = lax.broadcasted_iota(jnp.int32, rest.shape, 1)
        tbuf[:, main : main + 128] = jnp.where((lane >= 3 * rem) & (lane < 4 * rem), rest, 0.0)

    BLK = 128
    nblk = Dp // BLK

    def squares(v):
        return jnp.sum((v * v).reshape(v.shape[0] // 8, 8, rows), axis=0)

    def block_at(i):
        return pl.ds(pl.multiple_of(i * BLK, BLK), BLK)

    def inverse(sums):
        return lax.rsqrt(jnp.sum(sums, axis=0, keepdims=True) * (1.0 / width) + EPSILON)

    def gain_block(row, at):
        g = gains[row, at]
        return jnp.concatenate([g] * (rows // 128), axis=1)

    def sum_squares(source):
        def body(i, sums):
            return sums + squares(source[block_at(i)].astype(F32))

        return lax.fori_loop(0, nblk, body, jnp.zeros((8, rows), F32))

    def norm_to(source, sums, row):
        scale = inverse(sums)

        def body(i, carry):
            at = block_at(i)
            v = source[at].astype(F32) * scale * gain_block(row, at)
            normed[:, at] = v.T.astype(BF16)
            return carry

        lax.fori_loop(0, nblk, body, 0)

    def update(r, sums, source, row, factor):
        scale = inverse(sums) * factor

        def body(i, sums):
            at = block_at(i)
            v = source[at].astype(F32) + tot[r, at].astype(F32) * scale * gain_block(row, at)
            v = v.astype(BF16)
            res[r, at] = v
            return sums + squares(v.astype(F32))

        return lax.fori_loop(0, nblk, body, jnp.zeros((8, rows), F32))

    def hidden_copy(u, kind, k):
        source = hid.at[u, 2 if kind == 2 else 0, k]
        return pltpu.make_async_remote_copy(
            src_ref=source, dst_ref=hid.at[u, kind + 1, k], send_sem=hsem.at[0, kind, k],
            recv_sem=hsem.at[1, kind, k], device_id=x_peer if kind == 1 else core_peer,
            device_id_type=MESH,
        )

    def hidden(u, k):
        n = normed[...]
        gate_v = jnp.dot(n, ff[k, :, 0:hc], preferred_element_type=F32)
        up_v = jnp.dot(n, ff[k, :, hc : 2 * hc], preferred_element_type=F32)
        hid[u, 0, k] = (gate_v / (1.0 + jnp.exp(-gate_v)) * up_v).astype(BF16)
        hidden_copy(u, 1, k).start()
        hidden_copy(u, 0, k).start()

    def hidden_sent(u):
        for kind in range(3):
            for k in range(nff):
                hidden_copy(u, kind, k).wait_send()

    def product(u, i, k, at):
        return lax.dot_general(fd[i, k, at], hid[u, i, k], NT, preferred_element_type=F32)

    def keep_down():
        def body(s, carry):
            at = pl.ds(pl.multiple_of(s * shard, 16), shard)
            for k in range(nff):
                fd[0, k, at] = ff[
                    k, pl.ds(pl.multiple_of((s * Y + c) * shard, 16), shard), 2 * hc : 3 * hc
                ]
            return carry

        lax.fori_loop(0, Z, body, 0)

    def finish_ffn(u, r, hook, idle):
        def rows_of(j):
            return pl.ds(pl.multiple_of(j * shard, 16), shard)

        def own_part(j, carry):
            at = rows_of(j)
            total = product(u, 0, 0, at)
            for k in range(1, nff):
                total = total + product(u, 0, k, at)
            acc[at] = total
            return carry

        def add(i, ks):
            def body(j, carry):
                at = rows_of(j)
                total = acc[at]
                for k in ks:
                    total = total + product(u, i, k, at)
                acc[at] = total
                return carry

            lax.fori_loop(0, Z, body, 0)

        lax.fori_loop(0, Z, own_part, 0)
        for k in range(nff):
            hidden_copy(u, 0, k).wait_recv()
        add(1, range(nff))
        if idle:
            idle()
        for k in range(nff):
            hidden_copy(u, 1, k).wait_recv()
            hidden_copy(u, 2, k).start()
            if k > 0:
                hidden_copy(u, 2, k - 1).wait_recv()
                add(3, (k - 1,))
            add(2, (k,))
        if hook:
            hook()
        hidden_copy(u, 2, last).wait_recv()

        def final(j, sums):
            at = rows_of(j)
            v = (acc[at] + product(u, 3, last, at)).astype(BF16)
            tot[r, column(j, c)] = v
            tot_copy(r, j).start()
            return sums + squares(v.astype(F32))

        return both_squares(r, lax.fori_loop(0, Z, final, jnp.zeros((8, rows), F32)), lambda j: j)

    def pair_at(j):
        return pl.ds(pl.multiple_of(j * pair, 16), pair)

    def mixer_pair(r, j):
        remote(KB, j * Y + 1 - y, 2, dev_y).wait_recv()
        at = pair_at(j)
        total = lax.dot_general(gb[at], mixed[:, 0:main], NT, preferred_element_type=F32)
        total = total + lax.dot_general(
            gv[at, main : main + 128], mixed[:, main:], NT, preferred_element_type=F32
        )
        part_buf[j] = total.astype(BF16)

    mine = pl.ds(pl.multiple_of(c * shard, 16), shard)
    other = pl.ds(pl.multiple_of((1 - c) * shard, 16), shard)

    def core_copy(r, j):
        return pltpu.make_async_remote_copy(
            src_ref=part_buf.at[j, other], dst_ref=crecv.at[j], send_sem=csem.at[0, j],
            recv_sem=csem.at[1, j], device_id=core_peer, device_id_type=MESH,
        )

    def x_copy(r, j):
        return pltpu.make_async_remote_copy(
            src_ref=xsend.at[j], dst_ref=xrecv.at[j], send_sem=xsem.at[0, j],
            recv_sem=xsem.at[1, j], device_id=x_peer, device_id_type=MESH,
        )

    def column(j, v):
        return pl.ds(pl.multiple_of(j * pair + v * shard, 16), shard)

    def both_squares(r, mine_sums, at):
        def arrive(s, sums):
            tot_copy(r, at(s)).wait()
            return sums + squares(tot[r, column(at(s), 1 - c)].astype(F32))

        return mine_sums + lax.fori_loop(0, Z, arrive, jnp.zeros((8, rows), F32))

    def tot_copy(r, j):
        at = column(j, c)
        return pltpu.make_async_remote_copy(
            src_ref=tot.at[r, at], dst_ref=tot.at[r, at], send_sem=tsem.at[0, j],
            recv_sem=tsem.at[1, j], device_id=core_peer, device_id_type=MESH,
        )

    def toward():
        return dev_z(jnp.where(z == 0, z + 1, z - 1))

    def order(s):
        step = (s + 1) // 2
        close = jnp.where(s % 2 == 1, z - step, z + step)
        return jnp.where(s <= 2 * near, close, jnp.where(low, s, Z - 1 - s))

    def pass_on(j):
        remote(KB, j * Y + y, 0, toward()).wait_recv()
        across(KB, j, go)

    def end_steps(first, stop):
        source = toward()

        def step(s, carry):
            j = order(s)
            remote(K3, j * Y + y, 0, source).wait_recv()
            across(K3, j, go)
            return carry

        @pl.when(at_end)
        def _():
            lax.fori_loop(first, stop, step, 0)

    def reduce(r, compute):
        def cross(j):
            core_copy(r, j).wait_recv()
            xsend[j] = (part_buf[j, mine].astype(F32) + crecv[j].astype(F32)).astype(BF16)
            x_copy(r, j).start()

        def send(s, carry):
            j = order(s)
            @pl.when(at_end & (s > 0) & (s < Z - 1))
            def _():
                pass_on(order(s + 1))

            compute(r, j)
            core_copy(r, j).start()

            @pl.when(s > 0)
            def _():
                cross(order(s - 1))

            return carry

        def receive(s, sums):
            j = order(s)
            x_copy(r, j).wait_recv()
            v = (xsend[j].astype(F32) + xrecv[j].astype(F32)).astype(BF16)
            tot[r, column(j, c)] = v
            tot_copy(r, j).start()
            return sums + squares(v.astype(F32))

        lax.fori_loop(0, Z, send, 0)
        cross(order(Z - 1))
        return both_squares(r, lax.fori_loop(0, Z, receive, jnp.zeros((8, rows), F32)), order)

    def mixer():
        n = normed[...]
        outer_inner = jnp.dot(n, g3[...], preferred_element_type=F32)
        outer_inner = outer_inner.astype(BF16).astype(F32)
        value_rest = jnp.dot(n, gv[...], preferred_element_type=F32)
        value_rest = value_rest.astype(BF16).astype(F32)

        @pl.when(at_end)
        def _():
            pass_on(order(1))

        rest = value_rest[:, main:]
        lane = lax.broadcasted_iota(jnp.int32, rest.shape, 1)
        keep = (lane >= 3 * rem) & (lane < 4 * rem)
        rests = [jnp.where(keep, pltpu.roll(rest, (3 - j) * rem, 1), 0.0) for j in range(3)]
        parts = [
            (outer_inner[:, 0:main], outer_inner[:, main:], value_rest[:, 0:main], 0),
            (rests[0], rests[1], rests[2], main),
        ]
        for outer, inner, value, first in parts:
            lanes = outer.shape[1]
            gated = inner * value
            token = lax.broadcasted_iota(jnp.int32, gated.shape, 0)
            conv = jnp.zeros_like(gated)
            for j in range(CONV_K):
                back = CONV_K - 1 - j
                moved = gated
                if back:
                    moved = jnp.where(token >= back, pltpu.roll(gated, back, 0), 0.0)
                conv = conv + tbuf[j : j + 1, first : first + lanes] * moved
            mixed[:, first : first + lanes] = (outer * conv).astype(BF16)

    def drain_all():
        def done(copy):
            copy.wait_send()

        for k in range(nff + 3):
            def drain(s, carry):
                @pl.when(s <= z)
                def _():
                    right(k, s, done)

                @pl.when(s >= z)
                def _():
                    left(k, s, done)

                across(k, s, done)
                return carry

            lax.fori_loop(0, Z, drain, 0)
        for q in range(3):
            def drain_p(s, carry):
                alone = (s == z) & ~at_end if q == 1 else s < 0

                @pl.when((s <= z) & ~(alone & ~low))
                def _():
                    right_p(q, s, done)

                @pl.when((s >= z) & ~(alone & low))
                def _():
                    left_p(q, s, done)

                return carry

            lax.fori_loop(0, Z, drain_p, 0)
            across_p(q, f).wait_send()

        @pl.when(at_end)
        def _():
            value_y(y).wait_send()

        @pl.when(~at_end)
        def _():
            value_z(to_end()).wait_send()

        def drain_r(s, carry):
            core_copy(1, s).wait_send()
            x_copy(1, s).wait_send()
            for v in range(Y):
                spread(s, v, done)
            return carry

        lax.fori_loop(0, Z, drain_r, 0)

    def spread_across(s, carry):
        j = order(s)
        remote(0, j * Y + 1 - y, 2, dev_y).wait_recv()
        spread(j, 1 - y, go)
        return carry

    for k in range(2):
        local_wait(k)
        own_in(k)
        own_out(k)
        own_y(k)
        if k == 0:
            spread(z, y, go)
    local_wait(K3 + 1)
    pack_edges()
    for k in range(2, K3 + 1):
        local_wait(k)
    for q in range(3):
        across_p(q, f).start()

    @pl.when(at_end)
    def _():
        for k in range(2, KB + 1):
            own_in(k)

    own_out(2)
    own_y(2)
    local_wait(K3 + 2)
    prepare_gains()
    prepare_taps()
    norm_to(xt, sum_squares(xt), 0)
    zsteps(0)
    own_out(nff)
    own_y(nff)

    @pl.when(~at_end)
    def _():
        own_in(2)

    start_in(0)
    start_out(0)

    @pl.when(at_end)
    def _():
        for q in range(1, 3):
            start_in(q)

    zsteps(1)
    lax.fori_loop(0, Z // 2, spread_across, 0)

    @pl.when(~at_end)
    def _():
        own_in(nff)

    zsteps(2)
    own_out(K3)

    @pl.when(~at_end)
    def _():
        own_in(K3)
        start_in(1)
        start_in(2)
        own_in(KB)

    lax.fori_loop(Z // 2, Z, spread_across, 0)
    zsteps(nff)
    steps_p((0,), True)
    own_y(K3)
    keep_down()
    wait_across(1)
    hidden(0, 0)

    @pl.when(~at_end)
    def _():
        zsteps(K3)
        value_z(to_end()).start()
        start_out(2)
        steps_p((1, 2), True)
        own_out(KB)
        own_y(KB)
        zsteps(KB)

    wait_across(2)
    hidden(0, 1)

    def down_arrived(s, carry):
        for kind in range(3):
            down_copy(kind, s, c).wait_recv()
        return carry

    end_steps(1, 2)
    lax.fori_loop(0, Z, down_arrived, 0)
    wait_across(nff)
    steps_p((0,), False)
    hidden(0, last)
    sums = finish_ffn(0, 0, lambda: end_steps(2, Z - 1), None)
    norm_to(res.at[0], update(0, sums, xt, 1, 0.5), 2)
    end_steps(Z - 1, Z)

    @pl.when(at_end)
    def _():
        value_z(toward()).wait_recv()
        value_y(y).start()
        own_y(KB)

    hidden_sent(0)
    wait_across(K3)
    unpack_edges()
    steps_p((1,), False, 1)

    @pl.when(at_end)
    def _():
        value_y(1 - y).wait_recv()

    mixer()
    sums = reduce(1, mixer_pair)
    norm_to(res.at[1], update(1, sums, res.at[0], 3, 1.0), 4)

    def again(k, carry):
        hidden(1, k)
        return carry

    lax.fori_loop(0, nff, again, 0)
    scale = inverse(finish_ffn(1, 2, None, drain_all)) * 0.5
    for s in range(n_fs):
        at = pl.ds(s * shard, part)
        v = res[1, at].astype(F32) + tot[2, at].astype(F32) * scale * gain_block(5, at)
        out_ref[s * part : (s + 1) * part] = v.astype(BF16)
    hidden_sent(1)


def stream_form(mesh, Z):
    def local(stream_in, norm_gains, gate, up, down, outer_w, inner_w, value_w, mixer_w, conv_taps):
        rows, width = stream_in.shape
        part, hid = gate.shape
        channels = outer_w.shape[1]
        n_fs = 2 * Z
        shard = -(-part // 16) * 16
        Dp = n_fs * shard
        nff = 3
        hc = hid // nff
        main = channels // 128 * 128
        rem = channels - main
        grp = -(-part // 64) * 16
        lanes = -(-width // 128) * 128
        taps = -(-conv_taps.shape[1] // 128) * 128
        dma, vmem = pltpu.SemaphoreType.DMA, pltpu.VMEM
        out = pl.pallas_call(
            functools.partial(stream_kernel, (Z, shard, part, width, hc, nff, main, rem, grp)),
            out_shape=pltpu.VMEM((width, rows), BF16),
            in_specs=[pl.BlockSpec(memory_space=pl.ANY)] * 10,
            out_specs=pl.BlockSpec(memory_space=pltpu.VMEM),
            scratch_shapes=[
                vmem((nff, Dp, 3 * hc), BF16),
                vmem((Dp, 2 * main), BF16),
                vmem((Dp, main + 128), BF16),
                vmem((Dp, main), BF16),
                vmem((n_fs * grp, 128), BF16),
                vmem((4, part, channels), BF16),
                vmem((Dp, rows), BF16),
                vmem(norm_gains.shape, F32),
                vmem(conv_taps.shape, BF16),
                vmem((128, lanes), F32),
                vmem((lanes, 128), F32),
                vmem((6, Dp, 128), F32),
                vmem((8, taps), F32),
                vmem((rows, Dp), BF16),
                vmem((2, 4, nff, rows, hc), BF16),
                vmem((rows, main + 128), BF16),
                vmem((Z, 2 * shard, rows), BF16),
                vmem((Z, shard, rows), BF16),
                vmem((Z, shard, rows), BF16),
                vmem((Z, shard, rows), BF16),
                vmem((3, Dp, rows), BF16),
                vmem((2, Dp, rows), BF16),
                vmem((4, nff, Z * shard, hc), BF16),
                vmem((Z * shard, rows), F32),
                dma((3 * nff + 10 + n_fs,)),
                dma((nff + 3, 2 * Z + 1)),
                dma((nff + 3, n_fs)),
                dma((4, Z + 1)),
                dma((4, Z)),
                dma((4,)),
                dma((4,)),
                dma((2, Z)),
                dma((2, Z)),
                dma((2, Z)),
                dma((2, 3, Z)),
                dma((2, 3, nff)),
            ],
            compiler_params=pltpu.CompilerParams(
                collective_id=0, has_side_effects=True, vmem_limit_bytes=60 * 1024 * 1024
            ),
        )(gate, up, down, outer_w, inner_w, value_w, mixer_w, stream_in.T, norm_gains, conv_taps)
        return out.T

    return local


def y_count(mesh):
    try:
        found = len({d.coords[1] for d in mesh.devices.reshape(-1)})
    except AttributeError:
        found = 1
    return found if found == 2 and mesh.shape["fs"] % 2 == 0 else 1


def solution(mesh):
    n_fs, n_tp = mesh.shape["fs"], mesh.shape["tp"]
    Y = y_count(mesh)
    Z, X = n_fs // Y, n_tp // 2

    def chain_form(stream_in, norm_gains, gate, up, down, outer_w, inner_w, value_w, mixer_w, conv_taps):
        rows, width = stream_in.shape
        part, hid = gate.shape
        channels = outer_w.shape[1]
        shard = -(-part // 16) * 16
        Dp = n_fs * shard
        nff = 3 if hid % 384 == 0 else 1
        hc = hid // nff
        main = channels // 128 * 128
        rem = channels - main

        def widen(v):
            lead = v.shape[0]
            v = v.reshape(lead, n_fs, part)
            return jnp.pad(v, ((0, 0), (0, 0), (0, shard - part))).reshape(lead, Dp)

        sent = -(-part // 8) * 8

        def pack(w):
            return w if sent == part else jnp.pad(w, ((0, sent - part), (0, 0)))

        rest = [w[:, main:] for w in (outer_w, inner_w, value_w, mixer_w)]
        rest.append(jnp.zeros((part, 128 - 4 * rem), BF16))
        owns = [gate, up, down, outer_w, inner_w, value_w, mixer_w]
        owns = [pack(w) for w in owns + [jnp.concatenate(rest, axis=1)]]
        taps = lax.dynamic_slice_in_dim(
            conv_taps, lax.axis_index("tp") * channels, channels, 1
        ).astype(F32)
        taps = jnp.concatenate(
            [jnp.pad(taps[:, main:], ((0, 0), (3 * rem, 128 - 4 * rem))), taps[:, :main]], axis=1
        )
        half, quarter = rows // 2, rows // 4
        dma, vmem = pltpu.SemaphoreType.DMA, pltpu.VMEM
        out = pl.pallas_call(
            functools.partial(kernel, (Z, Y, X, shard, sent, width, hc, nff, main, rem)),
            out_shape=jax.ShapeDtypeStruct((rows, Dp), BF16),
            in_specs=[pl.BlockSpec(memory_space=pl.ANY)] * 8
            + [pl.BlockSpec(memory_space=pltpu.VMEM)] * 3,
            out_specs=pl.BlockSpec(memory_space=pltpu.VMEM),
            scratch_shapes=[
                vmem((nff, Dp, 3 * hc), BF16),
                vmem((Dp, 2 * main), BF16),
                vmem((Dp, 2 * main + 128), BF16),
                vmem((2, half, Dp), BF16),
                vmem((2, half, Dp), F32),
                vmem((2, half, main + 128), BF16),
                vmem((3, 2, quarter, Dp), BF16),
                vmem((3, 2, quarter, Dp), BF16),
                vmem((3, 2, quarter, Dp), BF16),
                vmem((3, 2, X - 1, quarter, Dp), BF16),
                vmem((3, rows, Dp), BF16),
                dma((3 * nff + 5,)),
                dma((nff + 2, 3, n_fs)),
                dma((nff + 2, n_fs)),
                dma((2, Z)),
                dma((Z,)),
                dma((2, 3, 2)),
                dma((3, 2, X - 1)),
                dma((3, 2, X - 1)),
                dma((2, 3, 2)),
            ],
            compiler_params=pltpu.CompilerParams(
                collective_id=0, has_side_effects=True, vmem_limit_bytes=60 * 1024 * 1024
            ),
        )(*owns, widen(stream_in), widen(norm_gains), taps)
        return out.reshape(rows, n_fs, shard)[:, :, :part].reshape(rows, width)

    def local(*args):
        rows, width = args[0].shape
        part, channels = args[5].shape
        rem = channels % 128
        fits = Y == 2 and X == 2 and part % 8 == 0 and 0 < rem <= 8 and rows % 128 == 0
        fits = fits and (n_fs * (-(-part // 16) * 16)) % 128 == 0 and channels > 128
        fits = fits and args[2].shape[1] % 384 == 0 and Z == 4
        return (stream_form(mesh, Z) if fits else chain_form)(*args)

    return jax.shard_map(
        local,
        mesh=mesh,
        in_specs=(P("fs", None), P()) + (P("fs", "tp"),) * 7 + (P(),),
        out_specs=P("fs", None),
        check_vma=False,
    )
```
